512 devices in a mesh: grp: 2 (over y), kv: 32 (over z, core), tp: 8 (over x).
Axes of the slice: x: 8, y: 2, z: 16, core: 2. Of those that a mesh axis runs over, the one named last changes fastest.
The devices are a block of a 8x8x16 slice.
Arguments:
- tokens: bfloat16 [256, 4096], P('grp', 'kv'), parts along dimension 0, may hold values from -16 to 16
- positions: int32 [256], P(('grp', 'kv')), parts along dimension 0, may hold values from 512 to 8191
- state: float32 [256, 16, 128, 128], P(('grp', 'kv'), 'tp'), parts along dimension 0, may hold values from -3 to 3
- norm_gain: float32 [4096], P('kv'), may hold values from 0.1 to 1.9
- w_query: bfloat16 [4096, 2048], P('kv', 'tp'), may hold values from -0.09375 to 0.09375
- w_key: bfloat16 [4096, 2048], P('kv', 'tp'), may hold values from -0.09375 to 0.09375
- w_value: bfloat16 [4096, 2048], P('kv', 'tp'), may hold values from -0.09375 to 0.09375
- w_gate: bfloat16 [4096, 2048], P('kv', 'tp'), may hold values from -0.09375 to 0.09375
- w_out: bfloat16 [2048, 4096], P('tp', 'kv'), may hold values from -0.125 to 0.125
- mlp_gain: float32 [4096], P('kv'), may hold values from 0.1 to 1.9
- w_up: bfloat16 [4096, 16384], P('kv', 'tp'), may hold values from -0.09375 to 0.09375
- w_down: bfloat16 [16384, 4096], P('tp', 'kv'), may hold values from -0.046875 to 0.046875
Outputs:
- layer_out: bfloat16 [256, 4096], P('grp', 'kv'), parts along dimension 0
- new_state: float32 [256, 16, 128, 128], P(('grp', 'kv'), 'tp'), parts along dimension 0
The draws below stay inside these ranges and needn't reach their ends.
There are 2 independent parts, one for each index of `grp`. The reference program is written for one: setup_inputs(seed, part) draws one part's arguments, and reference() takes and returns one part's arrays. A program takes and returns all parts, laid end to end along the dimension named above; an argument that names none is the same for every part. Nothing has to cross between parts.
All inputs are finite; a program needn't handle non-finite values.
Results may differ from the reference program's by a relative error of at most 0.007.
Values may be sent and summed in bfloat16 or wider, within the bound.
A program may use at most 64 MiB of HBM per device.

```python
import jax
import jax.numpy as jnp
from jax import lax

D = 4096
HEADS = 16
HEAD_DIM = 128
FF = 16384
BATCH = 128
RET = 2048


def draw_tokens(key, part):
    first = jax.random.fold_in(jax.random.fold_in(key, 11), 0)
    columns = jnp.exp(jnp.log(4.0) * jnp.arange(D, dtype=jnp.float32) / D) * 0.5
    base = jnp.clip(jax.random.normal(first, (BATCH, D), jnp.float32), -4.0, 4.0)
    values = base * columns[None, :]
    return values.astype(jnp.bfloat16)


def with_ends(values, own_key, low, top_value):
    longest = values.shape.index(max(values.shape))
    spots = []
    for shift in (0, 1):
        where = [jax.random.randint(jax.random.fold_in(own_key, axis), (), 0, length) for axis, length in enumerate(values.shape)]
        where[longest] = (where[longest] + shift) % values.shape[longest]
        spots.append(tuple(where))
    return values.at[spots[0]].set(low).at[spots[1]].set(top_value)


def block_scale(rng, shape, pieces, least, largest):
    def one(axis_at, blocks):
        steps = jax.random.uniform(jax.random.fold_in(jax.random.fold_in(rng, 6), axis_at), (blocks,), jnp.float32, least / len(pieces), largest / len(pieces))
        return jnp.repeat(jnp.exp(steps), shape[axis_at] // blocks).reshape((-1,) + (1,) * (len(shape) - axis_at - 1))

    level = one(*pieces[0])
    for cut in pieces[1:]:
        level = level * one(*cut)
    return level


def centred(key, dims, deviation, most, pieces=(), kind=jnp.bfloat16):
    values = deviation * jax.random.normal(key, dims, jnp.float32)
    if pieces:
        values = values * block_scale(key, dims, pieces, -0.22, 0.18)
    return jnp.clip(values, -most, most).astype(kind)


def setup_inputs(seed: int = 0, part: int = 0) -> dict:
    splits = jax.random.split(jax.random.key(seed), 13)
    part_keys = jax.random.split(jax.random.fold_in(splits[12], part), 13)
    tokens = draw_tokens(jax.random.fold_in(jax.random.fold_in(splits[12], part), 71), part)
    positions = with_ends(jax.random.randint(part_keys[1], (BATCH,), 512, 8192), jax.random.fold_in(part_keys[1], 1), 512, 8191).astype(jnp.int32)
    state = centred(part_keys[2], (BATCH, HEADS, HEAD_DIM, HEAD_DIM), 0.5, 3.0, ((0, 32), (1, 8)), jnp.float32)
    norm_gain = jnp.clip(1.0 + 0.18 * jax.random.normal(splits[3], (D,), jnp.float32), 0.1, 1.9)
    w_query = centred(splits[4], (D, RET), D ** -0.5, 0.09375, ((0, 32), (1, 8)))
    w_key = centred(splits[5], (D, RET), D ** -0.5, 0.09375, ((0, 32), (1, 8)))
    w_value = centred(splits[6], (D, RET), D ** -0.5, 0.09375, ((0, 32), (1, 8)))
    w_gate = centred(splits[7], (D, RET), D ** -0.5, 0.09375, ((0, 32), (1, 8)))
    w_out = centred(splits[8], (RET, D), RET ** -0.5, 0.125, ((0, 8), (1, 32)))
    mlp_gain = jnp.clip(1.0 + 0.18 * jax.random.normal(splits[9], (D,), jnp.float32), 0.1, 1.9)
    w_up = centred(splits[10], (D, FF), D ** -0.5, 0.09375, ((0, 32), (1, 8)))
    w_down = centred(splits[11], (FF, D), FF ** -0.5, 0.046875, ((0, 8), (1, 32)))
    return dict(tokens=tokens, positions=positions, state=state, norm_gain=norm_gain, w_query=w_query, w_key=w_key, w_value=w_value, w_gate=w_gate, w_out=w_out, mlp_gain=mlp_gain, w_up=w_up, w_down=w_down)


def turn(values, positions):
    half = values.shape[-1] // 2
    freq = 10000.0 ** (-(jnp.arange(half, dtype=jnp.float32) * 2.0) / values.shape[-1])
    angle = positions.astype(jnp.float32)[:, None, None] * freq[None, None, :]
    cosine = jnp.cos(angle)
    sine = jnp.sin(angle)
    first = values[..., :half]
    second = values[..., half:]
    return jnp.concatenate([first * cosine - second * sine, first * sine + second * cosine], axis=-1)

def reference(tokens, positions, state, norm_gain, w_query, w_key, w_value, w_gate, w_out, mlp_gain, w_up, w_down):
    rows = tokens.shape[0]
    inputs = tokens.astype(jnp.float32)
    scale1 = lax.rsqrt(lax.optimization_barrier(jnp.mean(inputs * inputs, axis=1)) + 1e-06)
    normed = (inputs * norm_gain).astype(jnp.bfloat16)

    def project(weight):
        raw = jnp.dot(normed, weight, preferred_element_type=jnp.float32) * scale1[:, None]
        return raw.reshape(rows, HEADS, HEAD_DIM)
    query = turn(project(w_query), positions)
    key = turn(project(w_key), positions) * HEAD_DIM ** (-0.5)
    value = project(w_value)
    gate = project(w_gate)
    heads = jnp.arange(HEADS, dtype=jnp.float32)
    gamma = 1.0 - 2.0 ** (-5.0 - 5.0 * heads / (HEADS - 1))
    new_state = gamma[None, :, None, None] * state + key[:, :, :, None] * value[:, :, None, :]
    read = jnp.einsum('bhd,bhde->bhe', query, new_state, precision=lax.Precision.HIGHEST)
    read = read * lax.rsqrt(lax.optimization_barrier(jnp.mean(read * read, axis=-1, keepdims=True)) + 1e-06)
    retained = (read * jax.nn.silu(gate)).reshape(rows, HEADS * HEAD_DIM).astype(jnp.bfloat16)
    mixed = (inputs + jnp.dot(retained, w_out, preferred_element_type=jnp.float32)).astype(jnp.bfloat16)
    middle = mixed.astype(jnp.float32)
    scale2 = lax.rsqrt(lax.optimization_barrier(jnp.mean(middle * middle, axis=1)) + 1e-06)
    normed2 = (middle * mlp_gain).astype(jnp.bfloat16)
    upward = jnp.dot(normed2, w_up, preferred_element_type=jnp.float32) * scale2[:, None]
    hidden = jnp.square(jax.nn.relu(upward)).astype(jnp.bfloat16)
    layer_out = (middle + jnp.dot(hidden, w_down, preferred_element_type=jnp.float32)).astype(jnp.bfloat16)
    return (layer_out, new_state)
```

```python
import functools

import jax
import jax.numpy as jnp
import numpy as np
from jax import lax
from jax.experimental import pallas as pl
from jax.experimental.pallas import tpu as pltpu
from jax.sharding import PartitionSpec as P

MESH = pl.DeviceIdType.MESH
F32 = jnp.float32
BF16 = jnp.bfloat16
EPS = 1e-06


def far_first(step, count):
    swing = (step + 1) // 2
    return count // 2 + swing * (2 * (step % 2) - 1)


def kernel(
    cfg,
    pos_ref,
    x_hbm,
    state_hbm,
    gain_hbm,
    wq_hbm,
    wk_hbm,
    wv_hbm,
    wg_hbm,
    wo_hbm,
    gain2_hbm,
    wu_hbm,
    wd_hbm,
    freq_ref,
    out_ref,
    state_out,
    x_in,
    gain_in,
    w_in,
    state_in,
    state_new,
    wo_in,
    wu_in,
    wd_in,
    tok2,
    gain2,
    part,
    swap_s,
    swap_r,
    sq_s,
    sq_r,
    send_a,
    recv_a,
    ret_s,
    ret_r,
    ret_f,
    send_c,
    recv_c,
    tok_rows,
    mix_s,
    mix_r,
    sq2_s,
    sq2_r,
    send_d,
    recv_d,
    hid_s,
    hid_r,
    out_s,
    out_r,
    load_sem,
    send_sem,
    recv_sem,
):
    nk, nt, nz, d_model, heads_all = cfg
    me = lax.axis_index("kv")
    tp = lax.axis_index("tp")
    z = me // 2
    c = me % 2
    mate = me + 1 - 2 * c
    block = tp * 2 + c
    nb = nt * 2
    rows = x_in.shape[0]
    width = x_in.shape[1]
    seqs = rows // nk
    per_chip = rows // nz
    size = width
    half_ff = wu_in.shape[1]

    def kv_peer(step):
        chip = lax.rem(z + far_first(step // 2, nz), nz)
        other = lax.rem(c + step % 2, 2)
        last = (step == nk - 2).astype(jnp.int32)
        return last * mate + (1 - last) * (chip * 2 + other)

    def chip_peer(step):
        return lax.rem(z + far_first(step, nz), nz) * 2 + c

    def block_peer(step):
        chip = lax.rem(tp + far_first(step // 2, nt), nt)
        other = lax.rem(c + step % 2, 2)
        last = (step == nb - 2).astype(jnp.int32)
        return last * tp + (1 - last) * chip, last * (1 - c) + (1 - last) * other

    def each(count, body):
        lax.fori_loop(0, count, lambda i, carry: (body(i), carry)[1], 0)

    barrier = pltpu.get_barrier_semaphore()

    def greet_kv(i):
        pl.semaphore_signal(barrier, inc=1, device_id={"kv": kv_peer(i)}, device_id_type=MESH)

    def greet_block(i):
        t, core = block_peer(i)
        pl.semaphore_signal(
            barrier, inc=1, device_id={"kv": z * 2 + core, "tp": t}, device_id_type=MESH
        )

    each(nk - 1, greet_kv)
    each(nb - 2, greet_block)

    def load(src, dst, sem):
        copy = pltpu.make_async_copy(src, dst, load_sem.at[sem])
        copy.start()
        return copy

    first = [
        load(x_hbm, x_in, 0),
        load(gain_hbm, gain_in, 1),
        load(wq_hbm, w_in.at[0], 2),
        load(wk_hbm, w_in.at[1], 3),
        load(wv_hbm, w_in.at[2], 4),
        load(wg_hbm, w_in.at[3], 5),
    ]
    here = pl.ds(pl.multiple_of(c * half_ff, 128), half_ff)
    there = pl.ds(pl.multiple_of((1 - c) * half_ff, 128), half_ff)
    mine = pl.ds(pl.multiple_of(c * size, 128), size)
    other_head = pl.ds(pl.multiple_of((1 - c) * size, 128), size)
    my_rows = pl.ds(pl.multiple_of(c * width, 128), width)
    later = [
        load(state_hbm, state_in, 6),
        load(wo_hbm.at[mine], wo_in.at[:, my_rows], 7),
        load(gain2_hbm, gain2.at[:, my_rows], 8),
        load(wu_hbm.at[:, here], wu_in.at[my_rows], 9),
        load(wd_hbm.at[here], wd_in.at[:, my_rows], 10),
    ]

    for copy in first:
        copy.wait()
    x = x_in[...].astype(F32)
    normed = (x * gain_in[...]).astype(BF16)
    square = x * x
    sq_s[...] = jnp.sum(jnp.transpose(square), axis=0, keepdims=True)
    sq_r[me] = sq_s[...]
    for n in range(4):
        both = jnp.dot(normed, w_in[n], preferred_element_type=F32)
        part[0, :, n * size : (n + 1) * size] = both[:, :size]
        part[1, :, n * size : (n + 1) * size] = both[:, size:]
    swap_s[...] = part[1 - c].astype(BF16)
    tok2[c] = x_in[...]

    pl.semaphore_wait(barrier, nk - 1 + nb - 2)

    def remote(src, dst, phase, kv, t=None):
        where = {"kv": kv} if t is None else {"kv": kv, "tp": t}
        pltpu.make_async_remote_copy(
            src_ref=src,
            dst_ref=dst,
            send_sem=send_sem.at[phase],
            recv_sem=recv_sem.at[phase],
            device_id=where,
            device_id_type=MESH,
        ).start()

    def arrived(ref, phase):
        pltpu.make_async_copy(ref, ref, recv_sem.at[phase]).wait()

    def left(ref, phase):
        pltpu.make_async_copy(ref, ref, send_sem.at[phase]).wait()

    remote(swap_s, swap_r, 0, mate)

    def send_squares(i):
        remote(sq_s, sq_r.at[me], 1, kv_peer(i))

    each(nk - 1, send_squares)
    remote(x_in, tok2.at[c], 2, mate)
    remote(gain2_hbm, gain2.at[:, my_rows], 3, mate)
    remote(wo_hbm.at[other_head], wo_in.at[:, my_rows], 4, mate)
    remote(wu_hbm.at[:, there], wu_in.at[my_rows], 5, mate)
    remote(wd_hbm.at[there], wd_in.at[:, my_rows], 6, mate)

    arrived(swap_r, 0)
    part[c] = part[c] + swap_r[...].astype(F32)
    for j in range(nk):
        send_a[j] = part[c, j * seqs : (j + 1) * seqs, :].astype(BF16)
    recv_a[me] = send_a[me]

    def send_terms(i):
        peer = kv_peer(i)
        remote(send_a.at[peer], recv_a.at[me], 7, peer)

    each(nk - 1, send_terms)

    row = lax.broadcasted_iota(jnp.int32, (seqs, size), 0)
    lane = lax.broadcasted_iota(jnp.int32, (seqs, size), 1)
    place = jnp.zeros((seqs, size), F32)
    for i in range(seqs):
        place = jnp.where(row == i, pos_ref[i].astype(F32), place)
    angle = place * freq_ref[...]
    cosine = jnp.cos(angle)
    sine = jnp.sin(angle)
    sine = jnp.where(lane < size // 2, -sine, sine)
    later[0].wait()

    arrived(sq_r.at[pl.ds(0, nk - 1)], 1)
    total_sq = jnp.sum(sq_r[...], axis=0)
    row_sq = jnp.sum(jnp.where(lane == row + me * seqs, total_sq, 0.0), axis=1, keepdims=True)
    scale1 = lax.rsqrt(row_sq / d_model + EPS)

    arrived(recv_a.at[pl.ds(0, nk - 1)], 7)
    queries, keys, values, gates = [], [], [], []

    def turn(v):
        return v * cosine + pltpu.roll(v, size // 2, 1) * sine

    for h in range(2):
        total = recv_a[h].astype(F32)
        for j in range(1, nz):
            total = total + recv_a[2 * j + h].astype(F32)
        total = total * scale1
        queries.append(turn(total[:, :size]))
        keys.append(turn(total[:, size : 2 * size]) * size**-0.5)
        values.append(total[:, 2 * size : 3 * size])
        gates.append(total[:, 3 * size :])
    pad = jnp.zeros((size - 4 * seqs, size), F32)
    columns = jnp.transpose(jnp.concatenate(queries + keys + [pad], axis=0))
    for h in range(2):
        head = (tp * 2 + h).astype(F32)
        power = jnp.full((1, size), -5.0, F32) - 5.0 * head / (heads_all - 1)
        gamma = 1.0 - jnp.exp2(power)
        reads = []
        for i in range(seqs):
            at = h * seqs + i
            new = (
                gamma * state_in[i, h]
                + columns[:, 2 * seqs + at : 2 * seqs + at + 1] * values[h][i : i + 1]
            )
            state_new[i, h] = new
            reads.append(jnp.sum(columns[:, at : at + 1] * new, axis=0, keepdims=True))
        read = jnp.concatenate(reads, axis=0)
        read = read * lax.rsqrt(jnp.mean(read * read, axis=1, keepdims=True) + EPS)
        gate = gates[h]
        ret_s[h] = (read * (gate / (1.0 + jnp.exp(-gate)))).astype(BF16)
    ret_r[me] = ret_s[c]

    def send_retained(i):
        peer = kv_peer(i)
        remote(ret_s.at[peer % 2], ret_r.at[me], 8, peer)

    each(nk - 1, send_retained)
    state_copy = load(state_new, state_out, 11)

    later[1].wait()
    later[2].wait()
    arrived(tok2.at[0], 2)
    arrived(gain2.at[:, pl.ds(0, width)], 3)
    arrived(wo_in.at[:, pl.ds(0, width)], 4)
    for m in range(nb):
        for s in range(2):
            tok_rows[m, :, s * width : (s + 1) * width] = tok2[
                s, m * per_chip : (m + 1) * per_chip
            ].astype(F32)

    arrived(ret_r.at[pl.ds(0, nk - 1)], 8)
    for j in range(nk):
        ret_f[j * seqs : (j + 1) * seqs] = ret_r[j].astype(F32)
    terms = jnp.dot(ret_f[...].astype(BF16), wo_in[...], preferred_element_type=F32)
    send_c[0] = terms.reshape(nb, per_chip, 2 * width).astype(BF16)
    recv_c[0, block] = send_c[0, block]

    def send_sums(which, phase):
        def send(i):
            t, core = block_peer(i)
            remote(send_c.at[which, t * 2 + core], recv_c.at[which, block], phase, z * 2 + core, t)

        each(nb - 1, send)

    send_sums(0, 9)
    arrived(recv_c.at[0, pl.ds(0, nb - 1)], 9)
    mixed = (tok_rows[block] + jnp.sum(recv_c[0].astype(F32), axis=0)).astype(BF16)
    mix_s[...] = mixed
    mix_r[block] = mixed

    def send_mixed(i):
        t, core = block_peer(i)
        remote(mix_s, mix_r.at[block], 10, z * 2 + core, t)

    each(nb - 1, send_mixed)
    later[3].wait()
    arrived(wu_in.at[pl.ds(0, width)], 5)
    arrived(mix_r.at[pl.ds(0, nb - 1)], 10)
    middle = mix_r[...].astype(F32).reshape(rows, 2 * width)
    square = middle * middle
    sq2_s[...] = jnp.sum(
        jnp.transpose(square[:, :width] + square[:, width:]), axis=0, keepdims=True
    )
    sq2_r[z] = sq2_s[...]

    def send_squares2(i):
        remote(sq2_s, sq2_r.at[z], 11, chip_peer(i))

    each(nz - 1, send_squares2)
    normed2 = (middle * gain2[...]).astype(BF16)
    upward = jnp.dot(normed2, wu_in[...], preferred_element_type=F32)
    send_d[...] = upward.reshape(nz, per_chip, half_ff).astype(BF16)
    recv_d[z] = send_d[z]

    def send_up(i):
        peer = chip_peer(i)
        remote(send_d.at[peer // 2], recv_d.at[z], 12, peer)

    each(nz - 1, send_up)
    row = lax.broadcasted_iota(jnp.int32, (per_chip, size), 0)
    lane = lax.broadcasted_iota(jnp.int32, (per_chip, size), 1)
    arrived(sq2_r.at[pl.ds(0, nz - 1)], 11)
    total_sq = jnp.sum(sq2_r[...], axis=0)
    row_sq = jnp.sum(jnp.where(lane == row + z * per_chip, total_sq, 0.0), axis=1, keepdims=True)
    scale2 = lax.rsqrt(row_sq / d_model + EPS)
    arrived(recv_d.at[pl.ds(0, nz - 1)], 12)
    total = recv_d[0].astype(F32)
    for j in range(1, nz):
        total = total + recv_d[j].astype(F32)
    hidden = jnp.maximum(total * scale2, 0.0)
    hid_s[...] = (hidden * hidden).astype(BF16)
    hid_r[z] = hid_s[...]

    def send_hidden(i):
        remote(hid_s, hid_r.at[z], 13, chip_peer(i))

    each(nz - 1, send_hidden)
    later[4].wait()
    arrived(wd_in.at[:, pl.ds(0, width)], 6)
    arrived(hid_r.at[pl.ds(0, nz - 1)], 13)
    hidden_all = hid_r[...].astype(F32).reshape(rows, half_ff).astype(BF16)
    terms = jnp.dot(hidden_all, wd_in[...], preferred_element_type=F32)
    send_c[1] = terms.reshape(nb, per_chip, 2 * width).astype(BF16)
    recv_c[1, block] = send_c[1, block]
    send_sums(1, 14)
    arrived(recv_c.at[1, pl.ds(0, nb - 1)], 14)
    final = (mix_s[...].astype(F32) + jnp.sum(recv_c[1].astype(F32), axis=0)).astype(BF16)
    for s in range(2):
        out_s[s] = final[:, s * width : (s + 1) * width]
    out_r[block] = out_s[c]

    def send_out(i):
        t, core = block_peer(i)
        remote(out_s.at[core], out_r.at[block], 15, z * 2 + core, t)

    each(nb - 1, send_out)

    state_copy.wait()
    left(swap_s, 0)
    left(sq_r.at[pl.ds(0, nk - 1)], 1)
    left(x_in, 2)
    left(gain_in, 3)
    left(w_in.at[0, :, pl.ds(0, width)], 4)
    left(wu_in.at[pl.ds(0, width)], 5)
    left(wd_in.at[:, pl.ds(0, width)], 6)
    left(send_a.at[pl.ds(0, nk - 1)], 7)
    left(ret_r.at[pl.ds(0, nk - 1)], 8)
    left(send_c.at[0, pl.ds(0, nb - 1)], 9)
    left(mix_r.at[pl.ds(0, nb - 1)], 10)
    left(sq2_r.at[pl.ds(0, nz - 1)], 11)
    left(send_d.at[pl.ds(0, nz - 1)], 12)
    left(hid_r.at[pl.ds(0, nz - 1)], 13)
    left(send_c.at[1, pl.ds(0, nb - 1)], 14)
    left(out_r.at[pl.ds(0, nb - 1)], 15)
    arrived(out_r.at[pl.ds(0, nb - 1)], 15)
    out_ref[...] = out_r[...].astype(F32).reshape(rows, width).astype(BF16)


def solution(mesh):
    nk, nt = mesh.shape["kv"], mesh.shape["tp"]
    nz = nk // 2

    def shards(
        tokens,
        positions,
        state,
        norm_gain,
        w_query,
        w_key,
        w_value,
        w_gate,
        w_out,
        mlp_gain,
        w_up,
        w_down,
    ):
        rows, width = tokens.shape
        seqs, heads, size, _ = state.shape
        ff = w_up.shape[1]
        per_chip = rows // nz
        nb = 2 * nt
        inverse = 10000.0 ** (-(np.arange(size // 2, dtype=np.float64) * 2.0) / size)
        freq = jnp.asarray(np.concatenate([inverse, inverse])[None, :].astype(np.float32))
        cfg = (nk, nt, nz, width * nk, heads * nt)
        anywhere = pl.BlockSpec(memory_space=pl.ANY)
        vmem = pl.BlockSpec(memory_space=pltpu.VMEM)
        smem = pl.BlockSpec(memory_space=pltpu.SMEM)
        scratch = [
            ((rows, width), BF16),
            ((1, width), F32),
            ((4, width, heads * size), BF16),
            (state.shape, F32),
            (state.shape, F32),
            ((size, 2 * width), BF16),
            ((2 * width, ff // 2), BF16),
            ((ff // 2, 2 * width), BF16),
            ((2, rows, width), BF16),
            ((1, 2 * width), F32),
            ((2, rows, 4 * size), F32),
            ((rows, 4 * size), BF16),
            ((rows, 4 * size), BF16),
            ((1, rows), F32),
            ((nk, 1, rows), F32),
            ((nk, seqs, 4 * size), BF16),
            ((nk, seqs, 4 * size), BF16),
            ((2, seqs, size), BF16),
            ((nk, seqs, size), BF16),
            ((rows, size), F32),
            ((2, nb, per_chip, 2 * width), BF16),
            ((2, nb, per_chip, 2 * width), BF16),
            ((nb, per_chip, 2 * width), F32),
            ((per_chip, 2 * width), BF16),
            ((nb, per_chip, 2 * width), BF16),
            ((1, rows), F32),
            ((nz, 1, rows), F32),
            ((nz, per_chip, ff // 2), BF16),
            ((nz, per_chip, ff // 2), BF16),
            ((per_chip, ff // 2), BF16),
            ((nz, per_chip, ff // 2), BF16),
            ((2, per_chip, width), BF16),
            ((nb, per_chip, width), BF16),
        ]
        return pl.pallas_call(
            functools.partial(kernel, cfg),
            out_shape=(
                jax.ShapeDtypeStruct((rows, width), BF16),
                jax.ShapeDtypeStruct(state.shape, F32),
            ),
            in_specs=[smem] + [anywhere] * 11 + [vmem],
            out_specs=(vmem, anywhere),
            scratch_shapes=[pltpu.VMEM(s, t) for s, t in scratch]
            + [
                pltpu.SemaphoreType.DMA((12,)),
                pltpu.SemaphoreType.DMA((16,)),
                pltpu.SemaphoreType.DMA((16,)),
            ],
            compiler_params=pltpu.CompilerParams(
                collective_id=0, has_side_effects=True, vmem_limit_bytes=40 * 1024 * 1024
            ),
            name="step",
        )(
            positions,
            tokens,
            state,
            norm_gain.reshape(1, width),
            w_query,
            w_key,
            w_value,
            w_gate,
            w_out,
            mlp_gain.reshape(1, width),
            w_up,
            w_down,
            freq,
        )

    return jax.shard_map(
        shards,
        mesh=mesh,
        in_specs=(
            P("grp", "kv"),
            P(("grp", "kv")),
            P(("grp", "kv"), "tp", None, None),
            P("kv"),
            P("kv", "tp"),
            P("kv", "tp"),
            P("kv", "tp"),
            P("kv", "tp"),
            P("tp", "kv"),
            P("kv"),
            P("kv", "tp"),
            P("tp", "kv"),
        ),
        out_specs=(P("grp", "kv"), P(("grp", "kv"), "tp", None, None)),
        check_vma=False,
    )
```

```python
import functools

import jax
import jax.numpy as jnp
import numpy as np
from jax import lax
from jax.experimental import pallas as pl
from jax.experimental.pallas import tpu as pltpu
from jax.sharding import PartitionSpec as P

MESH = pl.DeviceIdType.MESH
F32 = jnp.float32
BF16 = jnp.bfloat16
EPS = 1e-06


def far_first(step, count):
    swing = (step + 1) // 2
    return count // 2 + swing * (2 * (step % 2) - 1)


def kernel(
    cfg,
    pos_ref,
    x_hbm,
    state_hbm,
    gain_hbm,
    wq_hbm,
    wk_hbm,
    wv_hbm,
    wg_hbm,
    wo_hbm,
    gain2_hbm,
    wu_hbm,
    wd_hbm,
    freq_ref,
    out_ref,
    state_out,
    x_in,
    gain_in,
    w_in,
    state_in,
    state_new,
    wo_in,
    wu_in,
    wd_in,
    tok2,
    gain2,
    part,
    swap_s,
    swap_r,
    sq_s,
    sq_r,
    send_a,
    recv_a,
    ret_s,
    ret_r,
    ret_f,
    send_c,
    recv_c,
    tok_rows,
    mix_s,
    mix_r,
    sq2_s,
    sq2_r,
    send_d,
    recv_d,
    hid_s,
    hid_r,
    out_s,
    out_r,
    load_sem,
    send_sem,
    recv_sem,
):
    nk, nt, nz, d_model, heads_all = cfg
    me = lax.axis_index("kv")
    tp = lax.axis_index("tp")
    z = me // 2
    c = me % 2
    mate = me + 1 - 2 * c
    block = tp * 2 + c
    nb = nt * 2
    rows = x_in.shape[0]
    width = x_in.shape[1]
    seqs = rows // nk
    per_chip = rows // nz
    size = width
    half_ff = wu_in.shape[1]

    def kv_peer(step):
        chip = lax.rem(z + far_first(step // 2, nz), nz)
        other = lax.rem(c + step % 2, 2)
        last = (step == nk - 2).astype(jnp.int32)
        return last * mate + (1 - last) * (chip * 2 + other)

    def chip_peer(step):
        return lax.rem(z + far_first(step, nz), nz) * 2 + c

    def block_peer(step):
        chip = lax.rem(tp + far_first(step // 2, nt), nt)
        other = lax.rem(c + step % 2, 2)
        last = (step == nb - 2).astype(jnp.int32)
        return last * tp + (1 - last) * chip, last * (1 - c) + (1 - last) * other

    def each(count, body):
        lax.fori_loop(0, count, lambda i, carry: (body(i), carry)[1], 0)

    barrier = pltpu.get_barrier_semaphore()

    def greet_kv(i):
        pl.semaphore_signal(barrier, inc=1, device_id={"kv": kv_peer(i)}, device_id_type=MESH)

    def greet_block(i):
        t, core = block_peer(i)
        pl.semaphore_signal(
            barrier, inc=1, device_id={"kv": z * 2 + core, "tp": t}, device_id_type=MESH
        )

    each(nk - 1, greet_kv)
    each(nb - 2, greet_block)

    def load(src, dst, sem):
        copy = pltpu.make_async_copy(src, dst, load_sem.at[sem])
        copy.start()
        return copy

    first = [
        load(x_hbm, x_in, 0),
        load(gain_hbm, gain_in, 1),
        load(wq_hbm, w_in.at[0], 2),
        load(wk_hbm, w_in.at[1], 3),
        load(wv_hbm, w_in.at[2], 4),
        load(wg_hbm, w_in.at[3], 5),
    ]
    here = pl.ds(pl.multiple_of(c * half_ff, 128), half_ff)
    there = pl.ds(pl.multiple_of((1 - c) * half_ff, 128), half_ff)
    mine = pl.ds(pl.multiple_of(c * size, 128), size)
    other_head = pl.ds(pl.multiple_of((1 - c) * size, 128), size)
    my_rows = pl.ds(pl.multiple_of(c * width, 128), width)
    later = [
        load(state_hbm, state_in, 6),
        load(wo_hbm.at[mine], wo_in.at[:, my_rows], 7),
        load(gain2_hbm, gain2.at[:, my_rows], 8),
        load(wu_hbm.at[:, here], wu_in.at[my_rows], 9),
        load(wd_hbm.at[here], wd_in.at[:, my_rows], 10),
    ]

    for copy in first:
        copy.wait()
    x = x_in[...].astype(F32)
    normed = (x * gain_in[...]).astype(BF16)
    square = x * x
    sq_s[...] = jnp.sum(jnp.transpose(square), axis=0, keepdims=True)
    sq_r[me] = sq_s[...]
    for n in range(4):
        both = jnp.dot(normed, w_in[n], preferred_element_type=F32)
        part[0, :, n * size : (n + 1) * size] = both[:, :size]
        part[1, :, n * size : (n + 1) * size] = both[:, size:]
    swap_s[...] = part[1 - c].astype(BF16)
    tok2[c] = x_in[...]

    pl.semaphore_wait(barrier, nk - 1 + nb - 2)

    going, coming = {}, {}

    def remote(src, dst, phase, kv, t=None):
        where = {"kv": kv} if t is None else {"kv": kv, "tp": t}
        pltpu.make_async_remote_copy(
            src_ref=src,
            dst_ref=dst,
            send_sem=send_sem.at[phase],
            recv_sem=recv_sem.at[phase],
            device_id=where,
            device_id_type=MESH,
        ).start()

    def to_mate(src, dst, phase, amount):
        remote(src, dst, phase, mate)
        going[phase] = coming[phase] = amount

    def to_each(count, phase, amount, send):
        each(count, send)
        going[phase] = coming[phase] = amount.at[pl.ds(0, count)]

    def arrived(phase):
        ref = coming.pop(phase)
        pltpu.make_async_copy(ref, ref, recv_sem.at[phase]).wait()

    def finish():
        for phase in list(coming):
            arrived(phase)
        for phase, ref in going.items():
            pltpu.make_async_copy(ref, ref, send_sem.at[phase]).wait()

    to_mate(swap_s, swap_r, 0, swap_r)

    def send_squares(i):
        remote(sq_s, sq_r.at[me], 1, kv_peer(i))

    to_each(nk - 1, 1, sq_r, send_squares)
    to_mate(x_in, tok2.at[c], 2, x_in)
    to_mate(gain2_hbm, gain2.at[:, my_rows], 3, gain_in)
    to_mate(wo_hbm.at[other_head], wo_in.at[:, my_rows], 4, x_in)
    to_mate(wu_hbm.at[:, there], wu_in.at[my_rows], 5, wu_in.at[pl.ds(0, width)])
    to_mate(wd_hbm.at[there], wd_in.at[:, my_rows], 6, wd_in.at[:, pl.ds(0, width)])

    arrived(0)
    part[c] = part[c] + swap_r[...].astype(F32)
    for j in range(nk):
        send_a[j] = part[c, j * seqs : (j + 1) * seqs, :].astype(BF16)
    recv_a[me] = send_a[me]

    def send_terms(i):
        peer = kv_peer(i)
        remote(send_a.at[peer], recv_a.at[me], 7, peer)

    to_each(nk - 1, 7, recv_a, send_terms)

    row = lax.broadcasted_iota(jnp.int32, (seqs, size), 0)
    lane = lax.broadcasted_iota(jnp.int32, (seqs, size), 1)
    place = jnp.zeros((seqs, size), F32)
    for i in range(seqs):
        place = jnp.where(row == i, pos_ref[i].astype(F32), place)
    angle = place * freq_ref[...]
    cosine = jnp.cos(angle)
    sine = jnp.sin(angle)
    sine = jnp.where(lane < size // 2, -sine, sine)
    later[0].wait()

    arrived(1)
    total_sq = jnp.sum(sq_r[...], axis=0)
    row_sq = jnp.sum(jnp.where(lane == row + me * seqs, total_sq, 0.0), axis=1, keepdims=True)
    scale1 = lax.rsqrt(row_sq / d_model + EPS)

    arrived(7)
    queries, keys, values, gates = [], [], [], []

    def turn(v):
        return v * cosine + pltpu.roll(v, size // 2, 1) * sine

    for h in range(2):
        total = recv_a[h].astype(F32)
        for j in range(1, nz):
            total = total + recv_a[2 * j + h].astype(F32)
        total = total * scale1
        queries.append(turn(total[:, :size]))
        keys.append(turn(total[:, size : 2 * size]) * size**-0.5)
        values.append(total[:, 2 * size : 3 * size])
        gates.append(total[:, 3 * size :])
    pad = jnp.zeros((size - 4 * seqs, size), F32)
    columns = jnp.transpose(jnp.concatenate(queries + keys + [pad], axis=0))
    for h in range(2):
        head = (tp * 2 + h).astype(F32)
        power = jnp.full((1, size), -5.0, F32) - 5.0 * head / (heads_all - 1)
        gamma = 1.0 - jnp.exp2(power)
        reads = []
        for i in range(seqs):
            at = h * seqs + i
            new = (
                gamma * state_in[i, h]
                + columns[:, 2 * seqs + at : 2 * seqs + at + 1] * values[h][i : i + 1]
            )
            state_new[i, h] = new
            reads.append(jnp.sum(columns[:, at : at + 1] * new, axis=0, keepdims=True))
        read = jnp.concatenate(reads, axis=0)
        read = read * lax.rsqrt(jnp.mean(read * read, axis=1, keepdims=True) + EPS)
        gate = gates[h]
        ret_s[h] = (read * (gate / (1.0 + jnp.exp(-gate)))).astype(BF16)
    ret_r[me] = ret_s[c]

    def send_retained(i):
        peer = kv_peer(i)
        remote(ret_s.at[peer % 2], ret_r.at[me], 8, peer)

    to_each(nk - 1, 8, ret_r, send_retained)
    state_copy = load(state_new, state_out, 11)

    later[1].wait()
    later[2].wait()
    arrived(2)
    arrived(3)
    arrived(4)
    for m in range(nb):
        for s in range(2):
            tok_rows[m, :, s * width : (s + 1) * width] = tok2[
                s, m * per_chip : (m + 1) * per_chip
            ].astype(F32)

    arrived(8)
    for j in range(nk):
        ret_f[j * seqs : (j + 1) * seqs] = ret_r[j].astype(F32)
    terms = jnp.dot(ret_f[...].astype(BF16), wo_in[...], preferred_element_type=F32)
    send_c[0] = terms.reshape(nb, per_chip, 2 * width).astype(BF16)
    recv_c[0, block] = send_c[0, block]

    def send_sums(which, phase):
        def send(i):
            t, core = block_peer(i)
            remote(send_c.at[which, t * 2 + core], recv_c.at[which, block], phase, z * 2 + core, t)

        to_each(nb - 1, phase, recv_c.at[which], send)

    send_sums(0, 9)
    arrived(9)
    mixed = (tok_rows[block] + jnp.sum(recv_c[0].astype(F32), axis=0)).astype(BF16)
    mix_s[...] = mixed
    mix_r[block] = mixed

    def send_mixed(i):
        t, core = block_peer(i)
        remote(mix_s, mix_r.at[block], 10, z * 2 + core, t)

    to_each(nb - 1, 10, mix_r, send_mixed)
    later[3].wait()
    arrived(5)
    arrived(10)
    middle = mix_r[...].astype(F32).reshape(rows, 2 * width)
    square = middle * middle
    sq2_s[...] = jnp.sum(
        jnp.transpose(square[:, :width] + square[:, width:]), axis=0, keepdims=True
    )
    sq2_r[z] = sq2_s[...]

    def send_squares2(i):
        remote(sq2_s, sq2_r.at[z], 11, chip_peer(i))

    to_each(nz - 1, 11, sq2_r, send_squares2)
    normed2 = (middle * gain2[...]).astype(BF16)
    upward = jnp.dot(normed2, wu_in[...], preferred_element_type=F32)
    send_d[...] = upward.reshape(nz, per_chip, half_ff).astype(BF16)
    recv_d[z] = send_d[z]

    def send_up(i):
        peer = chip_peer(i)
        remote(send_d.at[peer // 2], recv_d.at[z], 12, peer)

    to_each(nz - 1, 12, recv_d, send_up)
    row = lax.broadcasted_iota(jnp.int32, (per_chip, size), 0)
    lane = lax.broadcasted_iota(jnp.int32, (per_chip, size), 1)
    arrived(11)
    total_sq = jnp.sum(sq2_r[...], axis=0)
    row_sq = jnp.sum(jnp.where(lane == row + z * per_chip, total_sq, 0.0), axis=1, keepdims=True)
    scale2 = lax.rsqrt(row_sq / d_model + EPS)
    arrived(12)
    total = recv_d[0].astype(F32)
    for j in range(1, nz):
        total = total + recv_d[j].astype(F32)
    hidden = jnp.maximum(total * scale2, 0.0)
    hid_s[...] = (hidden * hidden).astype(BF16)
    hid_r[z] = hid_s[...]

    def send_hidden(i):
        remote(hid_s, hid_r.at[z], 13, chip_peer(i))

    to_each(nz - 1, 13, hid_r, send_hidden)
    later[4].wait()
    arrived(6)
    arrived(13)
    hidden_all = hid_r[...].astype(F32).reshape(rows, half_ff).astype(BF16)
    terms = jnp.dot(hidden_all, wd_in[...], preferred_element_type=F32)
    send_c[1] = terms.reshape(nb, per_chip, 2 * width).astype(BF16)
    recv_c[1, block] = send_c[1, block]
    send_sums(1, 14)
    arrived(14)
    final = (mix_s[...].astype(F32) + jnp.sum(recv_c[1].astype(F32), axis=0)).astype(BF16)
    for s in range(2):
        out_s[s] = final[:, s * width : (s + 1) * width]
    out_r[block] = out_s[c]

    def send_out(i):
        t, core = block_peer(i)
        remote(out_s.at[core], out_r.at[block], 15, z * 2 + core, t)

    to_each(nb - 1, 15, out_r, send_out)

    state_copy.wait()
    finish()
    out_ref[...] = out_r[...].astype(F32).reshape(rows, width).astype(BF16)


def solution(mesh):
    nk, nt = mesh.shape["kv"], mesh.shape["tp"]
    nz = nk // 2

    def shards(
        tokens,
        positions,
        state,
        norm_gain,
        w_query,
        w_key,
        w_value,
        w_gate,
        w_out,
        mlp_gain,
        w_up,
        w_down,
    ):
        rows, width = tokens.shape
        seqs, heads, size, _ = state.shape
        ff = w_up.shape[1]
        per_chip = rows // nz
        nb = 2 * nt
        inverse = 10000.0 ** (-(np.arange(size // 2, dtype=np.float64) * 2.0) / size)
        freq = jnp.asarray(np.concatenate([inverse, inverse])[None, :].astype(np.float32))
        cfg = (nk, nt, nz, width * nk, heads * nt)
        anywhere = pl.BlockSpec(memory_space=pltpu.HBM)
        vmem = pl.BlockSpec(memory_space=pltpu.VMEM)
        smem = pl.BlockSpec(memory_space=pltpu.SMEM)
        scratch = [
            ((rows, width), BF16),
            ((1, width), F32),
            ((4, width, heads * size), BF16),
            (state.shape, F32),
            (state.shape, F32),
            ((size, 2 * width), BF16),
            ((2 * width, ff // 2), BF16),
            ((ff // 2, 2 * width), BF16),
            ((2, rows, width), BF16),
            ((1, 2 * width), F32),
            ((2, rows, 4 * size), F32),
            ((rows, 4 * size), BF16),
            ((rows, 4 * size), BF16),
            ((1, rows), F32),
            ((nk, 1, rows), F32),
            ((nk, seqs, 4 * size), BF16),
            ((nk, seqs, 4 * size), BF16),
            ((2, seqs, size), BF16),
            ((nk, seqs, size), BF16),
            ((rows, size), F32),
            ((2, nb, per_chip, 2 * width), BF16),
            ((2, nb, per_chip, 2 * width), BF16),
            ((nb, per_chip, 2 * width), F32),
            ((per_chip, 2 * width), BF16),
            ((nb, per_chip, 2 * width), BF16),
            ((1, rows), F32),
            ((nz, 1, rows), F32),
            ((nz, per_chip, ff // 2), BF16),
            ((nz, per_chip, ff // 2), BF16),
            ((per_chip, ff // 2), BF16),
            ((nz, per_chip, ff // 2), BF16),
            ((2, per_chip, width), BF16),
            ((nb, per_chip, width), BF16),
        ]
        return pl.pallas_call(
            functools.partial(kernel, cfg),
            out_shape=(
                jax.ShapeDtypeStruct((rows, width), BF16),
                jax.ShapeDtypeStruct(state.shape, F32),
            ),
            in_specs=[smem] + [anywhere] * 11 + [vmem],
            out_specs=(vmem, anywhere),
            scratch_shapes=[pltpu.VMEM(s, t) for s, t in scratch]
            + [
                pltpu.SemaphoreType.DMA((12,)),
                pltpu.SemaphoreType.DMA((16,)),
                pltpu.SemaphoreType.DMA((16,)),
            ],
            compiler_params=pltpu.CompilerParams(
                collective_id=0, has_side_effects=True
            ),
            name="step",
        )(
            positions,
            tokens,
            state,
            norm_gain.reshape(1, width),
            w_query,
            w_key,
            w_value,
            w_gate,
            w_out,
            mlp_gain.reshape(1, width),
            w_up,
            w_down,
            freq,
        )

    return jax.shard_map(
        shards,
        mesh=mesh,
        in_specs=(
            P("grp", "kv"),
            P(("grp", "kv")),
            P(("grp", "kv"), "tp", None, None),
            P("kv"),
            P("kv", "tp"),
            P("kv", "tp"),
            P("kv", "tp"),
            P("kv", "tp"),
            P("tp", "kv"),
            P("kv"),
            P("kv", "tp"),
            P("tp", "kv"),
        ),
        out_specs=(P("grp", "kv"), P(("grp", "kv"), "tp", None, None)),
        check_vma=False,
    )
```

```python
import functools

import jax
import jax.numpy as jnp
import numpy as np
from jax import lax
from jax.experimental import pallas as pl
from jax.experimental.pallas import tpu as pltpu
from jax.sharding import PartitionSpec as P

MESH = pl.DeviceIdType.MESH
F32 = jnp.float32
BF16 = jnp.bfloat16
EPS = 1e-06


def far_first(step, count):
    swing = (step + 1) // 2
    return count // 2 + swing * (2 * (step % 2) - 1)


def kernel(
    cfg,
    pos_hbm,
    x_hbm,
    state_hbm,
    gain_hbm,
    wq_hbm,
    wk_hbm,
    wv_hbm,
    wg_hbm,
    wo_hbm,
    gain2_hbm,
    wu_hbm,
    wd_hbm,
    freq_hbm,
    out_ref,
    state_out,
    pos_ref,
    freq_ref,
    x_in,
    gain_in,
    w_in,
    state_in,
    state_new,
    wo_in,
    wu_in,
    wd_in,
    tok2,
    gain2,
    part,
    swap_s,
    swap_r,
    sq_s,
    sq_r,
    send_a,
    recv_a,
    ret_s,
    ret_r,
    ret_f,
    send_c,
    recv_c,
    tok_rows,
    mix_s,
    mix_r,
    sq2_s,
    sq2_r,
    send_d,
    near_d,
    relay_d,
    recv_d,
    hid_s,
    hid_r,
    out_s,
    out_r,
    load_sem,
    send_sem,
    recv_sem,
    near_sem,
    far_sem,
):
    nk, nt, nz, d_model, heads_all, relayed = cfg
    me = lax.axis_index("kv")
    tp = lax.axis_index("tp")
    z = me // 2
    c = me % 2
    mate = me + 1 - 2 * c
    block = tp * 2 + c
    nb = nt * 2
    rows = x_in.shape[0]
    width = x_in.shape[1]
    seqs = rows // nk
    per_chip = rows // nz
    size = width
    half_ff = wu_in.shape[1]
    nr = near_d.shape[0]

    def kv_peer(step):
        chip = lax.rem(z + far_first(step // 2, nz), nz)
        other = lax.rem(c + step % 2, 2)
        last = (step == nk - 2).astype(jnp.int32)
        return last * mate + (1 - last) * (chip * 2 + other)

    def chip_peer(step):
        return lax.rem(z + far_first(step, nz), nz) * 2 + c

    def block_peer(step):
        chip = lax.rem(tp + far_first(step // 2, nt), nt)
        other = lax.rem(c + step % 2, 2)
        last = (step == nb - 2).astype(jnp.int32)
        return last * tp + (1 - last) * chip, last * (1 - c) + (1 - last) * other

    def each(count, body):
        lax.fori_loop(0, count, lambda i, carry: (body(i), carry)[1], 0)

    barrier = pltpu.get_barrier_semaphore()

    def greet_kv(i):
        pl.semaphore_signal(barrier, inc=1, device_id={"kv": kv_peer(i)}, device_id_type=MESH)

    def greet_block(i):
        t, core = block_peer(i)
        pl.semaphore_signal(
            barrier, inc=1, device_id={"kv": z * 2 + core, "tp": t}, device_id_type=MESH
        )

    def load(src, dst, sem):
        copy = pltpu.make_async_copy(src, dst, load_sem.at[sem])
        copy.start()
        return copy

    first = [
        load(x_hbm, x_in, 0),
        load(gain_hbm, gain_in, 1),
        load(wq_hbm, w_in.at[0], 2),
        load(wk_hbm, w_in.at[1], 3),
        load(wv_hbm, w_in.at[2], 4),
        load(wg_hbm, w_in.at[3], 5),
        load(pos_hbm, pos_ref, 12),
        load(freq_hbm, freq_ref, 13),
    ]
    each(nk - 1, greet_kv)
    each(nb - 2, greet_block)

    here = pl.ds(pl.multiple_of(c * half_ff, 128), half_ff)
    there = pl.ds(pl.multiple_of((1 - c) * half_ff, 128), half_ff)
    mine = pl.ds(pl.multiple_of(c * size, 128), size)
    other_head = pl.ds(pl.multiple_of((1 - c) * size, 128), size)
    my_rows = pl.ds(pl.multiple_of(c * width, 128), width)
    later = [
        load(state_hbm, state_in, 6),
        load(wo_hbm.at[mine], wo_in.at[:, my_rows], 7),
        load(gain2_hbm, gain2.at[:, my_rows], 8),
        load(wu_hbm.at[:, here], wu_in.at[my_rows], 9),
        load(wd_hbm.at[here], wd_in.at[:, my_rows], 10),
    ]

    for copy in first:
        copy.wait()
    x = x_in[...].astype(F32)
    normed = (x * gain_in[...]).astype(BF16)
    square = x * x
    sq_s[...] = jnp.sum(jnp.transpose(square), axis=0, keepdims=True)
    sq_r[me] = sq_s[...]
    for n in range(4):
        both = jnp.dot(normed, w_in[n], preferred_element_type=F32)
        part[0, :, n * size : (n + 1) * size] = both[:, :size]
        part[1, :, n * size : (n + 1) * size] = both[:, size:]
    swap_s[...] = part[1 - c].astype(BF16)
    tok2[c] = x_in[...]

    pl.semaphore_wait(barrier, nk - 1 + nb - 2)

    going, coming = {}, {}

    def remote(src, dst, phase, kv, t=None):
        where = {"kv": kv} if t is None else {"kv": kv, "tp": t}
        pltpu.make_async_remote_copy(
            src_ref=src,
            dst_ref=dst,
            send_sem=send_sem.at[phase],
            recv_sem=recv_sem.at[phase],
            device_id=where,
            device_id_type=MESH,
        ).start()

    def to_mate(src, dst, phase, amount):
        remote(src, dst, phase, mate)
        going[phase] = coming[phase] = amount

    def to_each(count, phase, amount, send):
        each(count, send)
        going[phase] = coming[phase] = amount.at[pl.ds(0, count)]

    def arrived(phase):
        ref = coming.pop(phase)
        pltpu.make_async_copy(ref, ref, recv_sem.at[phase]).wait()

    def finish():
        for phase in list(coming):
            arrived(phase)
        for phase, ref in going.items():
            pltpu.make_async_copy(ref, ref, send_sem.at[phase]).wait()

    to_mate(swap_s, swap_r, 0, swap_r)

    def send_squares(i):
        remote(sq_s, sq_r.at[me], 1, kv_peer(i))

    to_each(nk - 1, 1, sq_r, send_squares)
    to_mate(x_in, tok2.at[c], 2, x_in)
    to_mate(gain2_hbm, gain2.at[:, my_rows], 3, gain_in)
    to_mate(wo_hbm.at[other_head], wo_in.at[:, my_rows], 4, x_in)
    to_mate(wu_hbm.at[:, there], wu_in.at[my_rows], 5, wu_in.at[pl.ds(0, width)])
    to_mate(wd_hbm.at[there], wd_in.at[:, my_rows], 6, wd_in.at[:, pl.ds(0, width)])

    arrived(0)
    part[c] = part[c] + swap_r[...].astype(F32)
    for j in range(nk):
        send_a[j] = part[c, j * seqs : (j + 1) * seqs, :].astype(BF16)
    recv_a[me] = send_a[me]

    def send_terms(i):
        peer = kv_peer(i)
        remote(send_a.at[peer], recv_a.at[me], 7, peer)

    to_each(nk - 1, 7, recv_a, send_terms)

    row = lax.broadcasted_iota(jnp.int32, (seqs, size), 0)
    lane = lax.broadcasted_iota(jnp.int32, (seqs, size), 1)
    place = jnp.zeros((seqs, size), F32)
    for i in range(seqs):
        place = jnp.where(row == i, pos_ref[i].astype(F32), place)
    angle = place * freq_ref[...]
    cosine = jnp.cos(angle)
    sine = jnp.sin(angle)
    sine = jnp.where(lane < size // 2, -sine, sine)
    later[0].wait()

    arrived(1)
    total_sq = jnp.sum(sq_r[...], axis=0)
    row_sq = jnp.sum(jnp.where(lane == row + me * seqs, total_sq, 0.0), axis=1, keepdims=True)
    scale1 = lax.rsqrt(row_sq / d_model + EPS)

    arrived(7)
    queries, keys, values, gates = [], [], [], []

    def turn(v):
        return v * cosine + pltpu.roll(v, size // 2, 1) * sine

    for h in range(2):
        total = recv_a[h].astype(F32)
        for j in range(1, nz):
            total = total + recv_a[2 * j + h].astype(F32)
        total = total * scale1
        queries.append(turn(total[:, :size]))
        keys.append(turn(total[:, size : 2 * size]) * size**-0.5)
        values.append(total[:, 2 * size : 3 * size])
        gates.append(total[:, 3 * size :])
    pad = jnp.zeros((size - 4 * seqs, size), F32)
    columns = jnp.transpose(jnp.concatenate(queries + keys + [pad], axis=0))
    for h in range(2):
        head = (tp * 2 + h).astype(F32)
        power = jnp.full((1, size), -5.0, F32) - 5.0 * head / (heads_all - 1)
        gamma = 1.0 - jnp.exp2(power)
        reads = []
        for i in range(seqs):
            at = h * seqs + i
            new = (
                gamma * state_in[i, h]
                + columns[:, 2 * seqs + at : 2 * seqs + at + 1] * values[h][i : i + 1]
            )
            state_new[i, h] = new
            reads.append(jnp.sum(columns[:, at : at + 1] * new, axis=0, keepdims=True))
        read = jnp.concatenate(reads, axis=0)
        read = read * lax.rsqrt(jnp.mean(read * read, axis=1, keepdims=True) + EPS)
        gate = gates[h]
        ret_s[h] = (read * (gate / (1.0 + jnp.exp(-gate)))).astype(BF16)
    ret_r[me] = ret_s[c]

    def send_retained(i):
        peer = kv_peer(i)
        remote(ret_s.at[peer % 2], ret_r.at[me], 8, peer)

    to_each(nk - 1, 8, ret_r, send_retained)
    state_copy = load(state_new, state_out, 11)

    later[1].wait()
    later[2].wait()
    arrived(2)
    arrived(3)
    arrived(4)
    for m in range(nb):
        for s in range(2):
            tok_rows[m, :, s * width : (s + 1) * width] = tok2[
                s, m * per_chip : (m + 1) * per_chip
            ].astype(F32)

    arrived(8)
    for j in range(nk):
        ret_f[j * seqs : (j + 1) * seqs] = ret_r[j].astype(F32)
    terms = jnp.dot(ret_f[...].astype(BF16), wo_in[...], preferred_element_type=F32)
    send_c[0] = terms.reshape(nb, per_chip, 2 * width).astype(BF16)
    recv_c[0, block] = send_c[0, block]

    def send_sums(which, phase):
        def send(i):
            t, core = block_peer(i)
            remote(send_c.at[which, t * 2 + core], recv_c.at[which, block], phase, z * 2 + core, t)

        to_each(nb - 1, phase, recv_c.at[which], send)

    send_sums(0, 9)
    arrived(9)
    mixed = (tok_rows[block] + jnp.sum(recv_c[0].astype(F32), axis=0)).astype(BF16)
    mix_s[...] = mixed
    mix_r[block] = mixed

    def send_mixed(i):
        t, core = block_peer(i)
        remote(mix_s, mix_r.at[block], 10, z * 2 + core, t)

    to_each(nb - 1, 10, mix_r, send_mixed)
    later[3].wait()
    arrived(5)
    arrived(10)
    middle = mix_r[...].astype(F32).reshape(rows, 2 * width)
    square = middle * middle
    sq2_s[...] = jnp.sum(
        jnp.transpose(square[:, :width] + square[:, width:]), axis=0, keepdims=True
    )
    sq2_r[z] = sq2_s[...]

    def send_squares2(i):
        remote(sq2_s, sq2_r.at[z], 11, chip_peer(i))

    to_each(nz - 1, 11, sq2_r, send_squares2)
    normed2 = (middle * gain2[...]).astype(BF16)
    upward = jnp.dot(normed2, wu_in[...], preferred_element_type=F32)
    send_d[...] = upward.reshape(nz, per_chip, half_ff).astype(BF16)

    def round_z(chip):
        return chip - nz * (chip >= nz).astype(jnp.int32)

    right, left = round_z(z + 1), round_z(z + nz - 1)

    def near(src, dst, chip, at):
        pltpu.make_async_remote_copy(
            src_ref=src,
            dst_ref=dst,
            send_sem=send_sem.at[12],
            recv_sem=near_sem.at[at],
            device_id={"kv": chip * 2 + c},
            device_id_type=MESH,
        ).start()

    def far(src, dst, chip, phase, at):
        pltpu.make_async_remote_copy(
            src_ref=src,
            dst_ref=dst,
            send_sem=send_sem.at[phase],
            recv_sem=far_sem.at[at],
            device_id={"kv": chip * 2 + c},
            device_id_type=MESH,
        ).start()

    for k, offset in enumerate(relayed):
        near(send_d.at[round_z(right + offset)], near_d.at[k, 0], right, k)
        near(send_d.at[round_z(left + offset)], near_d.at[k, 1], left, k)
    going[12] = send_d.at[pl.ds(0, 2 * nr)]
    for k, offset in enumerate(relayed):
        target = round_z(z + offset)
        pltpu.make_async_copy(near_d.at[k], near_d.at[k], near_sem.at[k]).wait()
        relay_d[k] = (
            send_d[target].astype(F32) + near_d[k, 0].astype(F32) + near_d[k, 1].astype(F32)
        ).astype(BF16)
        far(relay_d.at[k], recv_d.at[k], target, 16, 0)
    going[16] = relay_d
    row = lax.broadcasted_iota(jnp.int32, (per_chip, size), 0)
    lane = lax.broadcasted_iota(jnp.int32, (per_chip, size), 1)
    arrived(11)
    total_sq = jnp.sum(sq2_r[...], axis=0)
    row_sq = jnp.sum(jnp.where(lane == row + z * per_chip, total_sq, 0.0), axis=1, keepdims=True)
    scale2 = lax.rsqrt(row_sq / d_model + EPS)
    pltpu.make_async_copy(recv_d, recv_d, far_sem.at[0]).wait()
    total = send_d[z].astype(F32)
    for k in range(nr):
        total = total + recv_d[k].astype(F32)
    hidden = jnp.maximum(total * scale2, 0.0)
    hid_s[...] = (hidden * hidden).astype(BF16)
    hid_r[z] = hid_s[...]

    for k, offset in enumerate(relayed):
        far(hid_s, hid_r.at[z], round_z(z + offset), 13, k + 1)
    going[13] = hid_r.at[pl.ds(0, nr)]
    for k in reversed(range(nr)):
        source = round_z(z + nz - relayed[k])
        pltpu.make_async_copy(hid_r.at[source], hid_r.at[source], far_sem.at[k + 1]).wait()
        for chip in (right, left):
            remote(hid_r.at[source], hid_r.at[source], 17, chip * 2 + c)
    going[17] = coming[17] = hid_r.at[pl.ds(0, 2 * nr)]
    later[4].wait()
    arrived(6)
    arrived(17)
    hidden_all = hid_r[...].astype(F32).reshape(rows, half_ff).astype(BF16)
    terms = jnp.dot(hidden_all, wd_in[...], preferred_element_type=F32)
    send_c[1] = terms.reshape(nb, per_chip, 2 * width).astype(BF16)
    recv_c[1, block] = send_c[1, block]
    send_sums(1, 14)
    arrived(14)
    final = (mix_s[...].astype(F32) + jnp.sum(recv_c[1].astype(F32), axis=0)).astype(BF16)
    for s in range(2):
        out_s[s] = final[:, s * width : (s + 1) * width]
    out_r[block] = out_s[c]

    def send_out(i):
        t, core = block_peer(i)
        remote(out_s.at[core], out_r.at[block], 15, z * 2 + core, t)

    to_each(nb - 1, 15, out_r, send_out)

    state_copy.wait()
    finish()
    out_ref[...] = out_r[...].astype(F32).reshape(rows, width).astype(BF16)


def solution(mesh):
    nk, nt = mesh.shape["kv"], mesh.shape["tp"]
    nz = nk // 2

    def shards(
        tokens,
        positions,
        state,
        norm_gain,
        w_query,
        w_key,
        w_value,
        w_gate,
        w_out,
        mlp_gain,
        w_up,
        w_down,
    ):
        rows, width = tokens.shape
        seqs, heads, size, _ = state.shape
        ff = w_up.shape[1]
        per_chip = rows // nz
        nb = 2 * nt
        inverse = 10000.0 ** (-(np.arange(size // 2, dtype=np.float64) * 2.0) / size)
        freq = jnp.asarray(np.concatenate([inverse, inverse])[None, :].astype(np.float32))
        anywhere = pl.BlockSpec(memory_space=pltpu.HBM)
        vmem = pl.BlockSpec(memory_space=pltpu.VMEM)
        relayed = (8, 5, 11, 2, 14)
        nr = len(relayed)
        cfg = (nk, nt, nz, width * nk, heads * nt, relayed)
        scratch = [
            ((1, size), F32),
            ((rows, width), BF16),
            ((1, width), F32),
            ((4, width, heads * size), BF16),
            (state.shape, F32),
            (state.shape, F32),
            ((size, 2 * width), BF16),
            ((2 * width, ff // 2), BF16),
            ((ff // 2, 2 * width), BF16),
            ((2, rows, width), BF16),
            ((1, 2 * width), F32),
            ((2, rows, 4 * size), F32),
            ((rows, 4 * size), BF16),
            ((rows, 4 * size), BF16),
            ((1, rows), F32),
            ((nk, 1, rows), F32),
            ((nk, seqs, 4 * size), BF16),
            ((nk, seqs, 4 * size), BF16),
            ((2, seqs, size), BF16),
            ((nk, seqs, size), BF16),
            ((rows, size), F32),
            ((2, nb, per_chip, 2 * width), BF16),
            ((2, nb, per_chip, 2 * width), BF16),
            ((nb, per_chip, 2 * width), F32),
            ((per_chip, 2 * width), BF16),
            ((nb, per_chip, 2 * width), BF16),
            ((1, rows), F32),
            ((nz, 1, rows), F32),
            ((nz, per_chip, ff // 2), BF16),
            ((nr, 2, per_chip, ff // 2), BF16),
            ((nr, per_chip, ff // 2), BF16),
            ((nr, per_chip, ff // 2), BF16),
            ((per_chip, ff // 2), BF16),
            ((nz, per_chip, ff // 2), BF16),
            ((2, per_chip, width), BF16),
            ((nb, per_chip, width), BF16),
        ]
        return pl.pallas_call(
            functools.partial(kernel, cfg),
            out_shape=(
                jax.ShapeDtypeStruct((rows, width), BF16),
                jax.ShapeDtypeStruct(state.shape, F32),
            ),
            in_specs=[anywhere] * 13,
            out_specs=(vmem, anywhere),
            scratch_shapes=[pltpu.SMEM((seqs,), jnp.int32)]
            + [pltpu.VMEM(s, t) for s, t in scratch]
            + [
                pltpu.SemaphoreType.DMA((14,)),
                pltpu.SemaphoreType.DMA((18,)),
                pltpu.SemaphoreType.DMA((18,)),
                pltpu.SemaphoreType.DMA((nr,)),
                pltpu.SemaphoreType.DMA((nr + 1,)),
            ],
            compiler_params=pltpu.CompilerParams(
                collective_id=0, has_side_effects=True
            ),
            name="step",
        )(
            positions,
            tokens,
            state,
            norm_gain.reshape(1, width),
            w_query,
            w_key,
            w_value,
            w_gate,
            w_out,
            mlp_gain.reshape(1, width),
            w_up,
            w_down,
            freq,
        )

    return jax.shard_map(
        shards,
        mesh=mesh,
        in_specs=(
            P("grp", "kv"),
            P(("grp", "kv")),
            P(("grp", "kv"), "tp", None, None),
            P("kv"),
            P("kv", "tp"),
            P("kv", "tp"),
            P("kv", "tp"),
            P("kv", "tp"),
            P("tp", "kv"),
            P("kv"),
            P("kv", "tp"),
            P("tp", "kv"),
        ),
        out_specs=(P("grp", "kv"), P(("grp", "kv"), "tp", None, None)),
        check_vma=False,
    )
```

```python
import functools

import jax
import jax.numpy as jnp
import numpy as np
from jax import lax
from jax.experimental import pallas as pl
from jax.experimental.pallas import tpu as pltpu
from jax.sharding import PartitionSpec as P

MESH = pl.DeviceIdType.MESH
F32 = jnp.float32
BF16 = jnp.bfloat16
EPS = 1e-06


def far_first(count):
    return sorted(range(1, count), key=lambda offset: -min(offset, count - offset))


def kernel(
    cfg,
    pos_hbm,
    x_hbm,
    state_hbm,
    gain_hbm,
    wq_hbm,
    wk_hbm,
    wv_hbm,
    wg_hbm,
    wo_hbm,
    gain2_hbm,
    wu_hbm,
    wd_hbm,
    freq_hbm,
    out_ref,
    state_out,
    pos_ref,
    freq_ref,
    x_in,
    gain_in,
    w_in,
    state_in,
    state_new,
    wo_in,
    wu_in,
    wd_in,
    tok2,
    gain2,
    part,
    swap_s,
    swap_r,
    sq_s,
    sq_m,
    sq_r,
    send_a,
    recv_a,
    ret_s,
    ret_r,
    ret_f,
    send_c,
    recv_c,
    tok_rows,
    mix_s,
    mix_r,
    sq2_s,
    sq2_r,
    send_d,
    near_d,
    relay_d,
    recv_d,
    hid_s,
    hid_r,
    out_s,
    out_r,
    load_sem,
    send_sem,
    recv_sem,
    near_sem,
    far_sem,
):
    nk, nt, nz, d_model, heads_all, relayed = cfg
    me = lax.axis_index("kv")
    tp = lax.axis_index("tp")
    z = me // 2
    c = me % 2
    mate = me + 1 - 2 * c
    block = tp * 2 + c
    nb = nt * 2
    rows = x_in.shape[0]
    width = x_in.shape[1]
    seqs = rows // nk
    per_chip = rows // nz
    size = width
    half_ff = wu_in.shape[1]
    nr = near_d.shape[0]

    def ring(at, count):
        return at - count * (at >= count).astype(jnp.int32)

    chips = [ring(z + offset, nz) for offset in far_first(nz)]
    columns_x = [ring(tp + offset, nt) for offset in far_first(nt)]
    kv_peers = [(chip * 2 + core, core) for chip in chips for core in range(2)] + [(mate, 1 - c)]
    block_peers = [(t, core) for t in columns_x for core in range(2)] + [(tp, 1 - c)]

    barrier = pltpu.get_barrier_semaphore()

    def load(src, dst, sem):
        copy = pltpu.make_async_copy(src, dst, load_sem.at[sem])
        copy.start()
        return copy

    first = [
        load(x_hbm, x_in, 0),
        load(gain_hbm, gain_in, 1),
        load(wq_hbm, w_in.at[0], 2),
        load(wk_hbm, w_in.at[1], 3),
        load(wv_hbm, w_in.at[2], 4),
        load(wg_hbm, w_in.at[3], 5),
        load(pos_hbm, pos_ref, 12),
        load(freq_hbm, freq_ref, 13),
    ]
    for peer, _ in kv_peers:
        pl.semaphore_signal(barrier, inc=1, device_id={"kv": peer}, device_id_type=MESH)
    for t, core in block_peers[:-1]:
        pl.semaphore_signal(
            barrier, inc=1, device_id={"kv": z * 2 + core, "tp": t}, device_id_type=MESH
        )

    here = pl.ds(pl.multiple_of(c * half_ff, 128), half_ff)
    there = pl.ds(pl.multiple_of((1 - c) * half_ff, 128), half_ff)
    mine = pl.ds(pl.multiple_of(c * size, 128), size)
    other_head = pl.ds(pl.multiple_of((1 - c) * size, 128), size)
    my_rows = pl.ds(pl.multiple_of(c * width, 128), width)
    later = [
        load(state_hbm, state_in, 6),
        load(wo_hbm.at[mine], wo_in.at[:, my_rows], 7),
        load(gain2_hbm, gain2.at[:, my_rows], 8),
        load(wu_hbm.at[:, here], wu_in.at[my_rows], 9),
        load(wd_hbm.at[here], wd_in.at[:, my_rows], 10),
    ]

    for copy in first:
        copy.wait()
    x = x_in[...].astype(F32)
    normed = (x * gain_in[...]).astype(BF16)
    square = x * x
    sq_s[...] = jnp.sum(jnp.transpose(square), axis=0, keepdims=True)
    for n in range(4):
        both = jnp.dot(normed, w_in[n], preferred_element_type=F32)
        part[0, :, n * size : (n + 1) * size] = both[:, :size]
        part[1, :, n * size : (n + 1) * size] = both[:, size:]
    swap_s[...] = part[1 - c].astype(BF16)
    tok2[c] = x_in[...]

    pl.semaphore_wait(barrier, nk - 1 + nb - 2)

    going, coming = {}, {}

    def remote(src, dst, phase, kv, t=None):
        where = {"kv": kv} if t is None else {"kv": kv, "tp": t}
        pltpu.make_async_remote_copy(
            src_ref=src,
            dst_ref=dst,
            send_sem=send_sem.at[phase],
            recv_sem=recv_sem.at[phase],
            device_id=where,
            device_id_type=MESH,
        ).start()

    def to_mate(src, dst, phase, amount):
        remote(src, dst, phase, mate)
        going[phase] = coming[phase] = amount

    def expect(count, phase, amount):
        going[phase] = coming[phase] = amount.at[pl.ds(0, count)]

    def arrived(phase):
        ref = coming.pop(phase)
        pltpu.make_async_copy(ref, ref, recv_sem.at[phase]).wait()

    def finish():
        for phase in list(coming):
            arrived(phase)
        for phase, ref in going.items():
            pltpu.make_async_copy(ref, ref, send_sem.at[phase]).wait()

    to_mate(swap_s, swap_r, 0, swap_r)

    to_mate(sq_s, sq_m, 18, sq_m)
    to_mate(x_in, tok2.at[c], 2, x_in)
    to_mate(gain2_hbm, gain2.at[:, my_rows], 3, gain_in)
    to_mate(wo_hbm.at[other_head], wo_in.at[:, my_rows], 4, x_in)
    to_mate(wu_hbm.at[:, there], wu_in.at[my_rows], 5, wu_in.at[pl.ds(0, width)])
    to_mate(wd_hbm.at[there], wd_in.at[:, my_rows], 6, wd_in.at[:, pl.ds(0, width)])

    arrived(18)
    sq_r[z] = sq_s[...] + sq_m[...]
    arrived(0)
    part[c] = part[c] + swap_r[...].astype(F32)
    for j in range(nk):
        send_a[j] = part[c, j * seqs : (j + 1) * seqs, :].astype(BF16)
    recv_a[me] = send_a[me]

    for chip in chips:
        for core in range(2):
            peer = chip * 2 + core
            remote(send_a.at[peer], recv_a.at[me], 7, peer)
        remote(sq_r.at[z], sq_r.at[z], 1, chip * 2 + c)
    remote(send_a.at[mate], recv_a.at[me], 7, mate)
    expect(nk - 1, 7, recv_a)
    expect(nz - 1, 1, sq_r)

    row = lax.broadcasted_iota(jnp.int32, (seqs, size), 0)
    lane = lax.broadcasted_iota(jnp.int32, (seqs, size), 1)
    place = jnp.zeros((seqs, size), F32)
    for i in range(seqs):
        place = jnp.where(row == i, pos_ref[i].astype(F32), place)
    angle = place * freq_ref[...]
    cosine = jnp.cos(angle)
    sine = jnp.sin(angle)
    sine = jnp.where(lane < size // 2, -sine, sine)
    later[0].wait()

    arrived(1)
    total_sq = jnp.sum(sq_r[...], axis=0)
    row_sq = jnp.sum(jnp.where(lane == row + me * seqs, total_sq, 0.0), axis=1, keepdims=True)
    scale1 = lax.rsqrt(row_sq / d_model + EPS)

    arrived(7)
    queries, keys, values, gates = [], [], [], []

    def turn(v):
        return v * cosine + pltpu.roll(v, size // 2, 1) * sine

    for h in range(2):
        total = recv_a[h].astype(F32)
        for j in range(1, nz):
            total = total + recv_a[2 * j + h].astype(F32)
        total = total * scale1
        queries.append(turn(total[:, :size]))
        keys.append(turn(total[:, size : 2 * size]) * size**-0.5)
        values.append(total[:, 2 * size : 3 * size])
        gates.append(total[:, 3 * size :])
    pad = jnp.zeros((size - 4 * seqs, size), F32)
    columns = jnp.transpose(jnp.concatenate(queries + keys + [pad], axis=0))
    for h in range(2):
        head = (tp * 2 + h).astype(F32)
        power = jnp.full((1, size), -5.0, F32) - 5.0 * head / (heads_all - 1)
        gamma = 1.0 - jnp.exp2(power)
        reads = []
        for i in range(seqs):
            at = h * seqs + i
            new = (
                gamma * state_in[i, h]
                + columns[:, 2 * seqs + at : 2 * seqs + at + 1] * values[h][i : i + 1]
            )
            state_new[i, h] = new
            reads.append(jnp.sum(columns[:, at : at + 1] * new, axis=0, keepdims=True))
        read = jnp.concatenate(reads, axis=0)
        read = read * lax.rsqrt(jnp.mean(read * read, axis=1, keepdims=True) + EPS)
        gate = gates[h]
        ret_s[h] = (read * (gate / (1.0 + jnp.exp(-gate)))).astype(BF16)
    ret_r[me] = ret_s[c]

    for peer, core in kv_peers:
        remote(ret_s.at[core], ret_r.at[me], 8, peer)
    expect(nk - 1, 8, ret_r)
    state_copy = load(state_new, state_out, 11)

    later[1].wait()
    later[2].wait()
    arrived(2)
    arrived(3)
    arrived(4)
    for m in range(nb):
        for s in range(2):
            tok_rows[m, :, s * width : (s + 1) * width] = tok2[
                s, m * per_chip : (m + 1) * per_chip
            ].astype(F32)

    arrived(8)
    for j in range(nk):
        ret_f[j * seqs : (j + 1) * seqs] = ret_r[j].astype(F32)
    terms = jnp.dot(ret_f[...].astype(BF16), wo_in[...], preferred_element_type=F32)
    send_c[0] = terms.reshape(nb, per_chip, 2 * width).astype(BF16)
    recv_c[0, block] = send_c[0, block]

    def send_sums(which, phase):
        for t, core in block_peers:
            remote(send_c.at[which, t * 2 + core], recv_c.at[which, block], phase, z * 2 + core, t)
        expect(nb - 1, phase, recv_c.at[which])

    send_sums(0, 9)
    arrived(9)
    mixed = (tok_rows[block] + jnp.sum(recv_c[0].astype(F32), axis=0)).astype(BF16)
    mix_s[...] = mixed
    mix_r[block] = mixed

    for t, core in block_peers:
        remote(mix_s, mix_r.at[block], 10, z * 2 + core, t)
    expect(nb - 1, 10, mix_r)
    later[3].wait()
    arrived(5)
    arrived(10)
    middle = mix_r[...].astype(F32).reshape(rows, 2 * width)
    square = middle * middle
    sq2_s[...] = jnp.sum(
        jnp.transpose(square[:, :width] + square[:, width:]), axis=0, keepdims=True
    )
    sq2_r[z] = sq2_s[...]

    for chip in chips:
        remote(sq2_s, sq2_r.at[z], 11, chip * 2 + c)
    expect(nz - 1, 11, sq2_r)
    normed2 = (middle * gain2[...]).astype(BF16)
    upward = jnp.dot(normed2, wu_in[...], preferred_element_type=F32)
    send_d[...] = upward.reshape(nz, per_chip, half_ff).astype(BF16)

    right, left = ring(z + 1, nz), ring(z + nz - 1, nz)

    def near(src, dst, chip, at):
        pltpu.make_async_remote_copy(
            src_ref=src,
            dst_ref=dst,
            send_sem=send_sem.at[12],
            recv_sem=near_sem.at[at],
            device_id={"kv": chip * 2 + c},
            device_id_type=MESH,
        ).start()

    def far(src, dst, chip, phase, at):
        pltpu.make_async_remote_copy(
            src_ref=src,
            dst_ref=dst,
            send_sem=send_sem.at[phase],
            recv_sem=far_sem.at[at],
            device_id={"kv": chip * 2 + c},
            device_id_type=MESH,
        ).start()

    for k, offset in enumerate(relayed):
        near(send_d.at[ring(right + offset, nz)], near_d.at[k, 0], right, k)
        near(send_d.at[ring(left + offset, nz)], near_d.at[k, 1], left, k)
    going[12] = send_d.at[pl.ds(0, 2 * nr)]
    for k, offset in enumerate(relayed):
        target = ring(z + offset, nz)
        pltpu.make_async_copy(near_d.at[k], near_d.at[k], near_sem.at[k]).wait()
        relay_d[k] = (
            send_d[target].astype(F32) + near_d[k, 0].astype(F32) + near_d[k, 1].astype(F32)
        ).astype(BF16)
        far(relay_d.at[k], recv_d.at[k], target, 16, 0)
    going[16] = relay_d
    row = lax.broadcasted_iota(jnp.int32, (per_chip, size), 0)
    lane = lax.broadcasted_iota(jnp.int32, (per_chip, size), 1)
    arrived(11)
    total_sq = jnp.sum(sq2_r[...], axis=0)
    row_sq = jnp.sum(jnp.where(lane == row + z * per_chip, total_sq, 0.0), axis=1, keepdims=True)
    scale2 = lax.rsqrt(row_sq / d_model + EPS)
    pltpu.make_async_copy(recv_d, recv_d, far_sem.at[0]).wait()
    total = send_d[z].astype(F32)
    for k in range(nr):
        total = total + recv_d[k].astype(F32)
    hidden = jnp.maximum(total * scale2, 0.0)
    hid_s[...] = (hidden * hidden).astype(BF16)
    hid_r[z] = hid_s[...]

    for k, offset in enumerate(relayed):
        far(hid_s, hid_r.at[z], ring(z + offset, nz), 13, k + 1)
    going[13] = hid_r.at[pl.ds(0, nr)]
    for k in reversed(range(nr)):
        source = ring(z + nz - relayed[k], nz)
        pltpu.make_async_copy(hid_r.at[source], hid_r.at[source], far_sem.at[k + 1]).wait()
        for chip in (right, left):
            remote(hid_r.at[source], hid_r.at[source], 17, chip * 2 + c)
    going[17] = coming[17] = hid_r.at[pl.ds(0, 2 * nr)]
    later[4].wait()
    arrived(6)
    arrived(17)
    hidden_all = hid_r[...].astype(F32).reshape(rows, half_ff).astype(BF16)
    terms = jnp.dot(hidden_all, wd_in[...], preferred_element_type=F32)
    send_c[1] = terms.reshape(nb, per_chip, 2 * width).astype(BF16)
    recv_c[1, block] = send_c[1, block]
    send_sums(1, 14)
    arrived(14)
    final = (mix_s[...].astype(F32) + jnp.sum(recv_c[1].astype(F32), axis=0)).astype(BF16)
    for s in range(2):
        out_s[s] = final[:, s * width : (s + 1) * width]
    out_r[block] = out_s[c]

    for t, core in block_peers:
        remote(out_s.at[core], out_r.at[block], 15, z * 2 + core, t)
    expect(nb - 1, 15, out_r)

    state_copy.wait()
    finish()
    out_ref[...] = out_r[...].astype(F32).reshape(rows, width).astype(BF16)


def solution(mesh):
    nk, nt = mesh.shape["kv"], mesh.shape["tp"]
    nz = nk // 2

    def shards(
        tokens,
        positions,
        state,
        norm_gain,
        w_query,
        w_key,
        w_value,
        w_gate,
        w_out,
        mlp_gain,
        w_up,
        w_down,
    ):
        rows, width = tokens.shape
        seqs, heads, size, _ = state.shape
        ff = w_up.shape[1]
        per_chip = rows // nz
        nb = 2 * nt
        inverse = 10000.0 ** (-(np.arange(size // 2, dtype=np.float64) * 2.0) / size)
        freq = jnp.asarray(np.concatenate([inverse, inverse])[None, :].astype(np.float32))
        anywhere = pl.BlockSpec(memory_space=pltpu.HBM)
        vmem = pl.BlockSpec(memory_space=pltpu.VMEM)
        relayed = (8, 5, 11, 2, 14)
        nr = len(relayed)
        cfg = (nk, nt, nz, width * nk, heads * nt, relayed)
        scratch = [
            ((1, size), F32),
            ((rows, width), BF16),
            ((1, width), F32),
            ((4, width, heads * size), BF16),
            (state.shape, F32),
            (state.shape, F32),
            ((size, 2 * width), BF16),
            ((2 * width, ff // 2), BF16),
            ((ff // 2, 2 * width), BF16),
            ((2, rows, width), BF16),
            ((1, 2 * width), F32),
            ((2, rows, 4 * size), F32),
            ((rows, 4 * size), BF16),
            ((rows, 4 * size), BF16),
            ((1, rows), F32),
            ((1, rows), F32),
            ((nz, 1, rows), F32),
            ((nk, seqs, 4 * size), BF16),
            ((nk, seqs, 4 * size), BF16),
            ((2, seqs, size), BF16),
            ((nk, seqs, size), BF16),
            ((rows, size), F32),
            ((2, nb, per_chip, 2 * width), BF16),
            ((2, nb, per_chip, 2 * width), BF16),
            ((nb, per_chip, 2 * width), F32),
            ((per_chip, 2 * width), BF16),
            ((nb, per_chip, 2 * width), BF16),
            ((1, rows), F32),
            ((nz, 1, rows), F32),
            ((nz, per_chip, ff // 2), BF16),
            ((nr, 2, per_chip, ff // 2), BF16),
            ((nr, per_chip, ff // 2), BF16),
            ((nr, per_chip, ff // 2), BF16),
            ((per_chip, ff // 2), BF16),
            ((nz, per_chip, ff // 2), BF16),
            ((2, per_chip, width), BF16),
            ((nb, per_chip, width), BF16),
        ]
        return pl.pallas_call(
            functools.partial(kernel, cfg),
            out_shape=(
                jax.ShapeDtypeStruct((rows, width), BF16),
                jax.ShapeDtypeStruct(state.shape, F32),
            ),
            in_specs=[anywhere] * 13,
            out_specs=(vmem, anywhere),
            scratch_shapes=[pltpu.SMEM((seqs,), jnp.int32)]
            + [pltpu.VMEM(s, t) for s, t in scratch]
            + [
                pltpu.SemaphoreType.DMA((14,)),
                pltpu.SemaphoreType.DMA((19,)),
                pltpu.SemaphoreType.DMA((19,)),
                pltpu.SemaphoreType.DMA((nr,)),
                pltpu.SemaphoreType.DMA((nr + 1,)),
            ],
            compiler_params=pltpu.CompilerParams(
                collective_id=0, has_side_effects=True
            ),
            name="step",
        )(
            positions,
            tokens,
            state,
            norm_gain.reshape(1, width),
            w_query,
            w_key,
            w_value,
            w_gate,
            w_out,
            mlp_gain.reshape(1, width),
            w_up,
            w_down,
            freq,
        )

    return jax.shard_map(
        shards,
        mesh=mesh,
        in_specs=(
            P("grp", "kv"),
            P(("grp", "kv")),
            P(("grp", "kv"), "tp", None, None),
            P("kv"),
            P("kv", "tp"),
            P("kv", "tp"),
            P("kv", "tp"),
            P("kv", "tp"),
            P("tp", "kv"),
            P("kv"),
            P("kv", "tp"),
            P("tp", "kv"),
        ),
        out_specs=(P("grp", "kv"), P(("grp", "kv"), "tp", None, None)),
        check_vma=False,
    )
```

```python
import functools

import jax
import jax.numpy as jnp
import numpy as np
from jax import lax
from jax.experimental import pallas as pl
from jax.experimental.pallas import tpu as pltpu
from jax.sharding import PartitionSpec as P

MESH = pl.DeviceIdType.MESH
F32 = jnp.float32
BF16 = jnp.bfloat16
EPS = 1e-06


def far_first(count):
    return sorted(range(1, count), key=lambda offset: -min(offset, count - offset))


def kernel(
    cfg,
    pos_hbm,
    x_hbm,
    state_hbm,
    gain_hbm,
    wq_hbm,
    wk_hbm,
    wv_hbm,
    wg_hbm,
    wo_hbm,
    gain2_hbm,
    wu_hbm,
    wd_hbm,
    freq_hbm,
    out_ref,
    state_out,
    pos_ref,
    freq_ref,
    x_in,
    gain_in,
    w_in,
    state_in,
    state_new,
    wo_in,
    wu_in,
    wd_in,
    tok2,
    gain2,
    part,
    swap_s,
    swap_r,
    sq_s,
    sq_m,
    sq_r,
    send_a,
    recv_a,
    ret_s,
    ret_r,
    ret_f,
    send_c,
    recv_c,
    tok_rows,
    mix_s,
    mix_r,
    sq2_s,
    sq2_r,
    send_d,
    near_d,
    relay_d,
    recv_d,
    hid_s,
    hid_in,
    hid_r,
    out_s,
    out_r,
    load_sem,
    send_sem,
    recv_sem,
    near_sem,
    far_sem,
):
    nk, nt, nz, d_model, heads_all, relayed = cfg
    me = lax.axis_index("kv")
    tp = lax.axis_index("tp")
    z = me // 2
    c = me % 2
    mate = me + 1 - 2 * c
    block = tp * 2 + c
    nb = nt * 2
    rows = x_in.shape[0]
    width = x_in.shape[1]
    seqs = rows // nk
    per_chip = rows // nz
    size = width
    half_ff = wu_in.shape[1]
    nr = near_d.shape[0]

    def ring(at, count):
        return at - count * (at >= count).astype(jnp.int32)

    chips = [ring(z + offset, nz) for offset in far_first(nz)]
    columns_x = [ring(tp + offset, nt) for offset in far_first(nt)]
    kv_peers = [(chip * 2 + core, core) for chip in chips for core in range(2)] + [(mate, 1 - c)]
    block_peers = [(t, core) for t in columns_x for core in range(2)] + [(tp, 1 - c)]

    barrier = pltpu.get_barrier_semaphore()

    def load(src, dst, sem):
        copy = pltpu.make_async_copy(src, dst, load_sem.at[sem])
        copy.start()
        return copy

    first = [
        load(x_hbm, x_in, 0),
        load(gain_hbm, gain_in, 1),
        load(wq_hbm, w_in.at[0], 2),
        load(wk_hbm, w_in.at[1], 3),
        load(wv_hbm, w_in.at[2], 4),
        load(wg_hbm, w_in.at[3], 5),
        load(pos_hbm, pos_ref, 12),
        load(freq_hbm, freq_ref, 13),
    ]
    for peer, _ in kv_peers:
        pl.semaphore_signal(barrier, inc=1, device_id={"kv": peer}, device_id_type=MESH)
    for t, core in block_peers[:-1]:
        pl.semaphore_signal(
            barrier, inc=1, device_id={"kv": z * 2 + core, "tp": t}, device_id_type=MESH
        )

    here = pl.ds(pl.multiple_of(c * half_ff, 128), half_ff)
    there = pl.ds(pl.multiple_of((1 - c) * half_ff, 128), half_ff)
    mine = pl.ds(pl.multiple_of(c * size, 128), size)
    other_head = pl.ds(pl.multiple_of((1 - c) * size, 128), size)
    my_rows = pl.ds(pl.multiple_of(c * width, 128), width)
    later = [
        load(state_hbm, state_in, 6),
        load(wo_hbm.at[mine], wo_in.at[:, my_rows], 7),
        load(gain2_hbm, gain2.at[:, my_rows], 8),
        load(wu_hbm.at[:, here], wu_in.at[my_rows], 9),
        load(wd_hbm.at[here], wd_in.at[:, my_rows], 10),
    ]

    for copy in first:
        copy.wait()
    x = x_in[...].astype(F32)
    normed = (x * gain_in[...]).astype(BF16)
    square = x * x
    sq_s[...] = jnp.sum(jnp.transpose(square), axis=0, keepdims=True)
    for n in range(4):
        both = jnp.dot(normed, w_in[n], preferred_element_type=F32)
        part[0, :, n * size : (n + 1) * size] = both[:, :size]
        part[1, :, n * size : (n + 1) * size] = both[:, size:]
    swap_s[...] = part[1 - c].astype(BF16)
    tok2[c] = x_in[...]

    pl.semaphore_wait(barrier, nk - 1 + nb - 2)

    going, coming = {}, {}

    def remote(src, dst, phase, kv, t=None):
        where = {"kv": kv} if t is None else {"kv": kv, "tp": t}
        pltpu.make_async_remote_copy(
            src_ref=src,
            dst_ref=dst,
            send_sem=send_sem.at[phase],
            recv_sem=recv_sem.at[phase],
            device_id=where,
            device_id_type=MESH,
        ).start()

    def to_mate(src, dst, phase, amount):
        remote(src, dst, phase, mate)
        going[phase] = coming[phase] = amount

    def expect(count, phase, amount):
        going[phase] = coming[phase] = amount.at[pl.ds(0, count)]

    def arrived(phase):
        ref = coming.pop(phase)
        pltpu.make_async_copy(ref, ref, recv_sem.at[phase]).wait()

    def finish():
        for phase in list(coming):
            arrived(phase)
        for phase, ref in going.items():
            pltpu.make_async_copy(ref, ref, send_sem.at[phase]).wait()

    to_mate(swap_s, swap_r, 0, swap_r)

    to_mate(sq_s, sq_m, 18, sq_m)
    to_mate(x_in, tok2.at[c], 2, x_in)
    to_mate(gain2_hbm, gain2.at[:, my_rows], 3, gain_in)
    to_mate(wo_hbm.at[other_head], wo_in.at[:, my_rows], 4, x_in)
    to_mate(wu_hbm.at[:, there], wu_in.at[my_rows], 5, wu_in.at[pl.ds(0, width)])
    to_mate(wd_hbm.at[there], wd_in.at[:, my_rows], 6, wd_in.at[:, pl.ds(0, width)])

    arrived(18)
    sq_r[z] = sq_s[...] + sq_m[...]
    arrived(0)
    part[c] = part[c] + swap_r[...].astype(F32)
    for j in range(nk):
        send_a[j] = part[c, j * seqs : (j + 1) * seqs, :].astype(BF16)
    recv_a[me] = send_a[me]

    for chip in chips:
        for core in range(2):
            peer = chip * 2 + core
            remote(send_a.at[peer], recv_a.at[me], 7, peer)
        remote(sq_r.at[z], sq_r.at[z], 1, chip * 2 + c)
    remote(send_a.at[mate], recv_a.at[me], 7, mate)
    expect(nk - 1, 7, recv_a)
    expect(nz - 1, 1, sq_r)

    row = lax.broadcasted_iota(jnp.int32, (seqs, size), 0)
    lane = lax.broadcasted_iota(jnp.int32, (seqs, size), 1)
    place = jnp.zeros((seqs, size), F32)
    for i in range(seqs):
        place = jnp.where(row == i, pos_ref[i].astype(F32), place)
    angle = place * freq_ref[...]
    cosine = jnp.cos(angle)
    sine = jnp.sin(angle)
    sine = jnp.where(lane < size // 2, -sine, sine)
    later[0].wait()

    arrived(1)
    total_sq = jnp.sum(sq_r[...], axis=0)
    row_sq = jnp.sum(jnp.where(lane == row + me * seqs, total_sq, 0.0), axis=1, keepdims=True)
    scale1 = lax.rsqrt(row_sq / d_model + EPS)

    arrived(7)
    queries, keys, values, gates = [], [], [], []

    def turn(v):
        return v * cosine + pltpu.roll(v, size // 2, 1) * sine

    for h in range(2):
        total = recv_a[h].astype(F32)
        for j in range(1, nz):
            total = total + recv_a[2 * j + h].astype(F32)
        total = total * scale1
        queries.append(turn(total[:, :size]))
        keys.append(turn(total[:, size : 2 * size]) * size**-0.5)
        values.append(total[:, 2 * size : 3 * size])
        gates.append(total[:, 3 * size :])
    pad = jnp.zeros((size - 4 * seqs, size), F32)
    columns = jnp.transpose(jnp.concatenate(queries + keys + [pad], axis=0))
    for h in range(2):
        head = (tp * 2 + h).astype(F32)
        power = jnp.full((1, size), -5.0, F32) - 5.0 * head / (heads_all - 1)
        gamma = 1.0 - jnp.exp2(power)
        reads = []
        for i in range(seqs):
            at = h * seqs + i
            new = (
                gamma * state_in[i, h]
                + columns[:, 2 * seqs + at : 2 * seqs + at + 1] * values[h][i : i + 1]
            )
            state_new[i, h] = new
            reads.append(jnp.sum(columns[:, at : at + 1] * new, axis=0, keepdims=True))
        read = jnp.concatenate(reads, axis=0)
        read = read * lax.rsqrt(jnp.mean(read * read, axis=1, keepdims=True) + EPS)
        gate = gates[h]
        ret_s[h] = (read * (gate / (1.0 + jnp.exp(-gate)))).astype(BF16)
    ret_r[me] = ret_s[c]

    for peer, core in kv_peers:
        remote(ret_s.at[core], ret_r.at[me], 8, peer)
    expect(nk - 1, 8, ret_r)
    state_copy = load(state_new, state_out, 11)

    later[1].wait()
    later[2].wait()
    arrived(2)
    arrived(3)
    arrived(4)
    for m in range(nb):
        for s in range(2):
            tok_rows[m, :, s * width : (s + 1) * width] = tok2[
                s, m * per_chip : (m + 1) * per_chip
            ].astype(F32)

    arrived(8)
    for j in range(nk):
        ret_f[j * seqs : (j + 1) * seqs] = ret_r[j].astype(F32)
    terms = jnp.dot(ret_f[...].astype(BF16), wo_in[...], preferred_element_type=F32)
    send_c[0] = terms.reshape(nb, per_chip, 2 * width).astype(BF16)
    recv_c[0, block] = send_c[0, block]

    def send_sums(which, phase):
        for t, core in block_peers:
            remote(send_c.at[which, t * 2 + core], recv_c.at[which, block], phase, z * 2 + core, t)
        expect(nb - 1, phase, recv_c.at[which])

    send_sums(0, 9)
    arrived(9)
    mixed = (tok_rows[block] + jnp.sum(recv_c[0].astype(F32), axis=0)).astype(BF16)
    mix_s[...] = mixed
    mix_r[block] = mixed

    for t, core in block_peers:
        remote(mix_s, mix_r.at[block], 10, z * 2 + core, t)
    expect(nb - 1, 10, mix_r)
    later[3].wait()
    arrived(5)
    arrived(10)
    middle = mix_r[...].astype(F32).reshape(rows, 2 * width)
    square = middle * middle
    sq2_s[...] = jnp.sum(
        jnp.transpose(square[:, :width] + square[:, width:]), axis=0, keepdims=True
    )
    sq2_r[z] = sq2_s[...]

    for chip in chips:
        remote(sq2_s, sq2_r.at[z], 11, chip * 2 + c)
    expect(nz - 1, 11, sq2_r)
    normed2 = (middle * gain2[...]).astype(BF16)
    upward = jnp.dot(normed2, wu_in[...], preferred_element_type=F32)
    send_d[...] = upward.reshape(nz, per_chip, half_ff).astype(BF16)

    right, left = ring(z + 1, nz), ring(z + nz - 1, nz)

    def hop(src, dst, kv, phase, sem):
        pltpu.make_async_remote_copy(
            src_ref=src,
            dst_ref=dst,
            send_sem=send_sem.at[phase],
            recv_sem=sem,
            device_id={"kv": kv},
            device_id_type=MESH,
        ).start()

    for k, offset in enumerate(relayed):
        hop(send_d.at[ring(right + offset, nz)], near_d.at[k, 0], right * 2 + c, 12, near_sem.at[k])
        hop(send_d.at[ring(left + offset, nz)], near_d.at[k, 1], left * 2 + c, 12, near_sem.at[k])
    going[12] = send_d.at[pl.ds(0, 2 * nr)]
    hop(send_d.at[z], recv_d.at[nr], mate, 19, far_sem.at[0])
    for k, offset in enumerate(relayed):
        target = ring(z + offset, nz)
        pltpu.make_async_copy(near_d.at[k], near_d.at[k], near_sem.at[k]).wait()
        relay_d[k] = (
            send_d[target].astype(F32) + near_d[k, 0].astype(F32) + near_d[k, 1].astype(F32)
        ).astype(BF16)
        hop(relay_d.at[k], recv_d.at[k], target * 2 + 1 - c, 16, far_sem.at[0])
    going[16] = relay_d
    going[19] = hid_s
    row = lax.broadcasted_iota(jnp.int32, (per_chip, size), 0)
    lane = lax.broadcasted_iota(jnp.int32, (per_chip, size), 1)
    arrived(11)
    total_sq = jnp.sum(sq2_r[...], axis=0)
    row_sq = jnp.sum(jnp.where(lane == row + z * per_chip, total_sq, 0.0), axis=1, keepdims=True)
    scale2 = lax.rsqrt(row_sq / d_model + EPS)
    pltpu.make_async_copy(recv_d, recv_d, far_sem.at[0]).wait()
    total = recv_d[0].astype(F32)
    for k in range(1, nr + 1):
        total = total + recv_d[k].astype(F32)
    hidden = jnp.maximum(total * scale2, 0.0)
    hid_s[...] = (hidden * hidden).astype(BF16)
    for k, offset in enumerate(relayed):
        hop(hid_s, hid_in.at[k], ring(z + offset, nz) * 2 + c, 13, far_sem.at[k + 1])
    going[13] = hid_in
    remote(hid_s, hid_r.at[z], 17, mate)
    for k in reversed(range(nr)):
        source = ring(z + nz - relayed[k], nz)
        pltpu.make_async_copy(hid_in.at[k], hid_in.at[k], far_sem.at[k + 1]).wait()
        for kv in (right * 2 + 1 - c, left * 2 + 1 - c, mate):
            remote(hid_in.at[k], hid_r.at[source], 17, kv)
    going[17] = coming[17] = hid_r
    later[4].wait()
    arrived(6)
    arrived(17)
    hidden_all = hid_r[...].astype(F32).reshape(rows, half_ff).astype(BF16)
    terms = jnp.dot(hidden_all, wd_in[...], preferred_element_type=F32)
    send_c[1] = terms.reshape(nb, per_chip, 2 * width).astype(BF16)
    recv_c[1, block] = send_c[1, block]
    send_sums(1, 14)
    arrived(14)
    final = (mix_s[...].astype(F32) + jnp.sum(recv_c[1].astype(F32), axis=0)).astype(BF16)
    for s in range(2):
        out_s[s] = final[:, s * width : (s + 1) * width]
    out_r[block] = out_s[c]

    for t, core in block_peers:
        remote(out_s.at[core], out_r.at[block], 15, z * 2 + core, t)
    expect(nb - 1, 15, out_r)

    state_copy.wait()
    finish()
    out_ref[...] = out_r[...].astype(F32).reshape(rows, width).astype(BF16)


def solution(mesh):
    nk, nt = mesh.shape["kv"], mesh.shape["tp"]
    nz = nk // 2

    def shards(
        tokens,
        positions,
        state,
        norm_gain,
        w_query,
        w_key,
        w_value,
        w_gate,
        w_out,
        mlp_gain,
        w_up,
        w_down,
    ):
        rows, width = tokens.shape
        seqs, heads, size, _ = state.shape
        ff = w_up.shape[1]
        per_chip = rows // nz
        nb = 2 * nt
        inverse = 10000.0 ** (-(np.arange(size // 2, dtype=np.float64) * 2.0) / size)
        freq = jnp.asarray(np.concatenate([inverse, inverse])[None, :].astype(np.float32))
        anywhere = pl.BlockSpec(memory_space=pltpu.HBM)
        vmem = pl.BlockSpec(memory_space=pltpu.VMEM)
        relayed = (8, 5, 11, 2, 14)
        nr = len(relayed)
        cfg = (nk, nt, nz, width * nk, heads * nt, relayed)
        scratch = [
            ((1, size), F32),
            ((rows, width), BF16),
            ((1, width), F32),
            ((4, width, heads * size), BF16),
            (state.shape, F32),
            (state.shape, F32),
            ((size, 2 * width), BF16),
            ((2 * width, ff // 2), BF16),
            ((ff // 2, 2 * width), BF16),
            ((2, rows, width), BF16),
            ((1, 2 * width), F32),
            ((2, rows, 4 * size), F32),
            ((rows, 4 * size), BF16),
            ((rows, 4 * size), BF16),
            ((1, rows), F32),
            ((1, rows), F32),
            ((nz, 1, rows), F32),
            ((nk, seqs, 4 * size), BF16),
            ((nk, seqs, 4 * size), BF16),
            ((2, seqs, size), BF16),
            ((nk, seqs, size), BF16),
            ((rows, size), F32),
            ((2, nb, per_chip, 2 * width), BF16),
            ((2, nb, per_chip, 2 * width), BF16),
            ((nb, per_chip, 2 * width), F32),
            ((per_chip, 2 * width), BF16),
            ((nb, per_chip, 2 * width), BF16),
            ((1, rows), F32),
            ((nz, 1, rows), F32),
            ((nz, per_chip, ff // 2), BF16),
            ((nr, 2, per_chip, ff // 2), BF16),
            ((nr, per_chip, ff // 2), BF16),
            ((nr + 1, per_chip, ff // 2), BF16),
            ((per_chip, ff // 2), BF16),
            ((nr, per_chip, ff // 2), BF16),
            ((nz, per_chip, ff // 2), BF16),
            ((2, per_chip, width), BF16),
            ((nb, per_chip, width), BF16),
        ]
        return pl.pallas_call(
            functools.partial(kernel, cfg),
            out_shape=(
                jax.ShapeDtypeStruct((rows, width), BF16),
                jax.ShapeDtypeStruct(state.shape, F32),
            ),
            in_specs=[anywhere] * 13,
            out_specs=(vmem, anywhere),
            scratch_shapes=[pltpu.SMEM((seqs,), jnp.int32)]
            + [pltpu.VMEM(s, t) for s, t in scratch]
            + [
                pltpu.SemaphoreType.DMA((14,)),
                pltpu.SemaphoreType.DMA((20,)),
                pltpu.SemaphoreType.DMA((20,)),
                pltpu.SemaphoreType.DMA((nr,)),
                pltpu.SemaphoreType.DMA((nr + 1,)),
            ],
            compiler_params=pltpu.CompilerParams(
                collective_id=0, has_side_effects=True
            ),
            name="step",
        )(
            positions,
            tokens,
            state,
            norm_gain.reshape(1, width),
            w_query,
            w_key,
            w_value,
            w_gate,
            w_out,
            mlp_gain.reshape(1, width),
            w_up,
            w_down,
            freq,
        )

    return jax.shard_map(
        shards,
        mesh=mesh,
        in_specs=(
            P("grp", "kv"),
            P(("grp", "kv")),
            P(("grp", "kv"), "tp", None, None),
            P("kv"),
            P("kv", "tp"),
            P("kv", "tp"),
            P("kv", "tp"),
            P("kv", "tp"),
            P("tp", "kv"),
            P("kv"),
            P("kv", "tp"),
            P("tp", "kv"),
        ),
        out_specs=(P("grp", "kv"), P(("grp", "kv"), "tp", None, None)),
        check_vma=False,
    )
```

```python
import functools

import jax
import jax.numpy as jnp
import numpy as np
from jax import lax
from jax.experimental import pallas as pl
from jax.experimental.pallas import tpu as pltpu
from jax.sharding import PartitionSpec as P

MESH = pl.DeviceIdType.MESH
F32 = jnp.float32
BF16 = jnp.bfloat16
EPS = 1e-06


def far_first(count):
    return sorted(range(1, count), key=lambda offset: -min(offset, count - offset))


def kernel(
    cfg,
    pos_hbm,
    x_hbm,
    state_hbm,
    gain_hbm,
    wq_hbm,
    wk_hbm,
    wv_hbm,
    wg_hbm,
    wo_hbm,
    gain2_hbm,
    wu_hbm,
    wd_hbm,
    freq_hbm,
    out_ref,
    state_out,
    pos_ref,
    freq_ref,
    x_in,
    gain_in,
    w_in,
    state_in,
    state_new,
    wo_in,
    wu_in,
    wd_in,
    tok2,
    gain2,
    part,
    swap_s,
    swap_r,
    sq_s,
    sq_m,
    sq_r,
    send_a,
    recv_a,
    ret_s,
    ret_r,
    ret_f,
    send_c,
    recv_c,
    tok_rows,
    mix_s,
    mix_r,
    sq2_s,
    sq2_r,
    send_d,
    near_d,
    relay_d,
    recv_d,
    hid_s,
    hid_in,
    hid_r,
    out_s,
    out_r,
    load_sem,
    send_sem,
    recv_sem,
    near_sem,
    far_sem,
):
    nk, nt, nz, d_model, heads_all, relayed = cfg
    me = lax.axis_index("kv")
    tp = lax.axis_index("tp")
    z = me // 2
    c = me % 2
    mate = me + 1 - 2 * c
    nb = nt * 2
    group = x_in.shape[0] // nt
    rows = x_in.shape[0]
    width = x_in.shape[1]
    seqs = rows // nk
    per_chip = rows // nz
    size = width
    half_ff = wu_in.shape[1]
    nr = near_d.shape[0]

    def ring(at, count):
        return at - count * (at >= count).astype(jnp.int32)

    chips = [ring(z + offset, nz) for offset in far_first(nz)]
    columns_x = [ring(tp + offset, nt) for offset in far_first(nt)]
    kv_peers = [(chip * 2 + core, core) for chip in chips for core in range(2)] + [(mate, 1 - c)]
    block_peers = [(t, core) for t in columns_x for core in range(2)] + [(tp, 1 - c)]

    barrier = pltpu.get_barrier_semaphore()

    def load(src, dst, sem):
        copy = pltpu.make_async_copy(src, dst, load_sem.at[sem])
        copy.start()
        return copy

    first = [
        load(x_hbm, x_in, 0),
        load(gain_hbm, gain_in, 1),
        load(wq_hbm, w_in.at[0], 2),
        load(wk_hbm, w_in.at[1], 3),
        load(wv_hbm, w_in.at[2], 4),
        load(wg_hbm, w_in.at[3], 5),
        load(pos_hbm, pos_ref, 12),
        load(freq_hbm, freq_ref, 13),
    ]
    for peer, _ in kv_peers:
        pl.semaphore_signal(barrier, inc=1, device_id={"kv": peer}, device_id_type=MESH)
    for t, core in block_peers[:-1]:
        pl.semaphore_signal(
            barrier, inc=1, device_id={"kv": z * 2 + core, "tp": t}, device_id_type=MESH
        )

    here = pl.ds(pl.multiple_of(c * half_ff, 128), half_ff)
    there = pl.ds(pl.multiple_of((1 - c) * half_ff, 128), half_ff)
    mine = pl.ds(pl.multiple_of(c * size, 128), size)
    other_head = pl.ds(pl.multiple_of((1 - c) * size, 128), size)
    my_rows = pl.ds(pl.multiple_of(c * width, 128), width)
    later = [
        load(state_hbm, state_in, 6),
        load(wo_hbm.at[mine], wo_in.at[:, my_rows], 7),
        load(gain2_hbm, gain2.at[:, my_rows], 8),
        load(wu_hbm.at[:, here], wu_in.at[my_rows], 9),
        load(wd_hbm.at[here], wd_in.at[:, my_rows], 10),
    ]

    for copy in first:
        copy.wait()
    x = x_in[...].astype(F32)
    normed = (x * gain_in[...]).astype(BF16)
    square = x * x
    sq_s[...] = jnp.sum(jnp.transpose(square), axis=0, keepdims=True)
    for n in range(4):
        both = jnp.dot(normed, w_in[n], preferred_element_type=F32)
        part[0, :, n * size : (n + 1) * size] = both[:, :size]
        part[1, :, n * size : (n + 1) * size] = both[:, size:]
    swap_s[...] = part[1 - c].astype(BF16)
    tok2[c] = x_in[...]

    pl.semaphore_wait(barrier, nk - 1 + nb - 2)

    going, coming = {}, {}

    def remote(src, dst, phase, kv, t=None):
        where = {"kv": kv} if t is None else {"kv": kv, "tp": t}
        pltpu.make_async_remote_copy(
            src_ref=src,
            dst_ref=dst,
            send_sem=send_sem.at[phase],
            recv_sem=recv_sem.at[phase],
            device_id=where,
            device_id_type=MESH,
        ).start()

    def to_mate(src, dst, phase, amount):
        remote(src, dst, phase, mate)
        going[phase] = coming[phase] = amount

    def expect(count, phase, amount):
        going[phase] = coming[phase] = amount.at[pl.ds(0, count)]

    def arrived(phase):
        pause(coming.pop(phase), recv_sem.at[phase])

    def pause(amount, sem):
        if isinstance(amount, tuple):
            for core, one in enumerate(amount):
                if one is not None:
                    pl.when(c == core)(functools.partial(pause, one, sem))
        else:
            pltpu.make_async_copy(amount, amount, sem).wait()

    def finish():
        for phase in list(coming):
            arrived(phase)
        for phase, amount in going.items():
            pause(amount, send_sem.at[phase])

    to_mate(swap_s, swap_r, 0, swap_r)

    to_mate(sq_s, sq_m, 18, sq_m)
    to_mate(x_in, tok2.at[c], 2, x_in)
    to_mate(gain2_hbm, gain2.at[:, my_rows], 3, gain_in)
    to_mate(wo_hbm.at[other_head], wo_in.at[:, my_rows], 4, x_in)
    to_mate(wu_hbm.at[:, there], wu_in.at[my_rows], 5, wu_in.at[pl.ds(0, width)])
    to_mate(wd_hbm.at[there], wd_in.at[:, my_rows], 6, wd_in.at[:, pl.ds(0, width)])

    arrived(18)
    sq_r[z] = sq_s[...] + sq_m[...]
    arrived(0)
    part[c] = part[c] + swap_r[...].astype(F32)
    for j in range(nk):
        send_a[j] = part[c, j * seqs : (j + 1) * seqs, :].astype(BF16)
    recv_a[me] = send_a[me]

    for chip in chips:
        for core in range(2):
            peer = chip * 2 + core
            remote(send_a.at[peer], recv_a.at[me], 7, peer)
        remote(sq_r.at[z], sq_r.at[z], 1, chip * 2 + c)
    remote(send_a.at[mate], recv_a.at[me], 7, mate)
    expect(nk - 1, 7, recv_a)
    expect(nz - 1, 1, sq_r)

    row = lax.broadcasted_iota(jnp.int32, (seqs, size), 0)
    lane = lax.broadcasted_iota(jnp.int32, (seqs, size), 1)
    place = jnp.zeros((seqs, size), F32)
    for i in range(seqs):
        place = jnp.where(row == i, pos_ref[i].astype(F32), place)
    angle = place * freq_ref[...]
    cosine = jnp.cos(angle)
    sine = jnp.sin(angle)
    sine = jnp.where(lane < size // 2, -sine, sine)
    later[0].wait()

    arrived(1)
    total_sq = jnp.sum(sq_r[...], axis=0)
    row_sq = jnp.sum(jnp.where(lane == row + me * seqs, total_sq, 0.0), axis=1, keepdims=True)
    scale1 = lax.rsqrt(row_sq / d_model + EPS)

    arrived(7)
    queries, keys, values, gates = [], [], [], []

    def turn(v):
        return v * cosine + pltpu.roll(v, size // 2, 1) * sine

    for h in range(2):
        total = recv_a[h].astype(F32)
        for j in range(1, nz):
            total = total + recv_a[2 * j + h].astype(F32)
        total = total * scale1
        queries.append(turn(total[:, :size]))
        keys.append(turn(total[:, size : 2 * size]) * size**-0.5)
        values.append(total[:, 2 * size : 3 * size])
        gates.append(total[:, 3 * size :])
    pad = jnp.zeros((size - 4 * seqs, size), F32)
    columns = jnp.transpose(jnp.concatenate(queries + keys + [pad], axis=0))
    for h in range(2):
        head = (tp * 2 + h).astype(F32)
        power = jnp.full((1, size), -5.0, F32) - 5.0 * head / (heads_all - 1)
        gamma = 1.0 - jnp.exp2(power)
        reads = []
        for i in range(seqs):
            at = h * seqs + i
            new = (
                gamma * state_in[i, h]
                + columns[:, 2 * seqs + at : 2 * seqs + at + 1] * values[h][i : i + 1]
            )
            state_new[i, h] = new
            reads.append(jnp.sum(columns[:, at : at + 1] * new, axis=0, keepdims=True))
        read = jnp.concatenate(reads, axis=0)
        read = read * lax.rsqrt(jnp.mean(read * read, axis=1, keepdims=True) + EPS)
        gate = gates[h]
        ret_s[h] = (read * (gate / (1.0 + jnp.exp(-gate)))).astype(BF16)
    ret_r[me] = ret_s[c]

    for peer, core in kv_peers:
        remote(ret_s.at[core], ret_r.at[me], 8, peer)
    expect(nk - 1, 8, ret_r)
    state_copy = load(state_new, state_out, 11)

    later[1].wait()
    later[2].wait()
    arrived(2)
    arrived(3)
    arrived(4)
    for m in range(nt):
        for s in range(2):
            tok_rows[m, :, s * width : (s + 1) * width] = tok2[
                s, m * group : (m + 1) * group
            ].astype(F32)

    arrived(8)
    for j in range(nk):
        ret_f[j * seqs : (j + 1) * seqs] = ret_r[j].astype(F32)
    terms = jnp.dot(ret_f[...].astype(BF16), wo_in[...], preferred_element_type=F32)

    def send_sums(which, phase):
        send_c[which] = terms.reshape(nt, group, 2 * width).astype(BF16)
        slot = recv_c.at[which, tp * 2 + c]
        for t in columns_x:
            remote(send_c.at[which, t], slot, phase, z * 2 + 1, t)

        @pl.when(c == 0)
        def _():
            remote(send_c.at[which, tp], slot, phase, mate)

        @pl.when(c == 1)
        def _():
            recv_c[which, tp * 2 + 1] = send_c[which, tp]

        going[phase] = (send_c.at[which], send_c.at[which, pl.ds(0, nt - 1)])
        coming[phase] = (None, recv_c.at[which, pl.ds(0, nb - 1)])

    def added(which):
        return jnp.sum(recv_c[which].astype(F32), axis=0)

    send_sums(0, 9)
    arrived(9)
    @pl.when(c == 1)
    def _():
        mixed = (tok_rows[tp] + added(0)).astype(BF16)
        mix_s[...] = mixed
        mix_r[tp] = mixed
        for t in columns_x:
            for core in range(2):
                remote(mix_s, mix_r.at[tp], 10, z * 2 + core, t)
        remote(mix_s, mix_r.at[tp], 10, mate)

    going[10] = (None, recv_c.at[0, pl.ds(0, nb - 1)])
    coming[10] = (mix_r, mix_r.at[pl.ds(0, nt - 1)])
    later[3].wait()
    arrived(5)
    arrived(10)
    middle = mix_r[...].astype(F32).reshape(rows, 2 * width)
    square = middle * middle
    sq2_s[...] = jnp.sum(
        jnp.transpose(square[:, :width] + square[:, width:]), axis=0, keepdims=True
    )
    sq2_r[z] = sq2_s[...]

    for chip in chips:
        remote(sq2_s, sq2_r.at[z], 11, chip * 2 + c)
    expect(nz - 1, 11, sq2_r)
    normed2 = (middle * gain2[...]).astype(BF16)
    upward = jnp.dot(normed2, wu_in[...], preferred_element_type=F32)
    send_d[...] = upward.reshape(nz, per_chip, half_ff).astype(BF16)

    right, left = ring(z + 1, nz), ring(z + nz - 1, nz)

    def hop(src, dst, kv, phase, sem):
        pltpu.make_async_remote_copy(
            src_ref=src,
            dst_ref=dst,
            send_sem=send_sem.at[phase],
            recv_sem=sem,
            device_id={"kv": kv},
            device_id_type=MESH,
        ).start()

    for k, offset in enumerate(relayed):
        hop(send_d.at[ring(right + offset, nz)], near_d.at[k, 0], right * 2 + c, 12, near_sem.at[k])
        hop(send_d.at[ring(left + offset, nz)], near_d.at[k, 1], left * 2 + c, 12, near_sem.at[k])
    going[12] = send_d.at[pl.ds(0, 2 * nr)]
    hop(send_d.at[z], recv_d.at[nr], mate, 19, far_sem.at[0])
    for k, offset in enumerate(relayed):
        target = ring(z + offset, nz)
        pltpu.make_async_copy(near_d.at[k], near_d.at[k], near_sem.at[k]).wait()
        relay_d[k] = (
            send_d[target].astype(F32) + near_d[k, 0].astype(F32) + near_d[k, 1].astype(F32)
        ).astype(BF16)
        hop(relay_d.at[k], recv_d.at[k], target * 2 + 1 - c, 16, far_sem.at[0])
    going[16] = relay_d
    going[19] = hid_s
    row = lax.broadcasted_iota(jnp.int32, (per_chip, size), 0)
    lane = lax.broadcasted_iota(jnp.int32, (per_chip, size), 1)
    arrived(11)
    total_sq = jnp.sum(sq2_r[...], axis=0)
    row_sq = jnp.sum(jnp.where(lane == row + z * per_chip, total_sq, 0.0), axis=1, keepdims=True)
    scale2 = lax.rsqrt(row_sq / d_model + EPS)
    pltpu.make_async_copy(recv_d, recv_d, far_sem.at[0]).wait()
    total = recv_d[0].astype(F32)
    for k in range(1, nr + 1):
        total = total + recv_d[k].astype(F32)
    hidden = jnp.maximum(total * scale2, 0.0)
    hid_s[...] = (hidden * hidden).astype(BF16)
    for k, offset in enumerate(relayed):
        hop(hid_s, hid_in.at[k], ring(z + offset, nz) * 2 + c, 13, far_sem.at[k + 1])
    going[13] = hid_in
    remote(hid_s, hid_r.at[z], 17, mate)
    for k in reversed(range(nr)):
        source = ring(z + nz - relayed[k], nz)
        pltpu.make_async_copy(hid_in.at[k], hid_in.at[k], far_sem.at[k + 1]).wait()
        for kv in (right * 2 + 1 - c, left * 2 + 1 - c, mate):
            remote(hid_in.at[k], hid_r.at[source], 17, kv)
    going[17] = coming[17] = hid_r
    later[4].wait()
    arrived(6)
    arrived(17)
    hidden_all = hid_r[...].astype(F32).reshape(rows, half_ff).astype(BF16)
    terms = jnp.dot(hidden_all, wd_in[...], preferred_element_type=F32)
    send_sums(1, 14)
    arrived(14)
    @pl.when(c == 1)
    def _():
        final = (mix_s[...].astype(F32) + added(1)).astype(BF16)
        for s in range(2):
            out_s[s] = final[:, s * width : (s + 1) * width]
        out_r[tp] = out_s[1]
        for t in columns_x:
            for core in range(2):
                remote(out_s.at[core], out_r.at[tp], 15, z * 2 + core, t)
        remote(out_s.at[0], out_r.at[tp], 15, mate)

    going[15] = (None, recv_c.at[0, pl.ds(0, nb - 1), :, pl.ds(0, width)])
    coming[15] = (out_r, out_r.at[pl.ds(0, nt - 1)])

    state_copy.wait()
    finish()
    out_ref[...] = out_r[...].reshape(rows, width)


def solution(mesh):
    nk, nt = mesh.shape["kv"], mesh.shape["tp"]
    nz = nk // 2

    def shards(
        tokens,
        positions,
        state,
        norm_gain,
        w_query,
        w_key,
        w_value,
        w_gate,
        w_out,
        mlp_gain,
        w_up,
        w_down,
    ):
        rows, width = tokens.shape
        seqs, heads, size, _ = state.shape
        ff = w_up.shape[1]
        per_chip = rows // nz
        nb = 2 * nt
        group = rows // nt
        inverse = 10000.0 ** (-(np.arange(size // 2, dtype=np.float64) * 2.0) / size)
        freq = jnp.asarray(np.concatenate([inverse, inverse])[None, :].astype(np.float32))
        anywhere = pl.BlockSpec(memory_space=pltpu.HBM)
        vmem = pl.BlockSpec(memory_space=pltpu.VMEM)
        relayed = (8, 5, 11, 2, 14)
        nr = len(relayed)
        cfg = (nk, nt, nz, width * nk, heads * nt, relayed)
        scratch = [
            ((1, size), F32),
            ((rows, width), BF16),
            ((1, width), F32),
            ((4, width, heads * size), BF16),
            (state.shape, F32),
            (state.shape, F32),
            ((size, 2 * width), BF16),
            ((2 * width, ff // 2), BF16),
            ((ff // 2, 2 * width), BF16),
            ((2, rows, width), BF16),
            ((1, 2 * width), F32),
            ((2, rows, 4 * size), F32),
            ((rows, 4 * size), BF16),
            ((rows, 4 * size), BF16),
            ((1, rows), F32),
            ((1, rows), F32),
            ((nz, 1, rows), F32),
            ((nk, seqs, 4 * size), BF16),
            ((nk, seqs, 4 * size), BF16),
            ((2, seqs, size), BF16),
            ((nk, seqs, size), BF16),
            ((rows, size), F32),
            ((2, nt, group, 2 * width), BF16),
            ((2, nb, group, 2 * width), BF16),
            ((nt, group, 2 * width), F32),
            ((group, 2 * width), BF16),
            ((nt, group, 2 * width), BF16),
            ((1, rows), F32),
            ((nz, 1, rows), F32),
            ((nz, per_chip, ff // 2), BF16),
            ((nr, 2, per_chip, ff // 2), BF16),
            ((nr, per_chip, ff // 2), BF16),
            ((nr + 1, per_chip, ff // 2), BF16),
            ((per_chip, ff // 2), BF16),
            ((nr, per_chip, ff // 2), BF16),
            ((nz, per_chip, ff // 2), BF16),
            ((2, group, width), BF16),
            ((nt, group, width), BF16),
        ]
        return pl.pallas_call(
            functools.partial(kernel, cfg),
            out_shape=(
                jax.ShapeDtypeStruct((rows, width), BF16),
                jax.ShapeDtypeStruct(state.shape, F32),
            ),
            in_specs=[anywhere] * 13,
            out_specs=(vmem, anywhere),
            scratch_shapes=[pltpu.SMEM((seqs,), jnp.int32)]
            + [pltpu.VMEM(s, t) for s, t in scratch]
            + [
                pltpu.SemaphoreType.DMA((14,)),
                pltpu.SemaphoreType.DMA((20,)),
                pltpu.SemaphoreType.DMA((20,)),
                pltpu.SemaphoreType.DMA((nr,)),
                pltpu.SemaphoreType.DMA((nr + 1,)),
            ],
            compiler_params=pltpu.CompilerParams(
                collective_id=0, has_side_effects=True
            ),
            name="step",
        )(
            positions,
            tokens,
            state,
            norm_gain.reshape(1, width),
            w_query,
            w_key,
            w_value,
            w_gate,
            w_out,
            mlp_gain.reshape(1, width),
            w_up,
            w_down,
            freq,
        )

    return jax.shard_map(
        shards,
        mesh=mesh,
        in_specs=(
            P("grp", "kv"),
            P(("grp", "kv")),
            P(("grp", "kv"), "tp", None, None),
            P("kv"),
            P("kv", "tp"),
            P("kv", "tp"),
            P("kv", "tp"),
            P("kv", "tp"),
            P("tp", "kv"),
            P("kv"),
            P("kv", "tp"),
            P("tp", "kv"),
        ),
        out_specs=(P("grp", "kv"), P(("grp", "kv"), "tp", None, None)),
        check_vma=False,
    )
```

```python
import functools

import jax
import jax.numpy as jnp
import numpy as np
from jax import lax
from jax.experimental import pallas as pl
from jax.experimental.pallas import tpu as pltpu
from jax.sharding import PartitionSpec as P

MESH = pl.DeviceIdType.MESH
F32 = jnp.float32
BF16 = jnp.bfloat16
EPS = 1e-06


def far_first(count):
    return sorted(range(1, count), key=lambda offset: -min(offset, count - offset))


def kernel(
    cfg,
    pos_hbm,
    x_hbm,
    state_hbm,
    gain_hbm,
    wq_hbm,
    wk_hbm,
    wv_hbm,
    wg_hbm,
    wo_hbm,
    gain2_hbm,
    wu_hbm,
    wd_hbm,
    freq_hbm,
    out_ref,
    state_out,
    pos_ref,
    freq_ref,
    x_in,
    gain_in,
    w_in,
    state_in,
    state_new,
    wo_in,
    wu_in,
    wd_in,
    tok2,
    gain2,
    part,
    swap_s,
    swap_r,
    sq_s,
    sq_m,
    sq_r,
    send_a,
    recv_a,
    ret_s,
    ret_r,
    ret_f,
    send_c,
    recv_c,
    tok_rows,
    mix_s,
    mix_r,
    sq2_s,
    sq2_r,
    send_d,
    recv_d,
    hid_s,
    hid_in,
    hid_r,
    out_s,
    out_r,
    load_sem,
    send_sem,
    recv_sem,
    far_sem,
):
    nk, nt, nz, d_model, heads_all, relayed = cfg
    me = lax.axis_index("kv")
    tp = lax.axis_index("tp")
    z = me // 2
    c = me % 2
    mate = me + 1 - 2 * c
    nb = nt * 2
    group = x_in.shape[0] // nt
    rows = x_in.shape[0]
    width = x_in.shape[1]
    seqs = rows // nk
    per_chip = rows // nz
    size = width
    half_ff = wd_in.shape[0]
    quarter = wu_in.shape[1]
    pair = z // 2
    b = z % 2
    beside = z + 1 - 2 * b
    half_nz = nz // 2
    nr = hid_in.shape[0]

    def ring(at, count):
        return at - count * (at >= count).astype(jnp.int32)

    chips = [ring(z + offset, nz) for offset in far_first(nz)]
    columns_x = [ring(tp + offset, nt) for offset in far_first(nt)]
    kv_peers = [(chip * 2 + core, core) for chip in chips for core in range(2)] + [(mate, 1 - c)]
    pairs = [ring(pair + offset, half_nz) for offset in far_first(half_nz)]

    barrier = pltpu.get_barrier_semaphore()

    def load(src, dst, sem):
        copy = pltpu.make_async_copy(src, dst, load_sem.at[sem])
        copy.start()
        return copy

    first = [
        load(x_hbm, x_in, 0),
        load(gain_hbm, gain_in, 1),
        load(wq_hbm, w_in.at[0], 2),
        load(wk_hbm, w_in.at[1], 3),
        load(wv_hbm, w_in.at[2], 4),
        load(wg_hbm, w_in.at[3], 5),
        load(pos_hbm, pos_ref, 12),
        load(freq_hbm, freq_ref, 13),
    ]
    for peer, _ in kv_peers:
        pl.semaphore_signal(barrier, inc=1, device_id={"kv": peer}, device_id_type=MESH)
    for t in columns_x:
        for chip in (z, beside):
            for core in range(2):
                pl.semaphore_signal(
                    barrier, inc=1, device_id={"kv": chip * 2 + core, "tp": t}, device_id_type=MESH
                )

    here = pl.ds(pl.multiple_of(c * half_ff, 128), half_ff)
    there = pl.ds(pl.multiple_of((1 - c) * half_ff, 128), half_ff)
    mine = pl.ds(pl.multiple_of(c * size, 128), size)
    other_head = pl.ds(pl.multiple_of((1 - c) * size, 128), size)
    my_rows = pl.ds(pl.multiple_of(c * width, 128), width)
    my_place = pl.ds(pl.multiple_of((b * 2 + c) * width, 128), width)

    def up_part(half, core):
        return pl.ds(pl.multiple_of(core * half_ff + half * quarter, 128), quarter)

    later = [
        load(state_hbm, state_in, 6),
        load(wo_hbm.at[mine], wo_in.at[:, my_rows], 7),
        load(gain2_hbm, gain2.at[:, my_place], 8),
        load(wu_hbm.at[:, up_part(b, c)], wu_in.at[my_place], 9),
        load(wd_hbm.at[here], wd_in.at[:, my_rows], 10),
    ]

    for copy in first:
        copy.wait()
    x = x_in[...].astype(F32)
    normed = (x * gain_in[...]).astype(BF16)
    square = x * x
    sq_s[...] = jnp.sum(jnp.transpose(square), axis=0, keepdims=True)
    for n in range(4):
        both = jnp.dot(normed, w_in[n], preferred_element_type=F32)
        part[0, :, n * size : (n + 1) * size] = both[:, :size]
        part[1, :, n * size : (n + 1) * size] = both[:, size:]
    swap_s[...] = part[1 - c].astype(BF16)
    tok2[c] = x_in[...]

    pl.semaphore_wait(barrier, nk - 1 + 4 * (nt - 1))

    going, coming = {}, {}

    def remote(src, dst, phase, kv, t=None):
        where = {"kv": kv} if t is None else {"kv": kv, "tp": t}
        pltpu.make_async_remote_copy(
            src_ref=src,
            dst_ref=dst,
            send_sem=send_sem.at[phase],
            recv_sem=recv_sem.at[phase],
            device_id=where,
            device_id_type=MESH,
        ).start()

    def to_mate(src, dst, phase, amount):
        remote(src, dst, phase, mate)
        going[phase] = coming[phase] = amount

    def expect(count, phase, amount):
        going[phase] = coming[phase] = amount.at[pl.ds(0, count)]

    def arrived(phase):
        pause(coming.pop(phase), recv_sem.at[phase])

    def pause(amount, sem):
        if isinstance(amount, tuple):
            for core, one in enumerate(amount):
                if one is not None:
                    pl.when(c == core)(functools.partial(pause, one, sem))
        else:
            pltpu.make_async_copy(amount, amount, sem).wait()

    def finish():
        for phase in list(coming):
            arrived(phase)
        for phase, amount in going.items():
            pause(amount, send_sem.at[phase])

    to_mate(swap_s, swap_r, 0, swap_r)

    to_mate(sq_s, sq_m, 18, sq_m)
    to_mate(x_in, tok2.at[c], 2, x_in)
    to_mate(wo_hbm.at[other_head], wo_in.at[:, my_rows], 4, x_in)
    to_mate(wd_hbm.at[there], wd_in.at[:, my_rows], 6, wd_in.at[:, pl.ds(0, width)])

    arrived(18)
    sq_r[z] = sq_s[...] + sq_m[...]
    arrived(0)
    part[c] = part[c] + swap_r[...].astype(F32)
    for j in range(nk):
        send_a[j] = part[c, j * seqs : (j + 1) * seqs, :].astype(BF16)
    recv_a[me] = send_a[me]

    for chip in chips:
        for core in range(2):
            peer = chip * 2 + core
            remote(send_a.at[peer], recv_a.at[me], 7, peer)
        remote(sq_r.at[z], sq_r.at[z], 1, chip * 2 + c)
    remote(send_a.at[mate], recv_a.at[me], 7, mate)
    expect(nk - 1, 7, recv_a)
    expect(nz - 1, 1, sq_r)

    row = lax.broadcasted_iota(jnp.int32, (seqs, size), 0)
    lane = lax.broadcasted_iota(jnp.int32, (seqs, size), 1)
    place = jnp.zeros((seqs, size), F32)
    for i in range(seqs):
        place = jnp.where(row == i, pos_ref[i].astype(F32), place)
    angle = place * freq_ref[...]
    cosine = jnp.cos(angle)
    sine = jnp.sin(angle)
    sine = jnp.where(lane < size // 2, -sine, sine)
    later[0].wait()

    arrived(1)
    total_sq = jnp.sum(sq_r[...], axis=0)
    row_sq = jnp.sum(jnp.where(lane == row + me * seqs, total_sq, 0.0), axis=1, keepdims=True)
    scale1 = lax.rsqrt(row_sq / d_model + EPS)

    arrived(7)
    queries, keys, values, gates = [], [], [], []

    def turn(v):
        return v * cosine + pltpu.roll(v, size // 2, 1) * sine

    for h in range(2):
        total = recv_a[h].astype(F32)
        for j in range(1, nz):
            total = total + recv_a[2 * j + h].astype(F32)
        total = total * scale1
        queries.append(turn(total[:, :size]))
        keys.append(turn(total[:, size : 2 * size]) * size**-0.5)
        values.append(total[:, 2 * size : 3 * size])
        gates.append(total[:, 3 * size :])
    pad = jnp.zeros((size - 4 * seqs, size), F32)
    columns = jnp.transpose(jnp.concatenate(queries + keys + [pad], axis=0))
    for h in range(2):
        head = (tp * 2 + h).astype(F32)
        power = jnp.full((1, size), -5.0, F32) - 5.0 * head / (heads_all - 1)
        gamma = 1.0 - jnp.exp2(power)
        reads = []
        for i in range(seqs):
            at = h * seqs + i
            new = (
                gamma * state_in[i, h]
                + columns[:, 2 * seqs + at : 2 * seqs + at + 1] * values[h][i : i + 1]
            )
            state_new[i, h] = new
            reads.append(jnp.sum(columns[:, at : at + 1] * new, axis=0, keepdims=True))
        read = jnp.concatenate(reads, axis=0)
        read = read * lax.rsqrt(jnp.mean(read * read, axis=1, keepdims=True) + EPS)
        gate = gates[h]
        ret_s[h] = (read * (gate / (1.0 + jnp.exp(-gate)))).astype(BF16)
    ret_r[me] = ret_s[c]

    for peer, core in kv_peers:
        remote(ret_s.at[core], ret_r.at[me], 8, peer)
    expect(nk - 1, 8, ret_r)
    for half, core in ((b, 1 - c), (1 - b, 0), (1 - b, 1)):
        kv = (pair * 2 + half) * 2 + core
        remote(gain2_hbm, gain2.at[:, my_place], 3, kv)
        remote(wu_hbm.at[:, up_part(half, core)], wu_in.at[my_place], 5, kv)
    going[3] = coming[3] = gain2.at[:, pl.ds(0, 3 * width)]
    going[5] = coming[5] = wu_in.at[pl.ds(0, 3 * width)]
    state_copy = load(state_new, state_out, 11)

    later[1].wait()
    later[2].wait()
    arrived(2)
    arrived(3)
    arrived(4)
    for m in range(nt):
        for s in range(2):
            tok_rows[m, :, s * width : (s + 1) * width] = tok2[
                s, m * group : (m + 1) * group
            ].astype(F32)

    arrived(8)
    for j in range(nk):
        ret_f[j * seqs : (j + 1) * seqs] = ret_r[j].astype(F32)
    terms = jnp.dot(ret_f[...].astype(BF16), wo_in[...], preferred_element_type=F32)

    def send_sums(which, phase):
        send_c[which] = terms.reshape(nt, group, 2 * width).astype(BF16)
        slot = recv_c.at[which, tp * 2 + c]
        for t in columns_x:
            remote(send_c.at[which, t], slot, phase, z * 2 + 1, t)

        @pl.when(c == 0)
        def _():
            remote(send_c.at[which, tp], slot, phase, mate)

        @pl.when(c == 1)
        def _():
            recv_c[which, tp * 2 + 1] = send_c[which, tp]

        going[phase] = (send_c.at[which], send_c.at[which, pl.ds(0, nt - 1)])
        coming[phase] = (None, recv_c.at[which, pl.ds(0, nb - 1)])

    def added(which):
        return jnp.sum(recv_c[which].astype(F32), axis=0)

    send_sums(0, 9)
    arrived(9)
    @pl.when(c == 1)
    def _():
        mixed = (tok_rows[tp] + added(0)).astype(BF16)
        mix_s[...] = mixed
        mix_r[b, tp] = mixed
        for t in columns_x:
            for core in range(2):
                remote(mix_s, mix_r.at[b, tp], 20, beside * 2 + core, t)
                remote(mix_s, mix_r.at[b, tp], 10, z * 2 + core, t)
        for core in range(2):
            remote(mix_s, mix_r.at[b, tp], 20, beside * 2 + core)
        remote(mix_s, mix_r.at[b, tp], 10, mate)

    going[10] = (None, recv_c.at[0, pl.ds(0, nb - 1)])
    going[20] = (None, recv_c.at[0])
    coming[10] = (mix_r.at[0], mix_r.at[0, pl.ds(0, nt - 1)])
    coming[20] = mix_r.at[0]
    later[3].wait()
    arrived(5)
    arrived(10)
    arrived(20)
    middle = jnp.concatenate(
        [mix_r[half].astype(F32).reshape(rows, 2 * width) for half in range(2)], axis=1
    )
    square = middle * middle
    square = sum(square[:, k * width : (k + 1) * width] for k in range(4))
    sq2_s[...] = jnp.sum(jnp.transpose(square), axis=0, keepdims=True)
    sq2_r[pair] = sq2_s[...]
    for other in pairs:
        remote(sq2_s, sq2_r.at[pair], 11, (other * 2 + b) * 2 + 1 - c)
    expect(half_nz - 1, 11, sq2_r)
    normed2 = (middle * gain2[...]).astype(BF16)
    upward = jnp.dot(normed2, wu_in[...], preferred_element_type=F32)
    send_d[...] = upward.reshape(half_nz, 2 * per_chip, quarter).astype(BF16)

    def hop(src, dst, kv, phase, sem):
        pltpu.make_async_remote_copy(
            src_ref=src,
            dst_ref=dst,
            send_sem=send_sem.at[phase],
            recv_sem=sem,
            device_id={"kv": kv},
            device_id_type=MESH,
        ).start()

    for other in pairs:
        remote(send_d.at[other], recv_d.at[pair], 12, (other * 2 + b) * 2 + 1 - c)
    remote(send_d.at[pair], recv_d.at[pair], 12, mate)
    going[12] = coming[12] = recv_d
    right, left = ring(z + 1, nz), ring(z + nz - 1, nz)
    row = lax.broadcasted_iota(jnp.int32, (2 * per_chip, size), 0)
    lane = lax.broadcasted_iota(jnp.int32, (2 * per_chip, size), 1)
    arrived(11)
    total_sq = jnp.sum(sq2_r[...], axis=0)
    row_sq = jnp.sum(jnp.where(lane == row + pair * 2 * per_chip, total_sq, 0.0), axis=1, keepdims=True)
    scale2 = lax.rsqrt(row_sq / d_model + EPS)
    arrived(12)
    total = recv_d[0].astype(F32)
    for k in range(1, half_nz):
        total = total + recv_d[k].astype(F32)
    hidden = jnp.maximum(total * scale2, 0.0)
    hid_s[...] = (hidden * hidden).astype(BF16)
    for k, offset in enumerate(relayed):
        hop(hid_s, hid_in.at[k], ring(z + offset, nz) * 2 + c, 13, far_sem.at[k])
    going[13] = hid_in
    remote(hid_s, hid_r.at[z], 17, mate)
    for k in reversed(range(nr)):
        source = ring(z + nz - relayed[k], nz)
        pltpu.make_async_copy(hid_in.at[k], hid_in.at[k], far_sem.at[k]).wait()
        for kv in (right * 2 + 1 - c, left * 2 + 1 - c, mate):
            remote(hid_in.at[k], hid_r.at[source], 17, kv)
    going[17] = coming[17] = hid_r
    later[4].wait()
    arrived(6)
    arrived(17)
    everyone = hid_r[...].reshape(half_nz, 2, 2 * per_chip, quarter)
    terms = sum(
        jnp.dot(
            everyone[:, half].reshape(rows, quarter),
            wd_in[half * quarter : (half + 1) * quarter],
            preferred_element_type=F32,
        )
        for half in range(2)
    )
    send_sums(1, 14)
    arrived(14)
    @pl.when(c == 1)
    def _():
        final = (mix_s[...].astype(F32) + added(1)).astype(BF16)
        for s in range(2):
            out_s[s] = final[:, s * width : (s + 1) * width]
        out_r[tp] = out_s[1]
        for t in columns_x:
            for core in range(2):
                remote(out_s.at[core], out_r.at[tp], 15, z * 2 + core, t)
        remote(out_s.at[0], out_r.at[tp], 15, mate)

    going[15] = (None, recv_c.at[0, pl.ds(0, nb - 1), :, pl.ds(0, width)])
    coming[15] = (out_r, out_r.at[pl.ds(0, nt - 1)])

    state_copy.wait()
    finish()
    out_ref[...] = out_r[...].reshape(rows, width)


def solution(mesh):
    nk, nt = mesh.shape["kv"], mesh.shape["tp"]
    nz = nk // 2

    def shards(
        tokens,
        positions,
        state,
        norm_gain,
        w_query,
        w_key,
        w_value,
        w_gate,
        w_out,
        mlp_gain,
        w_up,
        w_down,
    ):
        rows, width = tokens.shape
        seqs, heads, size, _ = state.shape
        ff = w_up.shape[1]
        per_chip = rows // nz
        nb = 2 * nt
        group = rows // nt
        inverse = 10000.0 ** (-(np.arange(size // 2, dtype=np.float64) * 2.0) / size)
        freq = jnp.asarray(np.concatenate([inverse, inverse])[None, :].astype(np.float32))
        anywhere = pl.BlockSpec(memory_space=pltpu.HBM)
        vmem = pl.BlockSpec(memory_space=pltpu.VMEM)
        relayed = (8, 5, 11, 2, 14)
        nr = len(relayed)
        cfg = (nk, nt, nz, width * nk, heads * nt, relayed)
        scratch = [
            ((1, size), F32),
            ((rows, width), BF16),
            ((1, width), F32),
            ((4, width, heads * size), BF16),
            (state.shape, F32),
            (state.shape, F32),
            ((size, 2 * width), BF16),
            ((4 * width, ff // 4), BF16),
            ((ff // 2, 2 * width), BF16),
            ((2, rows, width), BF16),
            ((1, 4 * width), F32),
            ((2, rows, 4 * size), F32),
            ((rows, 4 * size), BF16),
            ((rows, 4 * size), BF16),
            ((1, rows), F32),
            ((1, rows), F32),
            ((nz, 1, rows), F32),
            ((nk, seqs, 4 * size), BF16),
            ((nk, seqs, 4 * size), BF16),
            ((2, seqs, size), BF16),
            ((nk, seqs, size), BF16),
            ((rows, size), F32),
            ((2, nt, group, 2 * width), BF16),
            ((2, nb, group, 2 * width), BF16),
            ((nt, group, 2 * width), F32),
            ((group, 2 * width), BF16),
            ((2, nt, group, 2 * width), BF16),
            ((1, rows), F32),
            ((nz // 2, 1, rows), F32),
            ((nz // 2, 2 * per_chip, ff // 4), BF16),
            ((nz // 2, 2 * per_chip, ff // 4), BF16),
            ((2 * per_chip, ff // 4), BF16),
            ((nr, 2 * per_chip, ff // 4), BF16),
            ((nz, 2 * per_chip, ff // 4), BF16),
            ((2, group, width), BF16),
            ((nt, group, width), BF16),
        ]
        return pl.pallas_call(
            functools.partial(kernel, cfg),
            out_shape=(
                jax.ShapeDtypeStruct((rows, width), BF16),
                jax.ShapeDtypeStruct(state.shape, F32),
            ),
            in_specs=[anywhere] * 13,
            out_specs=(vmem, anywhere),
            scratch_shapes=[pltpu.SMEM((seqs,), jnp.int32)]
            + [pltpu.VMEM(s, t) for s, t in scratch]
            + [
                pltpu.SemaphoreType.DMA((14,)),
                pltpu.SemaphoreType.DMA((21,)),
                pltpu.SemaphoreType.DMA((21,)),
                pltpu.SemaphoreType.DMA((nr,)),
            ],
            compiler_params=pltpu.CompilerParams(
                collective_id=0, has_side_effects=True
            ),
            name="step",
        )(
            positions,
            tokens,
            state,
            norm_gain.reshape(1, width),
            w_query,
            w_key,
            w_value,
            w_gate,
            w_out,
            mlp_gain.reshape(1, width),
            w_up,
            w_down,
            freq,
        )

    return jax.shard_map(
        shards,
        mesh=mesh,
        in_specs=(
            P("grp", "kv"),
            P(("grp", "kv")),
            P(("grp", "kv"), "tp", None, None),
            P("kv"),
            P("kv", "tp"),
            P("kv", "tp"),
            P("kv", "tp"),
            P("kv", "tp"),
            P("tp", "kv"),
            P("kv"),
            P("kv", "tp"),
            P("tp", "kv"),
        ),
        out_specs=(P("grp", "kv"), P(("grp", "kv"), "tp", None, None)),
        check_vma=False,
    )
```

```python
import functools

import jax
import jax.numpy as jnp
import numpy as np
from jax import lax
from jax.experimental import pallas as pl
from jax.experimental.pallas import tpu as pltpu
from jax.sharding import PartitionSpec as P

MESH = pl.DeviceIdType.MESH
F32 = jnp.float32
BF16 = jnp.bfloat16
EPS = 1e-06


def far_first(count):
    return sorted(range(1, count), key=lambda offset: -min(offset, count - offset))


def kernel(
    cfg,
    pos_hbm,
    x_hbm,
    state_hbm,
    gain_hbm,
    wq_hbm,
    wk_hbm,
    wv_hbm,
    wg_hbm,
    wo_hbm,
    gain2_hbm,
    wu_hbm,
    wd_hbm,
    freq_hbm,
    out_ref,
    state_out,
    pos_ref,
    freq_ref,
    x_in,
    gain_in,
    w_in,
    state_in,
    wo_in,
    wu_in,
    wd_in,
    tok2,
    gain2,
    part,
    swap_s,
    swap_r,
    sq_s,
    sq_m,
    sq_r,
    send_a,
    recv_a,
    ret_s,
    ret_r,
    ret_f,
    send_c,
    recv_c,
    tok_rows,
    mix_s,
    mix_r,
    sq2_s,
    sq2_r,
    send_d,
    near_d,
    relay_d,
    recv_d,
    hid_s,
    hid_in,
    hid_r,
    out_s,
    out_r,
    load_sem,
    send_sem,
    recv_sem,
    near_sem,
    far_sem,
):
    nk, nt, nz, d_model, heads_all, relayed = cfg
    me = lax.axis_index("kv")
    tp = lax.axis_index("tp")
    z = me // 2
    c = me % 2
    mate = me + 1 - 2 * c
    nb = nt * 2
    group = x_in.shape[0] // nt
    rows = x_in.shape[0]
    width = x_in.shape[1]
    seqs = rows // nk
    per_chip = rows // nz
    size = width
    half_ff = wu_in.shape[1]
    nr = near_d.shape[0]

    def ring(at, count):
        return at - count * (at >= count).astype(jnp.int32)

    chips = [ring(z + offset, nz) for offset in far_first(nz)]
    columns_x = [ring(tp + offset, nt) for offset in far_first(nt)]
    kv_peers = [(chip * 2 + core, core) for chip in chips for core in range(2)] + [(mate, 1 - c)]
    block_peers = [(t, core) for t in columns_x for core in range(2)] + [(tp, 1 - c)]

    barrier = pltpu.get_barrier_semaphore()

    def load(src, dst, sem):
        copy = pltpu.make_async_copy(src, dst, load_sem.at[sem])
        copy.start()
        return copy

    first = [
        load(x_hbm, x_in, 0),
        load(gain_hbm, gain_in, 1),
        load(wq_hbm, w_in.at[0], 2),
        load(wk_hbm, w_in.at[1], 3),
        load(wv_hbm, w_in.at[2], 4),
        load(wg_hbm, w_in.at[3], 5),
        load(pos_hbm, pos_ref, 12),
        load(freq_hbm, freq_ref, 13),
    ]
    for peer, _ in kv_peers:
        pl.semaphore_signal(barrier, inc=1, device_id={"kv": peer}, device_id_type=MESH)
    for t, core in block_peers[:-1]:
        pl.semaphore_signal(
            barrier, inc=1, device_id={"kv": z * 2 + core, "tp": t}, device_id_type=MESH
        )

    here = pl.ds(pl.multiple_of(c * half_ff, 128), half_ff)
    there = pl.ds(pl.multiple_of((1 - c) * half_ff, 128), half_ff)
    mine = pl.ds(pl.multiple_of(c * size, 128), size)
    other_head = pl.ds(pl.multiple_of((1 - c) * size, 128), size)
    my_rows = pl.ds(pl.multiple_of(c * width, 128), width)
    later = [
        load(state_hbm, state_in, 6),
        load(wo_hbm.at[mine], wo_in.at[:, my_rows], 7),
        load(gain2_hbm, gain2.at[:, my_rows], 8),
        load(wu_hbm.at[:, here], wu_in.at[my_rows], 9),
        load(wd_hbm.at[here], wd_in.at[:, my_rows], 10),
    ]

    for copy in first:
        copy.wait()
    x = x_in[...].astype(F32)
    normed = (x * gain_in[...]).astype(BF16)
    square = x * x
    sq_s[...] = jnp.sum(jnp.transpose(square), axis=0, keepdims=True)
    for n in range(4):
        both = jnp.dot(normed, w_in[n], preferred_element_type=F32)
        part[0, :, n * size : (n + 1) * size] = both[:, :size]
        part[1, :, n * size : (n + 1) * size] = both[:, size:]
    swap_s[...] = part[1 - c].astype(BF16)
    tok2[c] = x_in[...]

    pl.semaphore_wait(barrier, nk - 1 + nb - 2)

    going, coming = {}, {}

    def remote(src, dst, phase, kv, t=None):
        where = {"kv": kv} if t is None else {"kv": kv, "tp": t}
        pltpu.make_async_remote_copy(
            src_ref=src,
            dst_ref=dst,
            send_sem=send_sem.at[phase],
            recv_sem=recv_sem.at[phase],
            device_id=where,
            device_id_type=MESH,
        ).start()

    def to_mate(src, dst, phase, amount):
        remote(src, dst, phase, mate)
        going[phase] = coming[phase] = amount

    def expect(count, phase, amount):
        going[phase] = coming[phase] = amount.at[pl.ds(0, count)]

    def arrived(phase):
        pause(coming.pop(phase), recv_sem.at[phase])

    def pause(amount, sem):
        if isinstance(amount, tuple):
            for core, one in enumerate(amount):
                if one is not None:
                    pl.when(c == core)(functools.partial(pause, one, sem))
        else:
            pltpu.make_async_copy(amount, amount, sem).wait()

    def finish():
        for phase in list(coming):
            arrived(phase)
        for phase, amount in going.items():
            pause(amount, send_sem.at[phase])

    to_mate(swap_s, swap_r, 0, swap_r)

    to_mate(sq_s, sq_m, 18, sq_m)
    to_mate(x_in, tok2.at[c], 2, x_in)
    to_mate(gain2_hbm, gain2.at[:, my_rows], 3, gain_in)
    to_mate(wo_hbm.at[other_head], wo_in.at[:, my_rows], 4, x_in)
    to_mate(wu_hbm.at[:, there], wu_in.at[my_rows], 5, wu_in.at[pl.ds(0, width)])
    to_mate(wd_hbm.at[there], wd_in.at[:, my_rows], 6, wd_in.at[:, pl.ds(0, width)])

    arrived(18)
    sq_r[z] = sq_s[...] + sq_m[...]
    arrived(0)
    part[c] = part[c] + swap_r[...].astype(F32)
    for j in range(nk):
        send_a[j] = part[c, j * seqs : (j + 1) * seqs, :].astype(BF16)
    recv_a[me] = send_a[me]

    for chip in chips:
        for core in range(2):
            peer = chip * 2 + core
            remote(send_a.at[peer], recv_a.at[me], 7, peer)
        remote(sq_r.at[z], sq_r.at[z], 1, chip * 2 + c)
    remote(send_a.at[mate], recv_a.at[me], 7, mate)
    expect(nk - 1, 7, recv_a)
    expect(nz - 1, 1, sq_r)

    row = lax.broadcasted_iota(jnp.int32, (seqs, size), 0)
    lane = lax.broadcasted_iota(jnp.int32, (seqs, size), 1)
    place = jnp.zeros((seqs, size), F32)
    for i in range(seqs):
        place = jnp.where(row == i, pos_ref[i].astype(F32), place)
    angle = place * freq_ref[...]
    cosine = jnp.cos(angle)
    sine = jnp.sin(angle)
    sine = jnp.where(lane < size // 2, -sine, sine)
    later[0].wait()

    arrived(1)
    total_sq = jnp.sum(sq_r[...], axis=0)
    row_sq = jnp.sum(jnp.where(lane == row + me * seqs, total_sq, 0.0), axis=1, keepdims=True)
    scale1 = lax.rsqrt(row_sq / d_model + EPS)

    arrived(7)
    queries, keys, values, gates = [], [], [], []

    def turn(v):
        return v * cosine + pltpu.roll(v, size // 2, 1) * sine

    for h in range(2):
        total = recv_a[h].astype(F32)
        for j in range(1, nz):
            total = total + recv_a[2 * j + h].astype(F32)
        total = total * scale1
        queries.append(turn(total[:, :size]))
        keys.append(turn(total[:, size : 2 * size]) * size**-0.5)
        values.append(total[:, 2 * size : 3 * size])
        gates.append(total[:, 3 * size :])
    pad = jnp.zeros((size - 4 * seqs, size), F32)
    columns = jnp.transpose(jnp.concatenate(queries + keys + [pad], axis=0))
    for h in range(2):
        head = (tp * 2 + h).astype(F32)
        power = jnp.full((1, size), -5.0, F32) - 5.0 * head / (heads_all - 1)
        gamma = 1.0 - jnp.exp2(power)
        reads = []
        for i in range(seqs):
            at = h * seqs + i
            new = (
                gamma * state_in[i, h]
                + columns[:, 2 * seqs + at : 2 * seqs + at + 1] * values[h][i : i + 1]
            )
            state_out[i, h] = new
            reads.append(jnp.sum(columns[:, at : at + 1] * new, axis=0, keepdims=True))
        read = jnp.concatenate(reads, axis=0)
        read = read * lax.rsqrt(jnp.mean(read * read, axis=1, keepdims=True) + EPS)
        gate = gates[h]
        ret_s[h] = (read * (gate / (1.0 + jnp.exp(-gate)))).astype(BF16)
    ret_r[me] = ret_s[c]

    for peer, core in kv_peers:
        remote(ret_s.at[core], ret_r.at[me], 8, peer)
    expect(nk - 1, 8, ret_r)

    later[1].wait()
    later[2].wait()
    arrived(2)
    arrived(3)
    arrived(4)
    for m in range(nt):
        for s in range(2):
            tok_rows[m, :, s * width : (s + 1) * width] = tok2[
                s, m * group : (m + 1) * group
            ].astype(F32)

    arrived(8)
    for j in range(nk):
        ret_f[j * seqs : (j + 1) * seqs] = ret_r[j].astype(F32)
    terms = jnp.dot(ret_f[...].astype(BF16), wo_in[...], preferred_element_type=F32)

    def send_sums(which, phase):
        send_c[which] = terms.reshape(nt, group, 2 * width).astype(BF16)
        slot = recv_c.at[which, tp * 2 + c]
        for t in columns_x:
            remote(send_c.at[which, t], slot, phase, z * 2 + 1, t)

        @pl.when(c == 0)
        def _():
            remote(send_c.at[which, tp], slot, phase, mate)

        @pl.when(c == 1)
        def _():
            recv_c[which, tp * 2 + 1] = send_c[which, tp]

        going[phase] = (send_c.at[which], send_c.at[which, pl.ds(0, nt - 1)])
        coming[phase] = (None, recv_c.at[which, pl.ds(0, nb - 1)])

    def added(which):
        return jnp.sum(recv_c[which].astype(F32), axis=0)

    send_sums(0, 9)
    arrived(9)
    @pl.when(c == 1)
    def _():
        mixed = (tok_rows[tp] + added(0)).astype(BF16)
        mix_s[...] = mixed
        mix_r[tp] = mixed
        for t in columns_x:
            for core in range(2):
                remote(mix_s, mix_r.at[tp], 10, z * 2 + core, t)
        remote(mix_s, mix_r.at[tp], 10, mate)

    going[10] = (None, recv_c.at[0, pl.ds(0, nb - 1)])
    coming[10] = (mix_r, mix_r.at[pl.ds(0, nt - 1)])
    later[3].wait()
    arrived(5)
    arrived(10)
    middle = mix_r[...].astype(F32).reshape(rows, 2 * width)
    square = middle * middle
    sq2_s[...] = jnp.sum(
        jnp.transpose(square[:, :width] + square[:, width:]), axis=0, keepdims=True
    )
    sq2_r[z] = sq2_s[...]

    for chip in chips:
        remote(sq2_s, sq2_r.at[z], 11, chip * 2 + c)
    expect(nz - 1, 11, sq2_r)
    normed2 = (middle * gain2[...]).astype(BF16)
    upward = jnp.dot(normed2, wu_in[...], preferred_element_type=F32)
    send_d[...] = upward.reshape(nz, per_chip, half_ff).astype(BF16)

    right, left = ring(z + 1, nz), ring(z + nz - 1, nz)

    def hop(src, dst, kv, phase, sem):
        pltpu.make_async_remote_copy(
            src_ref=src,
            dst_ref=dst,
            send_sem=send_sem.at[phase],
            recv_sem=sem,
            device_id={"kv": kv},
            device_id_type=MESH,
        ).start()

    for k, offset in enumerate(relayed):
        hop(send_d.at[ring(right + offset, nz)], near_d.at[k, 0], right * 2 + c, 12, near_sem.at[k])
        hop(send_d.at[ring(left + offset, nz)], near_d.at[k, 1], left * 2 + c, 12, near_sem.at[k])
    going[12] = send_d.at[pl.ds(0, 2 * nr)]
    hop(send_d.at[z], recv_d.at[nr], mate, 19, far_sem.at[0])
    for k, offset in enumerate(relayed):
        target = ring(z + offset, nz)
        pltpu.make_async_copy(near_d.at[k], near_d.at[k], near_sem.at[k]).wait()
        relay_d[k] = (
            send_d[target].astype(F32) + near_d[k, 0].astype(F32) + near_d[k, 1].astype(F32)
        ).astype(BF16)
        hop(relay_d.at[k], recv_d.at[k], target * 2 + 1 - c, 16, far_sem.at[0])
    going[16] = relay_d
    going[19] = hid_s
    row = lax.broadcasted_iota(jnp.int32, (per_chip, size), 0)
    lane = lax.broadcasted_iota(jnp.int32, (per_chip, size), 1)
    arrived(11)
    total_sq = jnp.sum(sq2_r[...], axis=0)
    row_sq = jnp.sum(jnp.where(lane == row + z * per_chip, total_sq, 0.0), axis=1, keepdims=True)
    scale2 = lax.rsqrt(row_sq / d_model + EPS)
    pltpu.make_async_copy(recv_d, recv_d, far_sem.at[0]).wait()
    total = recv_d[0].astype(F32)
    for k in range(1, nr + 1):
        total = total + recv_d[k].astype(F32)
    hidden = jnp.maximum(total * scale2, 0.0)
    hid_s[...] = (hidden * hidden).astype(BF16)
    for k, offset in enumerate(relayed):
        hop(hid_s, hid_in.at[k], ring(z + offset, nz) * 2 + c, 13, far_sem.at[k + 1])
    going[13] = hid_in
    remote(hid_s, hid_r.at[z], 17, mate)
    for k in reversed(range(nr)):
        source = ring(z + nz - relayed[k], nz)
        pltpu.make_async_copy(hid_in.at[k], hid_in.at[k], far_sem.at[k + 1]).wait()
        for kv in (right * 2 + 1 - c, left * 2 + 1 - c, mate):
            remote(hid_in.at[k], hid_r.at[source], 17, kv)
    going[17] = coming[17] = hid_r
    later[4].wait()
    arrived(6)
    arrived(17)
    hidden_all = hid_r[...].astype(F32).reshape(rows, half_ff).astype(BF16)
    terms = jnp.dot(hidden_all, wd_in[...], preferred_element_type=F32)
    send_sums(1, 14)
    arrived(14)
    @pl.when(c == 1)
    def _():
        final = (mix_s[...].astype(F32) + added(1)).astype(BF16)
        for s in range(2):
            out_s[s] = final[:, s * width : (s + 1) * width]
        out_r[tp] = out_s[1]
        for t in columns_x:
            for core in range(2):
                remote(out_s.at[core], out_r.at[tp], 15, z * 2 + core, t)
        remote(out_s.at[0], out_r.at[tp], 15, mate)

    going[15] = (None, recv_c.at[0, pl.ds(0, nb - 1), :, pl.ds(0, width)])
    coming[15] = (out_r, out_r.at[pl.ds(0, nt - 1)])

    finish()
    out_ref[...] = out_r[...].reshape(rows, width)


def solution(mesh):
    nk, nt = mesh.shape["kv"], mesh.shape["tp"]
    nz = nk // 2

    def shards(
        tokens,
        positions,
        state,
        norm_gain,
        w_query,
        w_key,
        w_value,
        w_gate,
        w_out,
        mlp_gain,
        w_up,
        w_down,
    ):
        rows, width = tokens.shape
        seqs, heads, size, _ = state.shape
        ff = w_up.shape[1]
        per_chip = rows // nz
        nb = 2 * nt
        group = rows // nt
        inverse = 10000.0 ** (-(np.arange(size // 2, dtype=np.float64) * 2.0) / size)
        freq = jnp.asarray(np.concatenate([inverse, inverse])[None, :].astype(np.float32))
        anywhere = pl.BlockSpec(memory_space=pltpu.HBM)
        vmem = pl.BlockSpec(memory_space=pltpu.VMEM)
        relayed = (8, 5, 11, 2, 14)
        nr = len(relayed)
        cfg = (nk, nt, nz, width * nk, heads * nt, relayed)
        scratch = [
            ((1, size), F32),
            ((rows, width), BF16),
            ((1, width), F32),
            ((4, width, heads * size), BF16),
            (state.shape, F32),
            ((size, 2 * width), BF16),
            ((2 * width, ff // 2), BF16),
            ((ff // 2, 2 * width), BF16),
            ((2, rows, width), BF16),
            ((1, 2 * width), F32),
            ((2, rows, 4 * size), F32),
            ((rows, 4 * size), BF16),
            ((rows, 4 * size), BF16),
            ((1, rows), F32),
            ((1, rows), F32),
            ((nz, 1, rows), F32),
            ((nk, seqs, 4 * size), BF16),
            ((nk, seqs, 4 * size), BF16),
            ((2, seqs, size), BF16),
            ((nk, seqs, size), BF16),
            ((rows, size), F32),
            ((2, nt, group, 2 * width), BF16),
            ((2, nb, group, 2 * width), BF16),
            ((nt, group, 2 * width), F32),
            ((group, 2 * width), BF16),
            ((nt, group, 2 * width), BF16),
            ((1, rows), F32),
            ((nz, 1, rows), F32),
            ((nz, per_chip, ff // 2), BF16),
            ((nr, 2, per_chip, ff // 2), BF16),
            ((nr, per_chip, ff // 2), BF16),
            ((nr + 1, per_chip, ff // 2), BF16),
            ((per_chip, ff // 2), BF16),
            ((nr, per_chip, ff // 2), BF16),
            ((nz, per_chip, ff // 2), BF16),
            ((2, group, width), BF16),
            ((nt, group, width), BF16),
        ]
        return pl.pallas_call(
            functools.partial(kernel, cfg),
            out_shape=(
                pltpu.VMEM((rows, width), BF16),
                pltpu.VMEM(state.shape, F32),
            ),
            in_specs=[anywhere] * 13,
            out_specs=(vmem, vmem),
            scratch_shapes=[pltpu.SMEM((seqs,), jnp.int32)]
            + [pltpu.VMEM(s, t) for s, t in scratch]
            + [
                pltpu.SemaphoreType.DMA((14,)),
                pltpu.SemaphoreType.DMA((20,)),
                pltpu.SemaphoreType.DMA((20,)),
                pltpu.SemaphoreType.DMA((nr,)),
                pltpu.SemaphoreType.DMA((nr + 1,)),
            ],
            compiler_params=pltpu.CompilerParams(
                collective_id=0, has_side_effects=True
            ),
            name="step",
        )(
            positions,
            tokens,
            state,
            norm_gain.reshape(1, width),
            w_query,
            w_key,
            w_value,
            w_gate,
            w_out,
            mlp_gain.reshape(1, width),
            w_up,
            w_down,
            freq,
        )

    return jax.shard_map(
        shards,
        mesh=mesh,
        in_specs=(
            P("grp", "kv"),
            P(("grp", "kv")),
            P(("grp", "kv"), "tp", None, None),
            P("kv"),
            P("kv", "tp"),
            P("kv", "tp"),
            P("kv", "tp"),
            P("kv", "tp"),
            P("tp", "kv"),
            P("kv"),
            P("kv", "tp"),
            P("tp", "kv"),
        ),
        out_specs=(P("grp", "kv"), P(("grp", "kv"), "tp", None, None)),
        check_vma=False,
    )
```

```python
import functools

import jax
import jax.numpy as jnp
import numpy as np
from jax import lax
from jax.experimental import pallas as pl
from jax.experimental.pallas import tpu as pltpu
from jax.sharding import PartitionSpec as P

MESH = pl.DeviceIdType.MESH
F32 = jnp.float32
BF16 = jnp.bfloat16
EPS = 1e-06


def far_first(count):
    return sorted(range(1, count), key=lambda offset: -min(offset, count - offset))


def kernel(
    cfg,
    pos_hbm,
    x_hbm,
    state_hbm,
    gain_hbm,
    wq_hbm,
    wk_hbm,
    wv_hbm,
    wg_hbm,
    wo_hbm,
    gain2_hbm,
    wu_hbm,
    wd_hbm,
    freq_hbm,
    out_ref,
    state_out,
    pos_ref,
    freq_ref,
    x_in,
    gain_in,
    w_in,
    state_in,
    wo_in,
    wu_in,
    wd_in,
    tok2,
    gain2,
    part,
    swap_s,
    swap_r,
    sq_s,
    sq_m,
    sq_r,
    send_a,
    recv_a,
    send_u,
    recv_u,
    sq_u,
    ret_s,
    ret_r,
    ret_f,
    send_c,
    recv_c,
    tok_rows,
    mix_s,
    mix_r,
    sq2_s,
    sq2_r,
    send_d,
    near_d,
    relay_d,
    recv_d,
    hid_s,
    hid_in,
    hid_r,
    out_s,
    out_r,
    load_sem,
    send_sem,
    recv_sem,
    near_sem,
    far_sem,
):
    nk, nt, nz, d_model, heads_all, relayed = cfg
    me = lax.axis_index("kv")
    tp = lax.axis_index("tp")
    z = me // 2
    c = me % 2
    mate = me + 1 - 2 * c
    nb = nt * 2
    group = x_in.shape[0] // nt
    rows = x_in.shape[0]
    width = x_in.shape[1]
    seqs = rows // nk
    per_chip = rows // nz
    size = width
    half_ff = wu_in.shape[1]
    nr = near_d.shape[0]

    def ring(at, count):
        return at - count * (at >= count).astype(jnp.int32)

    chips = [ring(z + offset, nz) for offset in far_first(nz)]
    nu = recv_u.shape[0]
    columns_x = [ring(tp + offset, nt) for offset in far_first(nt)]
    kv_peers = [(chip * 2 + core, core) for chip in chips for core in range(2)] + [(mate, 1 - c)]
    block_peers = [(t, core) for t in columns_x for core in range(2)] + [(tp, 1 - c)]

    barrier = pltpu.get_barrier_semaphore()

    def load(src, dst, sem):
        copy = pltpu.make_async_copy(src, dst, load_sem.at[sem])
        copy.start()
        return copy

    def greet(peers):
        for peer, _ in peers:
            pl.semaphore_signal(barrier, inc=1, device_id={"kv": peer}, device_id_type=MESH)

    greet(kv_peers[: 2 * nu])
    first = [
        load(x_hbm, x_in, 0),
        load(gain_hbm, gain_in, 1),
        load(wq_hbm, w_in.at[0], 2),
        load(wk_hbm, w_in.at[1], 3),
        load(wv_hbm, w_in.at[2], 4),
        load(wg_hbm, w_in.at[3], 5),
        load(pos_hbm, pos_ref, 12),
        load(freq_hbm, freq_ref, 13),
    ]
    greet(kv_peers[2 * nu :])
    for t, core in block_peers[:-1]:
        pl.semaphore_signal(
            barrier, inc=1, device_id={"kv": z * 2 + core, "tp": t}, device_id_type=MESH
        )

    here = pl.ds(pl.multiple_of(c * half_ff, 128), half_ff)
    there = pl.ds(pl.multiple_of((1 - c) * half_ff, 128), half_ff)
    mine = pl.ds(pl.multiple_of(c * size, 128), size)
    other_head = pl.ds(pl.multiple_of((1 - c) * size, 128), size)
    my_rows = pl.ds(pl.multiple_of(c * width, 128), width)
    later = [
        load(state_hbm, state_in, 6),
        load(wo_hbm.at[mine], wo_in.at[:, my_rows], 7),
        load(gain2_hbm, gain2.at[:, my_rows], 8),
        load(wu_hbm.at[:, here], wu_in.at[my_rows], 9),
        load(wd_hbm.at[here], wd_in.at[:, my_rows], 10),
    ]

    for copy in first:
        copy.wait()
    x = x_in[...].astype(F32)
    normed = (x * gain_in[...]).astype(BF16)
    square = x * x
    sq_s[...] = jnp.sum(jnp.transpose(square), axis=0, keepdims=True)
    for n in range(4):
        both = jnp.dot(normed, w_in[n], preferred_element_type=F32)
        part[0, :, n * size : (n + 1) * size] = both[:, :size]
        part[1, :, n * size : (n + 1) * size] = both[:, size:]
    swap_s[...] = part[1 - c].astype(BF16)
    tok2[c] = x_in[...]
    for j in range(nk):
        for h in range(2):
            send_u[j, h] = part[h, j * seqs : (j + 1) * seqs, :].astype(BF16)
    for offset in far_first(nz)[:nu]:
        source = ring(z + nz - offset, nz)
        sq_r[source] = jnp.zeros_like(sq_s)
        for core in range(2):
            recv_a[source * 2 + core] = jnp.zeros(recv_a.shape[1:], BF16)

    pl.semaphore_wait(barrier, nk - 1 + nb - 2)

    going, coming = {}, {}

    def remote(src, dst, phase, kv, t=None):
        where = {"kv": kv} if t is None else {"kv": kv, "tp": t}
        pltpu.make_async_remote_copy(
            src_ref=src,
            dst_ref=dst,
            send_sem=send_sem.at[phase],
            recv_sem=recv_sem.at[phase],
            device_id=where,
            device_id_type=MESH,
        ).start()

    def to_mate(src, dst, phase, amount):
        remote(src, dst, phase, mate)
        going[phase] = coming[phase] = amount

    def expect(count, phase, amount):
        going[phase] = coming[phase] = amount.at[pl.ds(0, count)]

    def arrived(phase):
        pause(coming.pop(phase), recv_sem.at[phase])

    def pause(amount, sem):
        if isinstance(amount, tuple):
            for core, one in enumerate(amount):
                if one is not None:
                    pl.when(c == core)(functools.partial(pause, one, sem))
        else:
            pltpu.make_async_copy(amount, amount, sem).wait()

    def finish():
        for phase in list(coming):
            arrived(phase)
        for phase, amount in going.items():
            pause(amount, send_sem.at[phase])

    to_mate(swap_s, swap_r, 0, swap_r)

    to_mate(sq_s, sq_m, 18, sq_m)
    for k in range(nu):
        for core in range(2):
            peer = chips[k] * 2 + core
            remote(send_u.at[peer], recv_u.at[k, c], 21, peer)
            remote(sq_s, sq_u.at[k, c], 22, peer)
    going[21] = coming[21] = recv_u
    going[22] = coming[22] = sq_u
    to_mate(x_in, tok2.at[c], 2, x_in)
    to_mate(gain2_hbm, gain2.at[:, my_rows], 3, gain_in)
    to_mate(wo_hbm.at[other_head], wo_in.at[:, my_rows], 4, x_in)
    to_mate(wu_hbm.at[:, there], wu_in.at[my_rows], 5, wu_in.at[pl.ds(0, width)])
    to_mate(wd_hbm.at[there], wd_in.at[:, my_rows], 6, wd_in.at[:, pl.ds(0, width)])

    arrived(18)
    sq_r[z] = sq_s[...] + sq_m[...]
    arrived(0)
    part[c] = part[c] + swap_r[...].astype(F32)
    for j in range(nk):
        send_a[j] = part[c, j * seqs : (j + 1) * seqs, :].astype(BF16)
    recv_a[me] = send_a[me]

    for chip in chips[nu:]:
        for core in range(2):
            peer = chip * 2 + core
            remote(send_a.at[peer], recv_a.at[me], 7, peer)
        remote(sq_r.at[z], sq_r.at[z], 1, chip * 2 + c)
    remote(send_a.at[mate], recv_a.at[me], 7, mate)
    expect(nk - 1 - 2 * nu, 7, recv_a)
    expect(nz - 1 - nu, 1, sq_r)

    row = lax.broadcasted_iota(jnp.int32, (seqs, size), 0)
    lane = lax.broadcasted_iota(jnp.int32, (seqs, size), 1)
    place = jnp.zeros((seqs, size), F32)
    for i in range(seqs):
        place = jnp.where(row == i, pos_ref[i].astype(F32), place)
    angle = place * freq_ref[...]
    cosine = jnp.cos(angle)
    sine = jnp.sin(angle)
    sine = jnp.where(lane < size // 2, -sine, sine)
    later[0].wait()

    arrived(1)
    arrived(22)
    total_sq = jnp.sum(sq_r[...], axis=0)
    for k in range(nu):
        total_sq = total_sq + sq_u[k, 0] + sq_u[k, 1]
    row_sq = jnp.sum(jnp.where(lane == row + me * seqs, total_sq, 0.0), axis=1, keepdims=True)
    scale1 = lax.rsqrt(row_sq / d_model + EPS)

    arrived(7)
    arrived(21)
    queries, keys, values, gates = [], [], [], []

    def turn(v):
        return v * cosine + pltpu.roll(v, size // 2, 1) * sine

    for h in range(2):
        total = recv_a[h].astype(F32)
        for j in range(1, nz):
            total = total + recv_a[2 * j + h].astype(F32)
        for k in range(nu):
            total = total + recv_u[k, 0, h].astype(F32) + recv_u[k, 1, h].astype(F32)
        total = total * scale1
        queries.append(turn(total[:, :size]))
        keys.append(turn(total[:, size : 2 * size]) * size**-0.5)
        values.append(total[:, 2 * size : 3 * size])
        gates.append(total[:, 3 * size :])
    pad = jnp.zeros((size - 4 * seqs, size), F32)
    columns = jnp.transpose(jnp.concatenate(queries + keys + [pad], axis=0))
    for h in range(2):
        head = (tp * 2 + h).astype(F32)
        power = jnp.full((1, size), -5.0, F32) - 5.0 * head / (heads_all - 1)
        gamma = 1.0 - jnp.exp2(power)
        reads = []
        for i in range(seqs):
            at = h * seqs + i
            new = (
                gamma * state_in[i, h]
                + columns[:, 2 * seqs + at : 2 * seqs + at + 1] * values[h][i : i + 1]
            )
            state_out[i, h] = new
            reads.append(jnp.sum(columns[:, at : at + 1] * new, axis=0, keepdims=True))
        read = jnp.concatenate(reads, axis=0)
        read = read * lax.rsqrt(jnp.mean(read * read, axis=1, keepdims=True) + EPS)
        gate = gates[h]
        ret_s[h] = (read * (gate / (1.0 + jnp.exp(-gate)))).astype(BF16)
    ret_r[me] = ret_s[c]

    for peer, core in kv_peers:
        remote(ret_s.at[core], ret_r.at[me], 8, peer)
    expect(nk - 1, 8, ret_r)

    later[1].wait()
    later[2].wait()
    arrived(2)
    arrived(3)
    arrived(4)
    for m in range(nt):
        for s in range(2):
            tok_rows[m, :, s * width : (s + 1) * width] = tok2[
                s, m * group : (m + 1) * group
            ].astype(F32)

    arrived(8)
    for j in range(nk):
        ret_f[j * seqs : (j + 1) * seqs] = ret_r[j].astype(F32)
    terms = jnp.dot(ret_f[...].astype(BF16), wo_in[...], preferred_element_type=F32)

    def send_sums(which, phase):
        send_c[which] = terms.reshape(nt, group, 2 * width).astype(BF16)
        slot = recv_c.at[which, tp * 2 + c]
        for t in columns_x:
            remote(send_c.at[which, t], slot, phase, z * 2 + 1, t)

        @pl.when(c == 0)
        def _():
            remote(send_c.at[which, tp], slot, phase, mate)

        @pl.when(c == 1)
        def _():
            recv_c[which, tp * 2 + 1] = send_c[which, tp]

        going[phase] = (send_c.at[which], send_c.at[which, pl.ds(0, nt - 1)])
        coming[phase] = (None, recv_c.at[which, pl.ds(0, nb - 1)])

    def added(which):
        return jnp.sum(recv_c[which].astype(F32), axis=0)

    send_sums(0, 9)
    arrived(9)
    @pl.when(c == 1)
    def _():
        mixed = (tok_rows[tp] + added(0)).astype(BF16)
        mix_s[...] = mixed
        mix_r[tp] = mixed
        for t in columns_x:
            for core in range(2):
                remote(mix_s, mix_r.at[tp], 10, z * 2 + core, t)
        remote(mix_s, mix_r.at[tp], 10, mate)

    going[10] = (None, recv_c.at[0, pl.ds(0, nb - 1)])
    coming[10] = (mix_r, mix_r.at[pl.ds(0, nt - 1)])
    later[3].wait()
    arrived(5)
    arrived(10)
    middle = mix_r[...].astype(F32).reshape(rows, 2 * width)
    square = middle * middle
    sq2_s[...] = jnp.sum(
        jnp.transpose(square[:, :width] + square[:, width:]), axis=0, keepdims=True
    )
    sq2_r[z] = sq2_s[...]

    for chip in chips:
        remote(sq2_s, sq2_r.at[z], 11, chip * 2 + c)
    expect(nz - 1, 11, sq2_r)
    normed2 = (middle * gain2[...]).astype(BF16)
    upward = jnp.dot(normed2, wu_in[...], preferred_element_type=F32)
    send_d[...] = upward.reshape(nz, per_chip, half_ff).astype(BF16)

    right, left = ring(z + 1, nz), ring(z + nz - 1, nz)

    def hop(src, dst, kv, phase, sem):
        pltpu.make_async_remote_copy(
            src_ref=src,
            dst_ref=dst,
            send_sem=send_sem.at[phase],
            recv_sem=sem,
            device_id={"kv": kv},
            device_id_type=MESH,
        ).start()

    for k, offset in enumerate(relayed):
        hop(send_d.at[ring(right + offset, nz)], near_d.at[k, 0], right * 2 + c, 12, near_sem.at[k])
        hop(send_d.at[ring(left + offset, nz)], near_d.at[k, 1], left * 2 + c, 12, near_sem.at[k])
    going[12] = send_d.at[pl.ds(0, 2 * nr)]
    hop(send_d.at[z], recv_d.at[nr], mate, 19, far_sem.at[0])
    for k, offset in enumerate(relayed):
        target = ring(z + offset, nz)
        pltpu.make_async_copy(near_d.at[k], near_d.at[k], near_sem.at[k]).wait()
        relay_d[k] = (
            send_d[target].astype(F32) + near_d[k, 0].astype(F32) + near_d[k, 1].astype(F32)
        ).astype(BF16)
        hop(relay_d.at[k], recv_d.at[k], target * 2 + 1 - c, 16, far_sem.at[0])
    going[16] = relay_d
    going[19] = hid_s
    row = lax.broadcasted_iota(jnp.int32, (per_chip, size), 0)
    lane = lax.broadcasted_iota(jnp.int32, (per_chip, size), 1)
    arrived(11)
    total_sq = jnp.sum(sq2_r[...], axis=0)
    row_sq = jnp.sum(jnp.where(lane == row + z * per_chip, total_sq, 0.0), axis=1, keepdims=True)
    scale2 = lax.rsqrt(row_sq / d_model + EPS)
    pltpu.make_async_copy(recv_d, recv_d, far_sem.at[0]).wait()
    total = recv_d[0].astype(F32)
    for k in range(1, nr + 1):
        total = total + recv_d[k].astype(F32)
    hidden = jnp.maximum(total * scale2, 0.0)
    hid_s[...] = (hidden * hidden).astype(BF16)
    for k, offset in enumerate(relayed):
        hop(hid_s, hid_in.at[k], ring(z + offset, nz) * 2 + c, 13, far_sem.at[k + 1])
    going[13] = hid_in
    remote(hid_s, hid_r.at[z], 17, mate)
    for k in reversed(range(nr)):
        source = ring(z + nz - relayed[k], nz)
        pltpu.make_async_copy(hid_in.at[k], hid_in.at[k], far_sem.at[k + 1]).wait()
        for kv in (right * 2 + 1 - c, left * 2 + 1 - c, mate):
            remote(hid_in.at[k], hid_r.at[source], 17, kv)
    going[17] = coming[17] = hid_r
    later[4].wait()
    arrived(6)
    arrived(17)
    hidden_all = hid_r[...].astype(F32).reshape(rows, half_ff).astype(BF16)
    terms = jnp.dot(hidden_all, wd_in[...], preferred_element_type=F32)
    send_sums(1, 14)
    arrived(14)
    @pl.when(c == 1)
    def _():
        final = (mix_s[...].astype(F32) + added(1)).astype(BF16)
        for s in range(2):
            out_s[s] = final[:, s * width : (s + 1) * width]
        out_r[tp] = out_s[1]
        for t in columns_x:
            for core in range(2):
                remote(out_s.at[core], out_r.at[tp], 15, z * 2 + core, t)
        remote(out_s.at[0], out_r.at[tp], 15, mate)

    going[15] = (None, recv_c.at[0, pl.ds(0, nb - 1), :, pl.ds(0, width)])
    coming[15] = (out_r, out_r.at[pl.ds(0, nt - 1)])

    finish()
    out_ref[...] = out_r[...].reshape(rows, width)


def solution(mesh):
    nk, nt = mesh.shape["kv"], mesh.shape["tp"]
    nz = nk // 2

    def shards(
        tokens,
        positions,
        state,
        norm_gain,
        w_query,
        w_key,
        w_value,
        w_gate,
        w_out,
        mlp_gain,
        w_up,
        w_down,
    ):
        rows, width = tokens.shape
        seqs, heads, size, _ = state.shape
        ff = w_up.shape[1]
        per_chip = rows // nz
        nb = 2 * nt
        group = rows // nt
        inverse = 10000.0 ** (-(np.arange(size // 2, dtype=np.float64) * 2.0) / size)
        freq = jnp.asarray(np.concatenate([inverse, inverse])[None, :].astype(np.float32))
        anywhere = pl.BlockSpec(memory_space=pltpu.HBM)
        vmem = pl.BlockSpec(memory_space=pltpu.VMEM)
        relayed = (8, 5, 11, 2, 14)
        nr = len(relayed)
        cfg = (nk, nt, nz, width * nk, heads * nt, relayed)
        scratch = [
            ((1, size), F32),
            ((rows, width), BF16),
            ((1, width), F32),
            ((4, width, heads * size), BF16),
            (state.shape, F32),
            ((size, 2 * width), BF16),
            ((2 * width, ff // 2), BF16),
            ((ff // 2, 2 * width), BF16),
            ((2, rows, width), BF16),
            ((1, 2 * width), F32),
            ((2, rows, 4 * size), F32),
            ((rows, 4 * size), BF16),
            ((rows, 4 * size), BF16),
            ((1, rows), F32),
            ((1, rows), F32),
            ((nz, 1, rows), F32),
            ((nk, seqs, 4 * size), BF16),
            ((nk, seqs, 4 * size), BF16),
            ((nk, 2, seqs, 4 * size), BF16),
            ((3, 2, 2, seqs, 4 * size), BF16),
            ((3, 2, 1, rows), F32),
            ((2, seqs, size), BF16),
            ((nk, seqs, size), BF16),
            ((rows, size), F32),
            ((2, nt, group, 2 * width), BF16),
            ((2, nb, group, 2 * width), BF16),
            ((nt, group, 2 * width), F32),
            ((group, 2 * width), BF16),
            ((nt, group, 2 * width), BF16),
            ((1, rows), F32),
            ((nz, 1, rows), F32),
            ((nz, per_chip, ff // 2), BF16),
            ((nr, 2, per_chip, ff // 2), BF16),
            ((nr, per_chip, ff // 2), BF16),
            ((nr + 1, per_chip, ff // 2), BF16),
            ((per_chip, ff // 2), BF16),
            ((nr, per_chip, ff // 2), BF16),
            ((nz, per_chip, ff // 2), BF16),
            ((2, group, width), BF16),
            ((nt, group, width), BF16),
        ]
        return pl.pallas_call(
            functools.partial(kernel, cfg),
            out_shape=(
                pltpu.VMEM((rows, width), BF16),
                pltpu.VMEM(state.shape, F32),
            ),
            in_specs=[anywhere] * 13,
            out_specs=(vmem, vmem),
            scratch_shapes=[pltpu.SMEM((seqs,), jnp.int32)]
            + [pltpu.VMEM(s, t) for s, t in scratch]
            + [
                pltpu.SemaphoreType.DMA((14,)),
                pltpu.SemaphoreType.DMA((23,)),
                pltpu.SemaphoreType.DMA((23,)),
                pltpu.SemaphoreType.DMA((nr,)),
                pltpu.SemaphoreType.DMA((nr + 1,)),
            ],
            compiler_params=pltpu.CompilerParams(
                collective_id=0, has_side_effects=True
            ),
            name="step",
        )(
            positions,
            tokens,
            state,
            norm_gain.reshape(1, width),
            w_query,
            w_key,
            w_value,
            w_gate,
            w_out,
            mlp_gain.reshape(1, width),
            w_up,
            w_down,
            freq,
        )

    return jax.shard_map(
        shards,
        mesh=mesh,
        in_specs=(
            P("grp", "kv"),
            P(("grp", "kv")),
            P(("grp", "kv"), "tp", None, None),
            P("kv"),
            P("kv", "tp"),
            P("kv", "tp"),
            P("kv", "tp"),
            P("kv", "tp"),
            P("tp", "kv"),
            P("kv"),
            P("kv", "tp"),
            P("tp", "kv"),
        ),
        out_specs=(P("grp", "kv"), P(("grp", "kv"), "tp", None, None)),
        check_vma=False,
    )
```

```python
import functools

import jax
import jax.numpy as jnp
import numpy as np
from jax import lax
from jax.experimental import pallas as pl
from jax.experimental.pallas import tpu as pltpu
from jax.sharding import PartitionSpec as P

MESH = pl.DeviceIdType.MESH
F32 = jnp.float32
BF16 = jnp.bfloat16
EPS = 1e-06


def far_first(count):
    return sorted(range(1, count), key=lambda offset: -min(offset, count - offset))


def kernel(
    cfg,
    pos_hbm,
    x_hbm,
    state_hbm,
    gain_hbm,
    wq_hbm,
    wk_hbm,
    wv_hbm,
    wg_hbm,
    wo_hbm,
    gain2_hbm,
    wu_hbm,
    wd_hbm,
    freq_hbm,
    out_ref,
    state_out,
    pos_ref,
    freq_ref,
    x_in,
    gain_in,
    w_in,
    state_in,
    wo_in,
    wu_in,
    wd_in,
    tok2,
    gain2,
    part,
    swap_s,
    swap_r,
    sq_s,
    sq_m,
    sq_r,
    send_a,
    recv_a,
    ret_s,
    ret_r,
    ret_f,
    send_c,
    recv_c,
    tok_rows,
    mix_s,
    mix_r,
    sq2_s,
    sq2_r,
    send_d,
    near_d,
    relay_d,
    recv_d,
    hid_s,
    hid_in,
    hid_r,
    out_s,
    out_r,
    load_sem,
    send_sem,
    recv_sem,
    near_sem,
    far_sem,
):
    nk, nt, nz, d_model, heads_all, relayed = cfg
    me = lax.axis_index("kv")
    tp = lax.axis_index("tp")
    z = me // 2
    c = me % 2
    mate = me + 1 - 2 * c
    nb = nt * 2
    group = x_in.shape[0] // nt
    rows = x_in.shape[0]
    width = x_in.shape[1]
    seqs = rows // nk
    per_chip = rows // nz
    size = width
    half_ff = wu_in.shape[1]
    nr = near_d.shape[0]

    def ring(at, count):
        return at - count * (at >= count).astype(jnp.int32)

    chips = [ring(z + offset, nz) for offset in far_first(nz)]
    columns_x = [ring(tp + offset, nt) for offset in far_first(nt)]
    kv_peers = [(chip * 2 + core, core) for chip in chips for core in range(2)] + [(mate, 1 - c)]
    block_peers = [(t, core) for t in columns_x for core in range(2)] + [(tp, 1 - c)]

    barrier = pltpu.get_barrier_semaphore()

    def load(src, dst, sem):
        copy = pltpu.make_async_copy(src, dst, load_sem.at[sem])
        copy.start()
        return copy

    first = [
        load(x_hbm, x_in, 0),
        load(gain_hbm, gain_in, 1),
        load(wq_hbm, w_in.at[0], 2),
        load(wk_hbm, w_in.at[1], 3),
        load(wv_hbm, w_in.at[2], 4),
        load(wg_hbm, w_in.at[3], 5),
        load(pos_hbm, pos_ref, 12),
        load(freq_hbm, freq_ref, 13),
    ]
    for peer, _ in kv_peers:
        pl.semaphore_signal(barrier, inc=1, device_id={"kv": peer}, device_id_type=MESH)
    for t, core in block_peers[:-1]:
        pl.semaphore_signal(
            barrier, inc=1, device_id={"kv": z * 2 + core, "tp": t}, device_id_type=MESH
        )

    here = pl.ds(pl.multiple_of(c * half_ff, 128), half_ff)
    there = pl.ds(pl.multiple_of((1 - c) * half_ff, 128), half_ff)
    my_rows = pl.ds(pl.multiple_of(c * width, 128), width)
    later = [
        load(state_hbm, state_in, 6),
        load(wo_hbm, wo_in.at[:, my_rows], 7),
        load(gain2_hbm, gain2.at[:, my_rows], 8),
        load(wu_hbm.at[:, here], wu_in.at[my_rows], 9),
        load(wd_hbm.at[here], wd_in.at[:, my_rows], 10),
    ]

    for copy in first:
        copy.wait()
    x = x_in[...].astype(F32)
    normed = (x * gain_in[...]).astype(BF16)
    square = x * x
    sq_s[...] = jnp.sum(jnp.transpose(square), axis=0, keepdims=True)
    for n in range(4):
        both = jnp.dot(normed, w_in[n], preferred_element_type=F32)
        part[0, :, n * size : (n + 1) * size] = both[:, :size]
        part[1, :, n * size : (n + 1) * size] = both[:, size:]
    swap_s[...] = part[1 - c].astype(BF16)
    tok2[c] = x_in[...]

    pl.semaphore_wait(barrier, nk - 1 + nb - 2)

    going, coming = {}, {}

    def remote(src, dst, phase, kv, t=None):
        where = {"kv": kv} if t is None else {"kv": kv, "tp": t}
        pltpu.make_async_remote_copy(
            src_ref=src,
            dst_ref=dst,
            send_sem=send_sem.at[phase],
            recv_sem=recv_sem.at[phase],
            device_id=where,
            device_id_type=MESH,
        ).start()

    def to_mate(src, dst, phase, amount):
        remote(src, dst, phase, mate)
        going[phase] = coming[phase] = amount

    def expect(count, phase, amount):
        going[phase] = coming[phase] = amount.at[pl.ds(0, count)]

    def arrived(phase):
        pause(coming.pop(phase), recv_sem.at[phase])

    def pause(amount, sem):
        if isinstance(amount, tuple):
            for core, one in enumerate(amount):
                if one is not None:
                    pl.when(c == core)(functools.partial(pause, one, sem))
        else:
            pltpu.make_async_copy(amount, amount, sem).wait()

    def finish():
        for phase in list(coming):
            arrived(phase)
        for phase, amount in going.items():
            pause(amount, send_sem.at[phase])

    to_mate(swap_s, swap_r, 0, swap_r)

    to_mate(sq_s, sq_m, 18, sq_m)
    to_mate(x_in, tok2.at[c], 2, x_in)
    to_mate(gain2_hbm, gain2.at[:, my_rows], 3, gain_in)

    @pl.when(c == 0)
    def _():
        remote(wo_hbm, wo_in.at[:, my_rows], 4, mate)

    going[4] = (wo_in.at[:, pl.ds(0, width)], None)
    coming[4] = (None, wo_in.at[:, pl.ds(0, width)])
    to_mate(wu_hbm.at[:, there], wu_in.at[my_rows], 5, wu_in.at[pl.ds(0, width)])
    to_mate(wd_hbm.at[there], wd_in.at[:, my_rows], 6, wd_in.at[:, pl.ds(0, width)])

    arrived(18)
    sq_r[z] = sq_s[...] + sq_m[...]
    arrived(0)
    part[c] = part[c] + swap_r[...].astype(F32)
    for j in range(nk):
        send_a[j] = part[c, j * seqs : (j + 1) * seqs, :].astype(BF16)
    recv_a[me] = send_a[me]

    for chip in chips:
        for core in range(2):
            peer = chip * 2 + core
            remote(send_a.at[peer], recv_a.at[me], 7, peer)
        remote(sq_r.at[z], sq_r.at[z], 1, chip * 2 + c)
    remote(send_a.at[mate], recv_a.at[me], 7, mate)
    expect(nk - 1, 7, recv_a)
    expect(nz - 1, 1, sq_r)

    row = lax.broadcasted_iota(jnp.int32, (seqs, size), 0)
    lane = lax.broadcasted_iota(jnp.int32, (seqs, size), 1)
    place = jnp.zeros((seqs, size), F32)
    for i in range(seqs):
        place = jnp.where(row == i, pos_ref[i].astype(F32), place)
    angle = place * freq_ref[...]
    cosine = jnp.cos(angle)
    sine = jnp.sin(angle)
    sine = jnp.where(lane < size // 2, -sine, sine)
    later[0].wait()

    arrived(1)
    total_sq = jnp.sum(sq_r[...], axis=0)
    row_sq = jnp.sum(jnp.where(lane == row + me * seqs, total_sq, 0.0), axis=1, keepdims=True)
    scale1 = lax.rsqrt(row_sq / d_model + EPS)

    arrived(7)
    queries, keys, values, gates = [], [], [], []

    def turn(v):
        return v * cosine + pltpu.roll(v, size // 2, 1) * sine

    for h in range(2):
        total = recv_a[h].astype(F32)
        for j in range(1, nz):
            total = total + recv_a[2 * j + h].astype(F32)
        total = total * scale1
        queries.append(turn(total[:, :size]))
        keys.append(turn(total[:, size : 2 * size]) * size**-0.5)
        values.append(total[:, 2 * size : 3 * size])
        gates.append(total[:, 3 * size :])
    pad = jnp.zeros((size - 4 * seqs, size), F32)
    columns = jnp.transpose(jnp.concatenate(queries + keys + [pad], axis=0))
    for h in range(2):
        head = (tp * 2 + h).astype(F32)
        power = jnp.full((1, size), -5.0, F32) - 5.0 * head / (heads_all - 1)
        gamma = 1.0 - jnp.exp2(power)
        reads = []
        for i in range(seqs):
            at = h * seqs + i
            new = (
                gamma * state_in[i, h]
                + columns[:, 2 * seqs + at : 2 * seqs + at + 1] * values[h][i : i + 1]
            )
            state_out[i, h] = new
            reads.append(jnp.sum(columns[:, at : at + 1] * new, axis=0, keepdims=True))
        read = jnp.concatenate(reads, axis=0)
        read = read * lax.rsqrt(jnp.mean(read * read, axis=1, keepdims=True) + EPS)
        gate = gates[h]
        ret_s[:, h * size : (h + 1) * size] = (read * (gate / (1.0 + jnp.exp(-gate)))).astype(BF16)
    for chip in chips:
        remote(ret_s, ret_r.at[me], 8, chip * 2 + 1)

    @pl.when(c == 0)
    def _():
        remote(ret_s, ret_r.at[me], 8, mate)

    @pl.when(c == 1)
    def _():
        ret_r[me] = ret_s[...]

    going[8] = (ret_r.at[pl.ds(0, nz)], ret_r.at[pl.ds(0, nz - 1)])
    coming[8] = (None, ret_r.at[pl.ds(0, nk - 1)])

    later[1].wait()
    later[2].wait()
    arrived(2)
    arrived(3)
    arrived(4)
    for m in range(nt):
        for s in range(2):
            tok_rows[m, :, s * width : (s + 1) * width] = tok2[
                s, m * group : (m + 1) * group
            ].astype(F32)

    arrived(8)
    @pl.when(c == 1)
    def _():
        for j in range(nk):
            ret_f[j * seqs : (j + 1) * seqs] = ret_r[j].astype(F32)
        head_terms = jnp.dot(ret_f[...].astype(BF16), wo_in[...], preferred_element_type=F32)
        send_c[0] = head_terms.reshape(nt, group, 2 * width).astype(BF16)
        for t in columns_x:
            remote(send_c.at[0, t], recv_c.at[0, tp], 9, me, t)
        recv_c[0, tp] = send_c[0, tp]

    going[9] = (None, send_c.at[0, pl.ds(0, nt - 1)])
    coming[9] = (None, recv_c.at[0, pl.ds(0, nt - 1)])

    def send_sums(which, phase):
        send_c[which] = terms.reshape(nt, group, 2 * width).astype(BF16)
        slot = recv_c.at[which, tp * 2 + c]
        for t in columns_x:
            remote(send_c.at[which, t], slot, phase, z * 2 + 1, t)

        @pl.when(c == 0)
        def _():
            remote(send_c.at[which, tp], slot, phase, mate)

        @pl.when(c == 1)
        def _():
            recv_c[which, tp * 2 + 1] = send_c[which, tp]

        going[phase] = (send_c.at[which], send_c.at[which, pl.ds(0, nt - 1)])
        coming[phase] = (None, recv_c.at[which, pl.ds(0, nb - 1)])

    arrived(9)
    @pl.when(c == 1)
    def _():
        added = jnp.sum(recv_c[0, :nt].astype(F32), axis=0)
        mixed = (tok_rows[tp] + added).astype(BF16)
        mix_s[...] = mixed
        mix_r[tp] = mixed
        for t in columns_x:
            for core in range(2):
                remote(mix_s, mix_r.at[tp], 10, z * 2 + core, t)
        remote(mix_s, mix_r.at[tp], 10, mate)

    going[10] = (None, recv_c.at[0, pl.ds(0, nb - 1)])
    coming[10] = (mix_r, mix_r.at[pl.ds(0, nt - 1)])
    later[3].wait()
    arrived(5)
    arrived(10)
    middle = mix_r[...].astype(F32).reshape(rows, 2 * width)
    square = middle * middle
    sq2_s[...] = jnp.sum(
        jnp.transpose(square[:, :width] + square[:, width:]), axis=0, keepdims=True
    )
    sq2_r[z] = sq2_s[...]

    for chip in chips:
        remote(sq2_s, sq2_r.at[z], 11, chip * 2 + c)
    expect(nz - 1, 11, sq2_r)
    normed2 = (middle * gain2[...]).astype(BF16)
    upward = jnp.dot(normed2, wu_in[...], preferred_element_type=F32)
    send_d[...] = upward.reshape(nz, per_chip, half_ff).astype(BF16)

    right, left = ring(z + 1, nz), ring(z + nz - 1, nz)

    def hop(src, dst, kv, phase, sem):
        pltpu.make_async_remote_copy(
            src_ref=src,
            dst_ref=dst,
            send_sem=send_sem.at[phase],
            recv_sem=sem,
            device_id={"kv": kv},
            device_id_type=MESH,
        ).start()

    for k, offset in enumerate(relayed):
        hop(send_d.at[ring(right + offset, nz)], near_d.at[k, 0], right * 2 + c, 12, near_sem.at[k])
        hop(send_d.at[ring(left + offset, nz)], near_d.at[k, 1], left * 2 + c, 12, near_sem.at[k])
    going[12] = send_d.at[pl.ds(0, 2 * nr)]
    hop(send_d.at[z], recv_d.at[nr], mate, 19, far_sem.at[0])
    for k, offset in enumerate(relayed):
        target = ring(z + offset, nz)
        pltpu.make_async_copy(near_d.at[k], near_d.at[k], near_sem.at[k]).wait()
        relay_d[k] = (
            send_d[target].astype(F32) + near_d[k, 0].astype(F32) + near_d[k, 1].astype(F32)
        ).astype(BF16)
        hop(relay_d.at[k], recv_d.at[k], target * 2 + 1 - c, 16, far_sem.at[0])
    going[16] = relay_d
    going[19] = hid_s
    row = lax.broadcasted_iota(jnp.int32, (per_chip, size), 0)
    lane = lax.broadcasted_iota(jnp.int32, (per_chip, size), 1)
    arrived(11)
    total_sq = jnp.sum(sq2_r[...], axis=0)
    row_sq = jnp.sum(jnp.where(lane == row + z * per_chip, total_sq, 0.0), axis=1, keepdims=True)
    scale2 = lax.rsqrt(row_sq / d_model + EPS)
    pltpu.make_async_copy(recv_d, recv_d, far_sem.at[0]).wait()
    total = recv_d[0].astype(F32)
    for k in range(1, nr + 1):
        total = total + recv_d[k].astype(F32)
    hidden = jnp.maximum(total * scale2, 0.0)
    hid_s[...] = (hidden * hidden).astype(BF16)
    for k, offset in enumerate(relayed):
        hop(hid_s, hid_in.at[k], ring(z + offset, nz) * 2 + c, 13, far_sem.at[k + 1])
    going[13] = hid_in
    remote(hid_s, hid_r.at[z], 17, mate)
    for k in reversed(range(nr)):
        source = ring(z + nz - relayed[k], nz)
        pltpu.make_async_copy(hid_in.at[k], hid_in.at[k], far_sem.at[k + 1]).wait()
        for kv in (right * 2 + 1 - c, left * 2 + 1 - c, mate):
            remote(hid_in.at[k], hid_r.at[source], 17, kv)
    going[17] = coming[17] = hid_r
    later[4].wait()
    arrived(6)
    arrived(17)
    hidden_all = hid_r[...].astype(F32).reshape(rows, half_ff).astype(BF16)
    terms = jnp.dot(hidden_all, wd_in[...], preferred_element_type=F32)
    send_sums(1, 14)
    arrived(14)
    @pl.when(c == 1)
    def _():
        added = jnp.sum(recv_c[1].astype(F32), axis=0)
        final = (mix_s[...].astype(F32) + added).astype(BF16)
        for s in range(2):
            out_s[s] = final[:, s * width : (s + 1) * width]
        out_r[tp] = out_s[1]
        for t in columns_x:
            for core in range(2):
                remote(out_s.at[core], out_r.at[tp], 15, z * 2 + core, t)
        remote(out_s.at[0], out_r.at[tp], 15, mate)

    going[15] = (None, recv_c.at[0, pl.ds(0, nb - 1), :, pl.ds(0, width)])
    coming[15] = (out_r, out_r.at[pl.ds(0, nt - 1)])

    finish()
    out_ref[...] = out_r[...].reshape(rows, width)


def solution(mesh):
    nk, nt = mesh.shape["kv"], mesh.shape["tp"]
    nz = nk // 2

    def shards(
        tokens,
        positions,
        state,
        norm_gain,
        w_query,
        w_key,
        w_value,
        w_gate,
        w_out,
        mlp_gain,
        w_up,
        w_down,
    ):
        rows, width = tokens.shape
        seqs, heads, size, _ = state.shape
        ff = w_up.shape[1]
        per_chip = rows // nz
        nb = 2 * nt
        group = rows // nt
        inverse = 10000.0 ** (-(np.arange(size // 2, dtype=np.float64) * 2.0) / size)
        freq = jnp.asarray(np.concatenate([inverse, inverse])[None, :].astype(np.float32))
        anywhere = pl.BlockSpec(memory_space=pltpu.HBM)
        vmem = pl.BlockSpec(memory_space=pltpu.VMEM)
        relayed = (8, 5, 11, 2, 14)
        nr = len(relayed)
        cfg = (nk, nt, nz, width * nk, heads * nt, relayed)
        scratch = [
            ((1, size), F32),
            ((rows, width), BF16),
            ((1, width), F32),
            ((4, width, heads * size), BF16),
            (state.shape, F32),
            ((heads * size, 2 * width), BF16),
            ((2 * width, ff // 2), BF16),
            ((ff // 2, 2 * width), BF16),
            ((2, rows, width), BF16),
            ((1, 2 * width), F32),
            ((2, rows, 4 * size), F32),
            ((rows, 4 * size), BF16),
            ((rows, 4 * size), BF16),
            ((1, rows), F32),
            ((1, rows), F32),
            ((nz, 1, rows), F32),
            ((nk, seqs, 4 * size), BF16),
            ((nk, seqs, 4 * size), BF16),
            ((seqs, heads * size), BF16),
            ((nk, seqs, heads * size), BF16),
            ((rows, heads * size), F32),
            ((2, nt, group, 2 * width), BF16),
            ((2, nb, group, 2 * width), BF16),
            ((nt, group, 2 * width), F32),
            ((group, 2 * width), BF16),
            ((nt, group, 2 * width), BF16),
            ((1, rows), F32),
            ((nz, 1, rows), F32),
            ((nz, per_chip, ff // 2), BF16),
            ((nr, 2, per_chip, ff // 2), BF16),
            ((nr, per_chip, ff // 2), BF16),
            ((nr + 1, per_chip, ff // 2), BF16),
            ((per_chip, ff // 2), BF16),
            ((nr, per_chip, ff // 2), BF16),
            ((nz, per_chip, ff // 2), BF16),
            ((2, group, width), BF16),
            ((nt, group, width), BF16),
        ]
        return pl.pallas_call(
            functools.partial(kernel, cfg),
            out_shape=(
                pltpu.VMEM((rows, width), BF16),
                pltpu.VMEM(state.shape, F32),
            ),
            in_specs=[anywhere] * 13,
            out_specs=(vmem, vmem),
            scratch_shapes=[pltpu.SMEM((seqs,), jnp.int32)]
            + [pltpu.VMEM(s, t) for s, t in scratch]
            + [
                pltpu.SemaphoreType.DMA((14,)),
                pltpu.SemaphoreType.DMA((20,)),
                pltpu.SemaphoreType.DMA((20,)),
                pltpu.SemaphoreType.DMA((nr,)),
                pltpu.SemaphoreType.DMA((nr + 1,)),
            ],
            compiler_params=pltpu.CompilerParams(
                collective_id=0, has_side_effects=True
            ),
            name="step",
        )(
            positions,
            tokens,
            state,
            norm_gain.reshape(1, width),
            w_query,
            w_key,
            w_value,
            w_gate,
            w_out,
            mlp_gain.reshape(1, width),
            w_up,
            w_down,
            freq,
        )

    return jax.shard_map(
        shards,
        mesh=mesh,
        in_specs=(
            P("grp", "kv"),
            P(("grp", "kv")),
            P(("grp", "kv"), "tp", None, None),
            P("kv"),
            P("kv", "tp"),
            P("kv", "tp"),
            P("kv", "tp"),
            P("kv", "tp"),
            P("tp", "kv"),
            P("kv"),
            P("kv", "tp"),
            P("tp", "kv"),
        ),
        out_specs=(P("grp", "kv"), P(("grp", "kv"), "tp", None, None)),
        check_vma=False,
    )
```

```python
import functools

import jax
import jax.numpy as jnp
import numpy as np
from jax import lax
from jax.experimental import pallas as pl
from jax.experimental.pallas import tpu as pltpu
from jax.sharding import PartitionSpec as P

MESH = pl.DeviceIdType.MESH
F32 = jnp.float32
BF16 = jnp.bfloat16
EPS = 1e-06


def far_first(count):
    return sorted(range(1, count), key=lambda offset: -min(offset, count - offset))


def kernel(
    cfg,
    pos_hbm,
    x_hbm,
    state_hbm,
    gain_hbm,
    wq_hbm,
    wk_hbm,
    wv_hbm,
    wg_hbm,
    wo_hbm,
    gain2_hbm,
    wu_hbm,
    wd_hbm,
    freq_hbm,
    out_ref,
    state_out,
    pos_ref,
    freq_ref,
    x_in,
    gain_in,
    w_in,
    state_in,
    wo_in,
    wu_in,
    wd_in,
    tok2,
    gain2,
    part,
    swap_s,
    swap_r,
    sq_s,
    sq_m,
    sq_r,
    send_a,
    recv_a,
    ret_s,
    ret_r,
    ret_f,
    send_c,
    recv_c,
    tok_rows,
    mix_s,
    mix_r,
    sq2_s,
    sq2_r,
    send_d,
    near_d,
    relay_d,
    recv_d,
    hid_s,
    hid_in,
    hid_r,
    out_s,
    out_r,
    load_sem,
    send_sem,
    recv_sem,
    near_sem,
    far_sem,
):
    nk, nt, nz, d_model, heads_all, relayed = cfg
    me = lax.axis_index("kv")
    tp = lax.axis_index("tp")
    z = me // 2
    c = me % 2
    mate = me + 1 - 2 * c
    nb = nt * 2
    group = x_in.shape[0] // nt
    rows = x_in.shape[0]
    width = x_in.shape[1]
    seqs = rows // nk
    per_chip = rows // nz
    size = width
    half_ff = wu_in.shape[1]
    nr = near_d.shape[0]

    def ring(at, count):
        return at - count * (at >= count).astype(jnp.int32)

    chips = [ring(z + offset, nz) for offset in far_first(nz)]
    columns_x = [ring(tp + offset, nt) for offset in far_first(nt)]
    kv_peers = [(chip * 2 + core, core) for chip in chips for core in range(2)] + [(mate, 1 - c)]
    block_peers = [(t, core) for t in columns_x for core in range(2)] + [(tp, 1 - c)]

    barrier = pltpu.get_barrier_semaphore()

    def load(src, dst, sem):
        copy = pltpu.make_async_copy(src, dst, load_sem.at[sem])
        copy.start()
        return copy

    def greet(peers):
        for peer, _ in peers:
            pl.semaphore_signal(barrier, inc=1, device_id={"kv": peer}, device_id_type=MESH)

    greet(kv_peers[:6])
    first = [
        load(x_hbm, x_in, 0),
        load(gain_hbm, gain_in, 1),
        load(wq_hbm, w_in.at[0], 2),
        load(wk_hbm, w_in.at[1], 3),
        load(wv_hbm, w_in.at[2], 4),
        load(wg_hbm, w_in.at[3], 5),
        load(pos_hbm, pos_ref, 12),
        load(freq_hbm, freq_ref, 13),
    ]
    greet(kv_peers[6:])
    for t, core in block_peers[:-1]:
        pl.semaphore_signal(
            barrier, inc=1, device_id={"kv": z * 2 + core, "tp": t}, device_id_type=MESH
        )

    here = pl.ds(pl.multiple_of(c * half_ff, 128), half_ff)
    there = pl.ds(pl.multiple_of((1 - c) * half_ff, 128), half_ff)
    my_rows = pl.ds(pl.multiple_of(c * width, 128), width)
    later = [
        load(state_hbm, state_in, 6),
        load(wo_hbm, wo_in.at[:, my_rows], 7),
        load(gain2_hbm, gain2.at[:, my_rows], 8),
        load(wu_hbm.at[:, here], wu_in.at[my_rows], 9),
        load(wd_hbm.at[here], wd_in.at[:, my_rows], 10),
    ]

    for copy in first:
        copy.wait()
    x = x_in[...].astype(F32)
    normed = (x * gain_in[...]).astype(BF16)
    for n in range(4):
        both = jnp.dot(normed, w_in[n], preferred_element_type=F32)
        part[0, :, n * size : (n + 1) * size] = both[:, :size]
        part[1, :, n * size : (n + 1) * size] = both[:, size:]
    swap_s[...] = part[1 - c].astype(BF16)

    pl.semaphore_wait(barrier, nk - 1 + nb - 2)

    going, coming = {}, {}

    def remote(src, dst, phase, kv, t=None):
        where = {"kv": kv} if t is None else {"kv": kv, "tp": t}
        pltpu.make_async_remote_copy(
            src_ref=src,
            dst_ref=dst,
            send_sem=send_sem.at[phase],
            recv_sem=recv_sem.at[phase],
            device_id=where,
            device_id_type=MESH,
        ).start()

    def to_mate(src, dst, phase, amount):
        remote(src, dst, phase, mate)
        going[phase] = coming[phase] = amount

    def expect(count, phase, amount):
        going[phase] = coming[phase] = amount.at[pl.ds(0, count)]

    def arrived(phase):
        pause(coming.pop(phase), recv_sem.at[phase])

    def pause(amount, sem):
        if isinstance(amount, tuple):
            for core, one in enumerate(amount):
                if one is not None:
                    pl.when(c == core)(functools.partial(pause, one, sem))
        else:
            pltpu.make_async_copy(amount, amount, sem).wait()

    def finish():
        for phase in list(coming):
            arrived(phase)
        for phase, amount in going.items():
            pause(amount, send_sem.at[phase])

    to_mate(swap_s, swap_r, 0, swap_r)

    square = x_in[...].astype(F32)
    square = square * square
    sq_s[...] = jnp.sum(jnp.transpose(square), axis=0, keepdims=True)
    to_mate(sq_s, sq_m, 18, sq_m)
    to_mate(x_in, tok2.at[c], 2, x_in)
    to_mate(gain2_hbm, gain2.at[:, my_rows], 3, gain_in)

    @pl.when(c == 0)
    def _():
        remote(wo_hbm, wo_in.at[:, my_rows], 4, mate)

    going[4] = (wo_in.at[:, pl.ds(0, width)], None)
    coming[4] = (None, wo_in.at[:, pl.ds(0, width)])
    to_mate(wu_hbm.at[:, there], wu_in.at[my_rows], 5, wu_in.at[pl.ds(0, width)])
    to_mate(wd_hbm.at[there], wd_in.at[:, my_rows], 6, wd_in.at[:, pl.ds(0, width)])

    arrived(18)
    sq_r[z] = sq_s[...] + sq_m[...]
    arrived(0)
    part[c] = part[c] + swap_r[...].astype(F32)
    for j in range(nk):
        send_a[j] = part[c, j * seqs : (j + 1) * seqs, :].astype(BF16)
    recv_a[me] = send_a[me]

    for chip in chips:
        for core in range(2):
            peer = chip * 2 + core
            remote(send_a.at[peer], recv_a.at[me], 7, peer)
        remote(sq_r.at[z], sq_r.at[z], 1, chip * 2 + c)
    remote(send_a.at[mate], recv_a.at[me], 7, mate)
    expect(nk - 1, 7, recv_a)
    expect(nz - 1, 1, sq_r)

    row = lax.broadcasted_iota(jnp.int32, (seqs, size), 0)
    lane = lax.broadcasted_iota(jnp.int32, (seqs, size), 1)
    place = jnp.zeros((seqs, size), F32)
    for i in range(seqs):
        place = jnp.where(row == i, pos_ref[i].astype(F32), place)
    angle = place * freq_ref[...]
    cosine = jnp.cos(angle)
    sine = jnp.sin(angle)
    sine = jnp.where(lane < size // 2, -sine, sine)
    later[0].wait()

    arrived(1)
    total_sq = jnp.sum(sq_r[...], axis=0)
    row_sq = jnp.sum(jnp.where(lane == row + me * seqs, total_sq, 0.0), axis=1, keepdims=True)
    scale1 = lax.rsqrt(row_sq / d_model + EPS)

    arrived(7)
    queries, keys, values, gates = [], [], [], []

    def turn(v):
        return v * cosine + pltpu.roll(v, size // 2, 1) * sine

    for h in range(2):
        total = recv_a[h].astype(F32)
        for j in range(1, nz):
            total = total + recv_a[2 * j + h].astype(F32)
        total = total * scale1
        queries.append(turn(total[:, :size]))
        keys.append(turn(total[:, size : 2 * size]) * size**-0.5)
        values.append(total[:, 2 * size : 3 * size])
        gates.append(total[:, 3 * size :])
    pad = jnp.zeros((size - 4 * seqs, size), F32)
    columns = jnp.transpose(jnp.concatenate(queries + keys + [pad], axis=0))
    for h in range(2):
        head = (tp * 2 + h).astype(F32)
        power = jnp.full((1, size), -5.0, F32) - 5.0 * head / (heads_all - 1)
        gamma = 1.0 - jnp.exp2(power)
        reads = []
        for i in range(seqs):
            at = h * seqs + i
            new = (
                gamma * state_in[i, h]
                + columns[:, 2 * seqs + at : 2 * seqs + at + 1] * values[h][i : i + 1]
            )
            state_out[i, h] = new
            reads.append(jnp.sum(columns[:, at : at + 1] * new, axis=0, keepdims=True))
        read = jnp.concatenate(reads, axis=0)
        read = read * lax.rsqrt(jnp.mean(read * read, axis=1, keepdims=True) + EPS)
        gate = gates[h]
        ret_s[:, h * size : (h + 1) * size] = (read * (gate / (1.0 + jnp.exp(-gate)))).astype(BF16)
    for chip in chips:
        remote(ret_s, ret_r.at[me], 8, chip * 2 + 1)

    @pl.when(c == 0)
    def _():
        remote(ret_s, ret_r.at[me], 8, mate)

    @pl.when(c == 1)
    def _():
        ret_r[me] = ret_s[...]

    going[8] = (ret_r.at[pl.ds(0, nz)], ret_r.at[pl.ds(0, nz - 1)])
    coming[8] = (None, ret_r.at[pl.ds(0, nk - 1)])

    later[1].wait()
    later[2].wait()
    arrived(2)
    tok2[c] = x_in[...]
    arrived(3)
    arrived(4)
    for m in range(nt):
        for s in range(2):
            tok_rows[m, :, s * width : (s + 1) * width] = tok2[
                s, m * group : (m + 1) * group
            ].astype(F32)

    arrived(8)
    @pl.when(c == 1)
    def _():
        for j in range(nk):
            ret_f[j * seqs : (j + 1) * seqs] = ret_r[j].astype(F32)
        head_terms = jnp.dot(ret_f[...].astype(BF16), wo_in[...], preferred_element_type=F32)
        send_c[0] = head_terms.reshape(nt, group, 2 * width).astype(BF16)
        for t in columns_x:
            remote(send_c.at[0, t], recv_c.at[0, tp], 9, me, t)
        recv_c[0, tp] = send_c[0, tp]

    going[9] = (None, send_c.at[0, pl.ds(0, nt - 1)])
    coming[9] = (None, recv_c.at[0, pl.ds(0, nt - 1)])

    def send_sums(which, phase):
        send_c[which] = terms.reshape(nt, group, 2 * width).astype(BF16)
        slot = recv_c.at[which, tp * 2 + c]
        for t in columns_x:
            remote(send_c.at[which, t], slot, phase, z * 2 + 1, t)

        @pl.when(c == 0)
        def _():
            remote(send_c.at[which, tp], slot, phase, mate)

        @pl.when(c == 1)
        def _():
            recv_c[which, tp * 2 + 1] = send_c[which, tp]

        going[phase] = (send_c.at[which], send_c.at[which, pl.ds(0, nt - 1)])
        coming[phase] = (None, recv_c.at[which, pl.ds(0, nb - 1)])

    arrived(9)
    @pl.when(c == 1)
    def _():
        added = jnp.sum(recv_c[0, :nt].astype(F32), axis=0)
        mixed = (tok_rows[tp] + added).astype(BF16)
        mix_s[...] = mixed
        mix_r[tp] = mixed
        for t in columns_x:
            for core in range(2):
                remote(mix_s, mix_r.at[tp], 10, z * 2 + core, t)
        remote(mix_s, mix_r.at[tp], 10, mate)

    going[10] = (None, recv_c.at[0, pl.ds(0, nb - 1)])
    coming[10] = (mix_r, mix_r.at[pl.ds(0, nt - 1)])
    later[3].wait()
    arrived(5)
    arrived(10)
    middle = mix_r[...].astype(F32).reshape(rows, 2 * width)
    normed2 = (middle * gain2[...]).astype(BF16)
    upward = jnp.dot(normed2, wu_in[...], preferred_element_type=F32)
    send_d[...] = upward.reshape(nz, per_chip, half_ff).astype(BF16)

    right, left = ring(z + 1, nz), ring(z + nz - 1, nz)

    def hop(src, dst, kv, phase, sem):
        pltpu.make_async_remote_copy(
            src_ref=src,
            dst_ref=dst,
            send_sem=send_sem.at[phase],
            recv_sem=sem,
            device_id={"kv": kv},
            device_id_type=MESH,
        ).start()

    for k, offset in enumerate(relayed):
        hop(send_d.at[ring(right + offset, nz)], near_d.at[k, 0], right * 2 + c, 12, near_sem.at[k])
        hop(send_d.at[ring(left + offset, nz)], near_d.at[k, 1], left * 2 + c, 12, near_sem.at[k])
    going[12] = send_d.at[pl.ds(0, 2 * nr)]
    hop(send_d.at[z], recv_d.at[nr], mate, 19, far_sem.at[0])
    square = middle * middle
    sq2_s[...] = jnp.sum(
        jnp.transpose(square[:, :width] + square[:, width:]), axis=0, keepdims=True
    )
    sq2_r[z] = sq2_s[...]

    for chip in chips:
        remote(sq2_s, sq2_r.at[z], 11, chip * 2 + c)
    expect(nz - 1, 11, sq2_r)
    for k, offset in enumerate(relayed):
        target = ring(z + offset, nz)
        pltpu.make_async_copy(near_d.at[k], near_d.at[k], near_sem.at[k]).wait()
        relay_d[k] = (
            send_d[target].astype(F32) + near_d[k, 0].astype(F32) + near_d[k, 1].astype(F32)
        ).astype(BF16)
        hop(relay_d.at[k], recv_d.at[k], target * 2 + 1 - c, 16, far_sem.at[0])
    going[16] = relay_d
    going[19] = hid_s
    row = lax.broadcasted_iota(jnp.int32, (per_chip, size), 0)
    lane = lax.broadcasted_iota(jnp.int32, (per_chip, size), 1)
    arrived(11)
    total_sq = jnp.sum(sq2_r[...], axis=0)
    row_sq = jnp.sum(jnp.where(lane == row + z * per_chip, total_sq, 0.0), axis=1, keepdims=True)
    scale2 = lax.rsqrt(row_sq / d_model + EPS)
    pltpu.make_async_copy(recv_d, recv_d, far_sem.at[0]).wait()
    total = recv_d[0].astype(F32)
    for k in range(1, nr + 1):
        total = total + recv_d[k].astype(F32)
    hidden = jnp.maximum(total * scale2, 0.0)
    hid_s[...] = (hidden * hidden).astype(BF16)
    for k, offset in enumerate(relayed):
        hop(hid_s, hid_in.at[k], ring(z + offset, nz) * 2 + c, 13, far_sem.at[k + 1])
    going[13] = hid_in
    remote(hid_s, hid_r.at[z], 17, mate)
    for k in reversed(range(nr)):
        source = ring(z + nz - relayed[k], nz)
        pltpu.make_async_copy(hid_in.at[k], hid_in.at[k], far_sem.at[k + 1]).wait()
        for kv in (right * 2 + 1 - c, left * 2 + 1 - c, mate):
            remote(hid_in.at[k], hid_r.at[source], 17, kv)
    going[17] = coming[17] = hid_r
    later[4].wait()
    arrived(6)
    arrived(17)
    hidden_all = hid_r[...].astype(F32).reshape(rows, half_ff).astype(BF16)
    terms = jnp.dot(hidden_all, wd_in[...], preferred_element_type=F32)
    send_sums(1, 14)
    arrived(14)
    @pl.when(c == 1)
    def _():
        added = jnp.sum(recv_c[1].astype(F32), axis=0)
        final = (mix_s[...].astype(F32) + added).astype(BF16)
        for s in range(2):
            out_s[s] = final[:, s * width : (s + 1) * width]
        out_r[tp] = out_s[1]
        for t in columns_x:
            for core in range(2):
                remote(out_s.at[core], out_r.at[tp], 15, z * 2 + core, t)
        remote(out_s.at[0], out_r.at[tp], 15, mate)

    going[15] = (None, recv_c.at[0, pl.ds(0, nb - 1), :, pl.ds(0, width)])
    coming[15] = (out_r, out_r.at[pl.ds(0, nt - 1)])

    finish()
    out_ref[...] = out_r[...].reshape(rows, width)


def solution(mesh):
    nk, nt = mesh.shape["kv"], mesh.shape["tp"]
    nz = nk // 2

    def shards(
        tokens,
        positions,
        state,
        norm_gain,
        w_query,
        w_key,
        w_value,
        w_gate,
        w_out,
        mlp_gain,
        w_up,
        w_down,
    ):
        rows, width = tokens.shape
        seqs, heads, size, _ = state.shape
        ff = w_up.shape[1]
        per_chip = rows // nz
        nb = 2 * nt
        group = rows // nt
        inverse = 10000.0 ** (-(np.arange(size // 2, dtype=np.float64) * 2.0) / size)
        freq = jnp.asarray(np.concatenate([inverse, inverse])[None, :].astype(np.float32))
        anywhere = pl.BlockSpec(memory_space=pltpu.HBM)
        vmem = pl.BlockSpec(memory_space=pltpu.VMEM)
        relayed = (8, 5, 11, 2, 14)
        nr = len(relayed)
        cfg = (nk, nt, nz, width * nk, heads * nt, relayed)
        scratch = [
            ((1, size), F32),
            ((rows, width), BF16),
            ((1, width), F32),
            ((4, width, heads * size), BF16),
            (state.shape, F32),
            ((heads * size, 2 * width), BF16),
            ((2 * width, ff // 2), BF16),
            ((ff // 2, 2 * width), BF16),
            ((2, rows, width), BF16),
            ((1, 2 * width), F32),
            ((2, rows, 4 * size), F32),
            ((rows, 4 * size), BF16),
            ((rows, 4 * size), BF16),
            ((1, rows), F32),
            ((1, rows), F32),
            ((nz, 1, rows), F32),
            ((nk, seqs, 4 * size), BF16),
            ((nk, seqs, 4 * size), BF16),
            ((seqs, heads * size), BF16),
            ((nk, seqs, heads * size), BF16),
            ((rows, heads * size), F32),
            ((2, nt, group, 2 * width), BF16),
            ((2, nb, group, 2 * width), BF16),
            ((nt, group, 2 * width), F32),
            ((group, 2 * width), BF16),
            ((nt, group, 2 * width), BF16),
            ((1, rows), F32),
            ((nz, 1, rows), F32),
            ((nz, per_chip, ff // 2), BF16),
            ((nr, 2, per_chip, ff // 2), BF16),
            ((nr, per_chip, ff // 2), BF16),
            ((nr + 1, per_chip, ff // 2), BF16),
            ((per_chip, ff // 2), BF16),
            ((nr, per_chip, ff // 2), BF16),
            ((nz, per_chip, ff // 2), BF16),
            ((2, group, width), BF16),
            ((nt, group, width), BF16),
        ]
        return pl.pallas_call(
            functools.partial(kernel, cfg),
            out_shape=(
                pltpu.VMEM((rows, width), BF16),
                pltpu.VMEM(state.shape, F32),
            ),
            in_specs=[anywhere] * 13,
            out_specs=(vmem, vmem),
            scratch_shapes=[pltpu.SMEM((seqs,), jnp.int32)]
            + [pltpu.VMEM(s, t) for s, t in scratch]
            + [
                pltpu.SemaphoreType.DMA((14,)),
                pltpu.SemaphoreType.DMA((20,)),
                pltpu.SemaphoreType.DMA((20,)),
                pltpu.SemaphoreType.DMA((nr,)),
                pltpu.SemaphoreType.DMA((nr + 1,)),
            ],
            compiler_params=pltpu.CompilerParams(
                collective_id=0, has_side_effects=True
            ),
            name="step",
        )(
            positions,
            tokens,
            state,
            norm_gain.reshape(1, width),
            w_query,
            w_key,
            w_value,
            w_gate,
            w_out,
            mlp_gain.reshape(1, width),
            w_up,
            w_down,
            freq,
        )

    return jax.shard_map(
        shards,
        mesh=mesh,
        in_specs=(
            P("grp", "kv"),
            P(("grp", "kv")),
            P(("grp", "kv"), "tp", None, None),
            P("kv"),
            P("kv", "tp"),
            P("kv", "tp"),
            P("kv", "tp"),
            P("kv", "tp"),
            P("tp", "kv"),
            P("kv"),
            P("kv", "tp"),
            P("tp", "kv"),
        ),
        out_specs=(P("grp", "kv"), P(("grp", "kv"), "tp", None, None)),
        check_vma=False,
    )
```

```python
import functools

import jax
import jax.numpy as jnp
import numpy as np
from jax import lax
from jax.experimental import pallas as pl
from jax.experimental.pallas import tpu as pltpu
from jax.sharding import PartitionSpec as P

MESH = pl.DeviceIdType.MESH
F32 = jnp.float32
BF16 = jnp.bfloat16
EPS = 1e-06


def far_first(count):
    return sorted(range(1, count), key=lambda offset: -min(offset, count - offset))


def kernel(
    cfg,
    pos_hbm,
    x_hbm,
    state_hbm,
    gain_hbm,
    wq_hbm,
    wk_hbm,
    wv_hbm,
    wg_hbm,
    wo_hbm,
    gain2_hbm,
    wu_hbm,
    wd_hbm,
    freq_hbm,
    out_ref,
    state_out,
    pos_ref,
    freq_ref,
    x_in,
    gain_in,
    w_in,
    state_in,
    wo_in,
    wu_in,
    wd_in,
    tok2,
    gain2,
    part,
    swap_s,
    swap_r,
    sq_s,
    sq_m,
    sq_r,
    send_a,
    recv_a,
    ret_s,
    ret_r,
    ret_f,
    send_c,
    recv_c,
    tok_rows,
    mix_s,
    mix_r,
    sq2_s,
    sq2_r,
    send_d,
    near_d,
    relay_d,
    recv_d,
    hid_s,
    hid_in,
    hid_r,
    out_s,
    out_r,
    load_sem,
    send_sem,
    recv_sem,
    near_sem,
    far_sem,
):
    nk, nt, nz, d_model, heads_all, relayed = cfg
    me = lax.axis_index("kv")
    tp = lax.axis_index("tp")
    z = me // 2
    c = me % 2
    mate = me + 1 - 2 * c
    nb = nt * 2
    group = x_in.shape[0] // nt
    rows = x_in.shape[0]
    width = x_in.shape[1]
    seqs = rows // nk
    per_chip = rows // nz
    size = width
    half_ff = wu_in.shape[1]
    nr = near_d.shape[0]

    def ring(at, count):
        return at - count * (at >= count).astype(jnp.int32)

    chips = [ring(z + offset, nz) for offset in far_first(nz)]
    columns_x = [ring(tp + offset, nt) for offset in far_first(nt)]
    kv_peers = [(chip * 2 + core, core) for chip in chips for core in range(2)] + [(mate, 1 - c)]
    block_peers = [(t, core) for t in columns_x for core in range(2)] + [(tp, 1 - c)]

    barrier = pltpu.get_barrier_semaphore()

    def load(src, dst, sem):
        copy = pltpu.make_async_copy(src, dst, load_sem.at[sem])
        copy.start()
        return copy

    def greet(peers):
        for peer, _ in peers:
            pl.semaphore_signal(barrier, inc=1, device_id={"kv": peer}, device_id_type=MESH)

    greet(kv_peers[:6])
    first = [
        load(x_hbm, x_in, 0),
        load(gain_hbm, gain_in, 1),
        load(wq_hbm, w_in.at[0], 2),
        load(wk_hbm, w_in.at[1], 3),
        load(wv_hbm, w_in.at[2], 4),
        load(wg_hbm, w_in.at[3], 5),
        load(pos_hbm, pos_ref, 12),
        load(freq_hbm, freq_ref, 13),
    ]
    greet(kv_peers[6:])
    for t, core in block_peers[:-1]:
        pl.semaphore_signal(
            barrier, inc=1, device_id={"kv": z * 2 + core, "tp": t}, device_id_type=MESH
        )

    here = pl.ds(pl.multiple_of(c * half_ff, 128), half_ff)
    there = pl.ds(pl.multiple_of((1 - c) * half_ff, 128), half_ff)
    my_rows = pl.ds(pl.multiple_of(c * width, 128), width)
    later = [
        load(state_hbm, state_in, 6),
        load(wo_hbm, wo_in.at[:, my_rows], 7),
        load(gain2_hbm, gain2.at[:, my_rows], 8),
        load(wu_hbm.at[:, here], wu_in.at[my_rows], 9),
        load(wd_hbm.at[here], wd_in.at[:, my_rows], 10),
    ]

    for copy in first:
        copy.wait()
    x = x_in[...].astype(F32)
    normed = (x * gain_in[...]).astype(BF16)
    for n in range(4):
        both = jnp.dot(normed, w_in[n], preferred_element_type=F32)
        part[0, :, n * size : (n + 1) * size] = both[:, :size]
        part[1, :, n * size : (n + 1) * size] = both[:, size:]
    swap_s[...] = part[1 - c].astype(BF16)

    pl.semaphore_wait(barrier, nk - 1 + nb - 2)

    going, coming = {}, {}

    def remote(src, dst, phase, kv, t=None):
        where = {"kv": kv} if t is None else {"kv": kv, "tp": t}
        pltpu.make_async_remote_copy(
            src_ref=src,
            dst_ref=dst,
            send_sem=send_sem.at[phase],
            recv_sem=recv_sem.at[phase],
            device_id=where,
            device_id_type=MESH,
        ).start()

    def to_mate(src, dst, phase, amount):
        remote(src, dst, phase, mate)
        going[phase] = coming[phase] = amount

    def expect(count, phase, amount):
        going[phase] = coming[phase] = amount.at[pl.ds(0, count)]

    def arrived(phase):
        pause(coming.pop(phase), recv_sem.at[phase])

    def pause(amount, sem):
        if isinstance(amount, tuple):
            for core, one in enumerate(amount):
                if one is not None:
                    pl.when(c == core)(functools.partial(pause, one, sem))
        else:
            pltpu.make_async_copy(amount, amount, sem).wait()

    def finish():
        for phase in list(coming):
            arrived(phase)
        for phase, amount in going.items():
            pause(amount, send_sem.at[phase])

    to_mate(swap_s, swap_r, 0, swap_r)

    square = x_in[...].astype(F32)
    square = square * square
    sq_s[...] = jnp.sum(jnp.transpose(square), axis=0, keepdims=True)
    to_mate(sq_s, sq_m, 18, sq_m)
    to_mate(x_in, tok2.at[c], 2, x_in)
    to_mate(gain2_hbm, gain2.at[:, my_rows], 3, gain_in)

    @pl.when(c == 0)
    def _():
        remote(wo_hbm, wo_in.at[:, my_rows], 4, mate)

    going[4] = (wo_in.at[:, pl.ds(0, width)], None)
    coming[4] = (None, wo_in.at[:, pl.ds(0, width)])
    to_mate(wu_hbm.at[:, there], wu_in.at[my_rows], 5, wu_in.at[pl.ds(0, width)])
    to_mate(wd_hbm.at[there], wd_in.at[:, my_rows], 6, wd_in.at[:, pl.ds(0, width)])

    arrived(18)
    sq_r[z] = sq_s[...] + sq_m[...]
    arrived(0)
    part[c] = part[c] + swap_r[...].astype(F32)
    for j in range(nk):
        send_a[j] = part[c, j * seqs : (j + 1) * seqs, :].astype(BF16)
    recv_a[me] = send_a[me]

    for chip in chips:
        for core in range(2):
            peer = chip * 2 + core
            remote(send_a.at[peer], recv_a.at[me], 7, peer)
        remote(sq_r.at[z], sq_r.at[z], 1, chip * 2 + c)
    remote(send_a.at[mate], recv_a.at[me], 7, mate)
    expect(nk - 1, 7, recv_a)
    expect(nz - 1, 1, sq_r)

    row = lax.broadcasted_iota(jnp.int32, (seqs, size), 0)
    lane = lax.broadcasted_iota(jnp.int32, (seqs, size), 1)
    place = jnp.zeros((seqs, size), F32)
    for i in range(seqs):
        place = jnp.where(row == i, pos_ref[i].astype(F32), place)
    angle = place * freq_ref[...]
    cosine = jnp.cos(angle)
    sine = jnp.sin(angle)
    sine = jnp.where(lane < size // 2, -sine, sine)
    later[0].wait()

    arrived(1)
    total_sq = jnp.sum(sq_r[...], axis=0)
    row_sq = jnp.sum(jnp.where(lane == row + me * seqs, total_sq, 0.0), axis=1, keepdims=True)
    scale1 = lax.rsqrt(row_sq / d_model + EPS)

    arrived(7)
    queries, keys, values, gates = [], [], [], []

    def turn(v):
        return v * cosine + pltpu.roll(v, size // 2, 1) * sine

    for h in range(2):
        total = recv_a[h].astype(F32)
        for j in range(1, nz):
            total = total + recv_a[2 * j + h].astype(F32)
        total = total * scale1
        queries.append(turn(total[:, :size]))
        keys.append(turn(total[:, size : 2 * size]) * size**-0.5)
        values.append(total[:, 2 * size : 3 * size])
        gates.append(total[:, 3 * size :])
    pad = jnp.zeros((size - 4 * seqs, size), F32)
    columns = jnp.transpose(jnp.concatenate(queries + keys + [pad], axis=0))
    for h in range(2):
        head = (tp * 2 + h).astype(F32)
        power = jnp.full((1, size), -5.0, F32) - 5.0 * head / (heads_all - 1)
        gamma = 1.0 - jnp.exp2(power)
        reads = []
        for i in range(seqs):
            at = h * seqs + i
            new = (
                gamma * state_in[i, h]
                + columns[:, 2 * seqs + at : 2 * seqs + at + 1] * values[h][i : i + 1]
            )
            state_out[i, h] = new
            reads.append(jnp.sum(columns[:, at : at + 1] * new, axis=0, keepdims=True))
        read = jnp.concatenate(reads, axis=0)
        read = read * lax.rsqrt(jnp.mean(read * read, axis=1, keepdims=True) + EPS)
        gate = gates[h]
        ret_s[:, h * size : (h + 1) * size] = (read * (gate / (1.0 + jnp.exp(-gate)))).astype(BF16)
    for chip in chips:
        remote(ret_s, ret_r.at[me], 8, chip * 2 + 1)

    @pl.when(c == 0)
    def _():
        remote(ret_s, ret_r.at[me], 8, mate)

    @pl.when(c == 1)
    def _():
        ret_r[me] = ret_s[...]

    going[8] = (ret_r.at[pl.ds(0, nz)], ret_r.at[pl.ds(0, nz - 1)])
    coming[8] = (None, ret_r.at[pl.ds(0, nk - 1)])

    later[1].wait()
    later[2].wait()
    arrived(2)
    tok2[c] = x_in[...]
    arrived(3)
    arrived(4)
    for m in range(nt):
        for s in range(2):
            tok_rows[m, :, s * width : (s + 1) * width] = tok2[
                s, m * group : (m + 1) * group
            ].astype(F32)

    arrived(8)
    @pl.when(c == 1)
    def _():
        for j in range(nk):
            ret_f[j * seqs : (j + 1) * seqs] = ret_r[j].astype(F32)
        head_terms = jnp.dot(ret_f[...].astype(BF16), wo_in[...], preferred_element_type=F32)
        send_c[0] = head_terms.reshape(nt, group, 2 * width).astype(BF16)
        for t in columns_x:
            remote(send_c.at[0, t], recv_c.at[0, tp], 9, me, t)
        recv_c[0, tp] = send_c[0, tp]

    going[9] = (None, send_c.at[0, pl.ds(0, nt - 1)])
    coming[9] = (None, recv_c.at[0, pl.ds(0, nt - 1)])

    def send_sums(which, phase):
        send_c[which] = terms.reshape(nt, group, 2 * width).astype(BF16)
        slot = recv_c.at[which, tp * 2 + c]
        for t in columns_x:
            remote(send_c.at[which, t], slot, phase, z * 2 + 1, t)

        @pl.when(c == 0)
        def _():
            remote(send_c.at[which, tp], slot, phase, mate)

        @pl.when(c == 1)
        def _():
            recv_c[which, tp * 2 + 1] = send_c[which, tp]

        going[phase] = (send_c.at[which], send_c.at[which, pl.ds(0, nt - 1)])
        coming[phase] = (None, recv_c.at[which, pl.ds(0, nb - 1)])

    arrived(9)
    @pl.when(c == 1)
    def _():
        added = jnp.sum(recv_c[0, :nt].astype(F32), axis=0)
        mixed = (tok_rows[tp] + added).astype(BF16)
        mix_s[...] = mixed
        mix_r[tp] = mixed
        for t in columns_x:
            for core in range(2):
                remote(mix_s, mix_r.at[tp], 10, z * 2 + core, t)
        remote(mix_s, mix_r.at[tp], 10, mate)

    going[10] = (None, recv_c.at[0, pl.ds(0, nb - 1)])
    coming[10] = (mix_r, mix_r.at[pl.ds(0, nt - 1)])
    later[3].wait()
    arrived(5)
    arrived(10)
    middle = mix_r[...].astype(F32).reshape(rows, 2 * width)
    normed2 = (middle * gain2[...]).astype(BF16)
    upward = jnp.dot(normed2, wu_in[...], preferred_element_type=F32)
    send_d[...] = upward.reshape(nz, per_chip, half_ff).astype(BF16)

    right, left = ring(z + 1, nz), ring(z + nz - 1, nz)

    def hop(src, dst, kv, phase, sem):
        pltpu.make_async_remote_copy(
            src_ref=src,
            dst_ref=dst,
            send_sem=send_sem.at[phase],
            recv_sem=sem,
            device_id={"kv": kv},
            device_id_type=MESH,
        ).start()

    for k, offset in enumerate(relayed):
        hop(send_d.at[ring(right + offset, nz)], near_d.at[k, 0], right * 2 + c, 12, near_sem.at[k])
        hop(send_d.at[ring(left + offset, nz)], near_d.at[k, 1], left * 2 + c, 12, near_sem.at[k])
    going[12] = send_d.at[pl.ds(0, 2 * nr)]
    hop(send_d.at[z], recv_d.at[nr], mate, 19, far_sem.at[0])
    square = middle * middle
    sq2_s[...] = jnp.sum(
        jnp.transpose(square[:, :width] + square[:, width:]), axis=0, keepdims=True
    )
    sq2_r[z] = sq2_s[...]

    for chip in chips:
        remote(sq2_s, sq2_r.at[z], 11, chip * 2 + c)
    expect(nz - 1, 11, sq2_r)
    for k, offset in enumerate(relayed):
        target = ring(z + offset, nz)
        pltpu.make_async_copy(near_d.at[k], near_d.at[k], near_sem.at[k]).wait()
        relay_d[k] = (
            send_d[target].astype(F32) + near_d[k, 0].astype(F32) + near_d[k, 1].astype(F32)
        ).astype(BF16)
        hop(relay_d.at[k], recv_d.at[k], target * 2 + 1 - c, 16, far_sem.at[0])
    going[16] = relay_d
    going[19] = hid_s
    row = lax.broadcasted_iota(jnp.int32, (per_chip, size), 0)
    lane = lax.broadcasted_iota(jnp.int32, (per_chip, size), 1)
    arrived(11)
    total_sq = jnp.sum(sq2_r[...], axis=0)
    row_sq = jnp.sum(jnp.where(lane == row + z * per_chip, total_sq, 0.0), axis=1, keepdims=True)
    scale2 = lax.rsqrt(row_sq / d_model + EPS)
    pltpu.make_async_copy(recv_d, recv_d, far_sem.at[0]).wait()
    total = recv_d[0].astype(F32)
    for k in range(1, nr + 1):
        total = total + recv_d[k].astype(F32)
    hidden = jnp.maximum(total * scale2, 0.0)
    hid_s[...] = (hidden * hidden).astype(BF16)
    for k, offset in enumerate(relayed):
        hop(hid_s, hid_in.at[k], ring(z + offset, nz) * 2 + c, 13, far_sem.at[k + 1])
    going[13] = hid_in
    remote(hid_s, hid_r.at[z], 17, mate)
    for k in reversed(range(nr)):
        source = ring(z + nz - relayed[k], nz)
        pltpu.make_async_copy(hid_in.at[k], hid_in.at[k], far_sem.at[k + 1]).wait()
        for kv in (right * 2 + 1 - c, left * 2 + 1 - c, mate):
            remote(hid_in.at[k], hid_r.at[source], 17, kv)
    going[17] = coming[17] = hid_r
    later[4].wait()
    arrived(6)
    arrived(17)
    hidden_all = hid_r[...].astype(F32).reshape(rows, half_ff).astype(BF16)
    terms = jnp.dot(hidden_all, wd_in[...], preferred_element_type=F32)
    send_sums(1, 14)
    arrived(14)
    @pl.when(c == 1)
    def _():
        added = jnp.sum(recv_c[1].astype(F32), axis=0)
        final = (mix_s[...].astype(F32) + added).astype(BF16)
        for s in range(2):
            out_s[s] = final[:, s * width : (s + 1) * width]
        out_r[tp] = out_s[1]
        for t in columns_x:
            for core in range(2):
                remote(out_s.at[core], out_r.at[tp], 15, z * 2 + core, t)
        remote(out_s.at[0], out_r.at[tp], 15, mate)

    going[15] = (None, recv_c.at[0, pl.ds(0, nb - 1), :, pl.ds(0, width)])
    coming[15] = (out_r, out_r.at[pl.ds(0, nt - 1)])

    finish()
    out_ref[...] = out_r[...].reshape(rows, width)


def deliver(layer_ref, state_ref, layer_out, state_out, sem):
    first = pltpu.make_async_copy(state_ref, state_out, sem.at[0])
    second = pltpu.make_async_copy(layer_ref, layer_out, sem.at[1])
    first.start()
    second.start()
    first.wait()
    second.wait()


def solution(mesh):
    nk, nt = mesh.shape["kv"], mesh.shape["tp"]
    nz = nk // 2

    def shards(
        tokens,
        positions,
        state,
        norm_gain,
        w_query,
        w_key,
        w_value,
        w_gate,
        w_out,
        mlp_gain,
        w_up,
        w_down,
    ):
        rows, width = tokens.shape
        seqs, heads, size, _ = state.shape
        ff = w_up.shape[1]
        per_chip = rows // nz
        nb = 2 * nt
        group = rows // nt
        inverse = 10000.0 ** (-(np.arange(size // 2, dtype=np.float64) * 2.0) / size)
        freq = jnp.asarray(np.concatenate([inverse, inverse])[None, :].astype(np.float32))
        anywhere = pl.BlockSpec(memory_space=pltpu.HBM)
        vmem = pl.BlockSpec(memory_space=pltpu.VMEM)
        relayed = (8, 5, 11, 2, 14)
        nr = len(relayed)
        cfg = (nk, nt, nz, width * nk, heads * nt, relayed)
        scratch = [
            ((1, size), F32),
            ((rows, width), BF16),
            ((1, width), F32),
            ((4, width, heads * size), BF16),
            (state.shape, F32),
            ((heads * size, 2 * width), BF16),
            ((2 * width, ff // 2), BF16),
            ((ff // 2, 2 * width), BF16),
            ((2, rows, width), BF16),
            ((1, 2 * width), F32),
            ((2, rows, 4 * size), F32),
            ((rows, 4 * size), BF16),
            ((rows, 4 * size), BF16),
            ((1, rows), F32),
            ((1, rows), F32),
            ((nz, 1, rows), F32),
            ((nk, seqs, 4 * size), BF16),
            ((nk, seqs, 4 * size), BF16),
            ((seqs, heads * size), BF16),
            ((nk, seqs, heads * size), BF16),
            ((rows, heads * size), F32),
            ((2, nt, group, 2 * width), BF16),
            ((2, nb, group, 2 * width), BF16),
            ((nt, group, 2 * width), F32),
            ((group, 2 * width), BF16),
            ((nt, group, 2 * width), BF16),
            ((1, rows), F32),
            ((nz, 1, rows), F32),
            ((nz, per_chip, ff // 2), BF16),
            ((nr, 2, per_chip, ff // 2), BF16),
            ((nr, per_chip, ff // 2), BF16),
            ((nr + 1, per_chip, ff // 2), BF16),
            ((per_chip, ff // 2), BF16),
            ((nr, per_chip, ff // 2), BF16),
            ((nz, per_chip, ff // 2), BF16),
            ((2, group, width), BF16),
            ((nt, group, width), BF16),
        ]
        layer, new_state = pl.pallas_call(
            functools.partial(kernel, cfg),
            out_shape=(
                pltpu.VMEM((rows, width), BF16),
                pltpu.VMEM(state.shape, F32),
            ),
            in_specs=[anywhere] * 13,
            out_specs=(vmem, vmem),
            scratch_shapes=[pltpu.SMEM((seqs,), jnp.int32)]
            + [pltpu.VMEM(s, t) for s, t in scratch]
            + [
                pltpu.SemaphoreType.DMA((14,)),
                pltpu.SemaphoreType.DMA((20,)),
                pltpu.SemaphoreType.DMA((20,)),
                pltpu.SemaphoreType.DMA((nr,)),
                pltpu.SemaphoreType.DMA((nr + 1,)),
            ],
            compiler_params=pltpu.CompilerParams(
                collective_id=0, has_side_effects=True
            ),
            name="step",
        )(
            positions,
            tokens,
            state,
            norm_gain.reshape(1, width),
            w_query,
            w_key,
            w_value,
            w_gate,
            w_out,
            mlp_gain.reshape(1, width),
            w_up,
            w_down,
            freq,
        )
        return pl.pallas_call(
            deliver,
            out_shape=(
                jax.ShapeDtypeStruct(layer.shape, BF16),
                jax.ShapeDtypeStruct(state.shape, F32),
            ),
            in_specs=[vmem, vmem],
            out_specs=(anywhere, anywhere),
            scratch_shapes=[pltpu.SemaphoreType.DMA((2,))],
            name="deliver",
        )(
            pltpu.with_memory_space_constraint(layer, pltpu.VMEM),
            pltpu.with_memory_space_constraint(new_state, pltpu.VMEM),
        )

    return jax.shard_map(
        shards,
        mesh=mesh,
        in_specs=(
            P("grp", "kv"),
            P(("grp", "kv")),
            P(("grp", "kv"), "tp", None, None),
            P("kv"),
            P("kv", "tp"),
            P("kv", "tp"),
            P("kv", "tp"),
            P("kv", "tp"),
            P("tp", "kv"),
            P("kv"),
            P("kv", "tp"),
            P("tp", "kv"),
        ),
        out_specs=(P("grp", "kv"), P(("grp", "kv"), "tp", None, None)),
        check_vma=False,
    )
```
